32 devices in a mesh: sp: 16 (over z, y, x), tp: 2 (over core).
Axes of the slice: x: 2, y: 2, z: 4, core: 2. Of those that a mesh axis runs over, the one named last changes fastest.
Arguments:
- value_in: bfloat16 [4096, 2048], P('sp', 'tp'), may hold values from -25 to 25, as said below
- gate_in: bfloat16 [4096, 2048], P('sp', 'tp'), may hold values from -6 to 6
- taps: float32 [31, 2048], P(None, 'tp'), may hold values from -1 to 1
- gain: float32 [2048], P('tp'), may hold values from 0.1 to 1.9
- shift: float32 [2048], P('tp'), may hold values from -3 to 3
- w_out: bfloat16 [2048, 2048], P('tp'), may hold values from -0.125 to 0.125
- grad_out: bfloat16 [4096, 2048], P('sp'), may hold values from -6 to 6
Outputs:
- d_value: bfloat16 [4096, 2048], P('sp', 'tp')
- d_gate: bfloat16 [4096, 2048], P('sp', 'tp')
- d_taps: float32 [31, 2048], P(None, 'tp')
- d_gain: float32 [2048], P('tp')
- d_shift: float32 [2048], P('tp')
The draws below stay inside these ranges and needn't reach their ends.
Inputs may be any that keep to these rules, and one draw needn't show every extreme that they name: `value_in`: channel blocks of different magnitude.
All inputs are finite; a program needn't handle non-finite values.
Results may differ from the reference program's by a relative error of at most 0.007.
Values may be sent and summed in bfloat16 or wider, within the bound.
A program may use at most 64 MiB of HBM per device.

```python
import math
import jax
import jax.numpy as jnp
from jax import lax

C = 2048
D = 2048
KERNEL = 31
TOK_DEV = 256
TOKENS = 4096
N_SP = 16


def draw_value_in(key, part):
    key_base = jax.random.fold_in(key, 11)
    key_group = jax.random.fold_in(key, 12)
    key_flip = jax.random.fold_in(key, 13)
    base = jnp.clip(jax.random.normal(key_base, (TOKENS, C), jnp.float32), -4.0, 4.0)
    column = jnp.exp(jax.random.uniform(key_group, (C,), jnp.float32, -0.7, 0.7))
    flip = jax.random.randint(key_flip, (), 0, 2)
    upper = (jnp.arange(C) >= C // 2).astype(jnp.int32)
    factor = jnp.where(upper == flip, 3.0, 1.0)
    return (base * column * factor).astype(jnp.bfloat16)


def shard_levels(own_key, extent, pieces, low, high):
    factor_of = 1.0
    for position, shards_of in pieces:
        heights = jax.random.uniform(jax.random.fold_in(jax.random.fold_in(own_key, 6), position), (shards_of,), jnp.float32, low / len(pieces), high / len(pieces))
        factor_of = factor_of * jnp.repeat(jnp.exp(heights), extent[position] // shards_of).reshape((-1,) + (1,) * (len(extent) - 1 - position))
    return factor_of


def noise(rng, extent, scale, most, pieces=(), kind=jnp.bfloat16):
    array = scale * jax.random.normal(rng, extent, jnp.float32)
    if pieces:
        array = array * shard_levels(rng, extent, pieces, -0.22, 0.18)
    return jnp.clip(array, -most, most).astype(kind)


def setup_inputs(seed: int = 0) -> dict:
    splits = jax.random.split(jax.random.key(seed), 8)
    return {
        "value_in": draw_value_in(jax.random.fold_in(splits[7], 71), 0),
        "gate_in": noise(splits[1], (TOKENS, C), 1.5, 6.0, ((0, 16), (1, 2))),
        "taps": noise(splits[2], (KERNEL, C), 0.18, 1.0, ((1, 2),), jnp.float32),
        "gain": jnp.clip(1.0 + 0.18 * jax.random.normal(splits[3], (C,), jnp.float32), 0.1, 1.9),
        "shift": noise(splits[4], (C,), 0.5, 3.0, ((0, 2),), jnp.float32),
        "w_out": noise(splits[5], (C, D), D ** -0.5, 0.125, ((0, 2),)),
        "grad_out": noise(splits[6], (TOKENS, D), 1.0, 6.0, ((0, 16),)),
    }


EPS = 1e-05

def convolve(window, taps, count):
    total = jnp.zeros((count, window.shape[1]), jnp.float32)
    for offset in range(taps.shape[0]):
        total = total + taps[offset] * window[offset:offset + count]
    return total

def norm_backward(conv_out, grad_rows, gain, shift, w_out):
    width = conv_out.shape[1]
    mean = lax.optimization_barrier(jnp.sum(conv_out, 1)) / width
    var = lax.optimization_barrier(jnp.sum(conv_out * conv_out, 1)) / width - mean * mean
    inv = lax.rsqrt(var + EPS)
    normed = (conv_out - mean[:, None]) * inv[:, None]
    pre = normed * gain + shift
    grad_mix = jnp.dot(grad_rows, w_out.T, preferred_element_type=jnp.float32)
    sig = jax.nn.sigmoid(pre)
    grad_pre = grad_mix * sig * (1.0 + pre * (1.0 - sig))
    grad_normed = grad_pre * gain
    first = lax.optimization_barrier(jnp.sum(grad_normed, 1)) / width
    second = lax.optimization_barrier(jnp.sum(grad_normed * normed, 1)) / width
    grad_conv = inv[:, None] * (grad_normed - first[:, None] - normed * second[:, None])
    return (grad_conv, grad_pre, normed)

def reference(value_in, gate_in, taps, gain, shift, w_out, grad_out):
    half = KERNEL // 2
    gate_sig = jax.nn.sigmoid(gate_in.astype(jnp.float32))
    gated = (value_in.astype(jnp.float32) * gate_sig).astype(jnp.bfloat16)
    gated_pad = jnp.pad(gated, ((half, half), (0, 0)))

    def first_pass(index):
        start = (index * TOK_DEV).astype(jnp.int32)
        window = lax.dynamic_slice_in_dim(gated_pad, start, TOK_DEV + 2 * half, 0).astype(jnp.float32)
        conv_out = convolve(window, taps, TOK_DEV)
        grad_rows = lax.dynamic_slice_in_dim(grad_out, start, TOK_DEV, 0)
        grad_conv, grad_pre, normed = norm_backward(conv_out, grad_rows, gain, shift, w_out)
        return (grad_conv, lax.optimization_barrier(jnp.sum(grad_pre * normed, 0)), lax.optimization_barrier(jnp.sum(grad_pre, 0)))
    blocks = jnp.arange(N_SP, dtype=jnp.int32)
    grad_conv, gain_parts, shift_parts = lax.map(first_pass, blocks)
    grad_conv = grad_conv.reshape(TOKENS, C)
    grad_pad = jnp.pad(grad_conv, ((half, half), (0, 0)))

    def second_pass(index):
        start = (index * TOK_DEV).astype(jnp.int32)
        window = lax.dynamic_slice_in_dim(gated_pad, start, TOK_DEV + 2 * half, 0).astype(jnp.float32)
        grad_win = lax.dynamic_slice_in_dim(grad_pad, start, TOK_DEV + 2 * half, 0)
        own = grad_win[half:half + TOK_DEV]
        grad_gated = jnp.zeros((TOK_DEV, C), jnp.float32)
        for offset in range(KERNEL):
            grad_gated = grad_gated + taps[offset] * grad_win[2 * half - offset:2 * half - offset + TOK_DEV]
        tap_terms = jnp.stack([lax.optimization_barrier(jnp.sum(own * window[offset:offset + TOK_DEV], 0)) for offset in range(KERNEL)])
        return (grad_gated, tap_terms)
    grad_gated, tap_parts = lax.map(second_pass, blocks)
    grad_gated = grad_gated.reshape(TOKENS, C)
    scale = 1.0 / math.sqrt(TOKENS)
    d_value = (grad_gated * gate_sig).astype(jnp.bfloat16)
    d_gate = (grad_gated * value_in.astype(jnp.float32) * gate_sig * (1.0 - gate_sig)).astype(jnp.bfloat16)
    d_taps = lax.optimization_barrier(jnp.sum(tap_parts, 0)) * scale
    d_gain = lax.optimization_barrier(jnp.sum(gain_parts, 0)) * scale
    d_shift = lax.optimization_barrier(jnp.sum(shift_parts, 0)) * scale
    return (d_value, d_gate, d_taps, d_gain, d_shift)
```

```python
import functools
import math

import jax
import jax.numpy as jnp
import numpy as np
from jax import lax
from jax.experimental import pallas as pl
from jax.experimental.pallas import tpu as pltpu
from jax.sharding import PartitionSpec as P

EPS = 1e-05
ALIGN = 16
LANES = 128
CHUNK = 256
VMEM_GRANT = 48 * 1024 * 1024
F32 = jnp.float32
BF16 = jnp.bfloat16


class Plan:
    def __init__(self, rows, kernel, total):
        self.half = kernel // 2
        self.kernel = kernel
        self.rows = rows
        self.edge = -(-self.half // ALIGN) * ALIGN
        edge = self.edge
        self.block = rows // 2
        self.size = self.block + 2 * edge
        size = self.size
        self.freqs = size // 2
        self.wide = rows + 2 * edge
        omega = 2.0 * np.pi * (np.arange(self.freqs) + 0.5) / size

        def spectrum(times):
            angle = omega[:, None] * times[None, :]
            return np.concatenate([np.cos(angle), np.sin(angle)], 0)

        def inverse(times):
            angle = times[:, None] * omega[None, :]
            return np.concatenate([np.cos(angle), -np.sin(angle)], 1)

        own = np.arange(self.block)
        self.tap_rows = -(-kernel // ALIGN) * ALIGN
        lags = inverse(np.arange(self.tap_rows) - self.half)
        lags[kernel:] = 0.0
        self.mats = np.concatenate(
            [
                spectrum(np.arange(size)),
                inverse(own + edge - self.half),
                inverse(own + edge + self.half),
                lags,
            ],
            0,
        )
        self.at_conv = size
        self.at_grad = self.at_conv + self.block
        self.at_lags = self.at_grad + self.block
        self.own = spectrum(own + edge)
        taps = np.zeros((size, self.tap_rows))
        taps[:, :kernel] = spectrum(np.arange(kernel)) * (2.0 / size)
        high = taps.astype(jnp.bfloat16)
        low = taps - high.astype(np.float64)
        self.taps = np.concatenate([high.astype(np.float64), high.astype(np.float64), low], 1)
        self.lag_scale = 2.0 / size / math.sqrt(total)


class Owners:
    def __init__(self, n, tiles):
        self.count = max(1, min(n // 2, tiles))
        self.per = -(-tiles // self.count)
        self.first = (n - self.count) // 2


def dot(a, b):
    return jnp.dot(a, b, preferred_element_type=F32)


def sigmoid(x):
    return 0.5 * jnp.tanh(0.5 * x) + 0.5


def body(
    plan, n, tiles, owners, total,
    value_h, gate_h, taps_h, gain_h, shift_h, w_h, go_h, mats_h, own_h, ft_h,
    dv, dg, dt_o, dgs_o,
    value, gate, taps, gain, shift, w, go, mats, own, ft,
    sig_s, gw, conv, gm, gcw, tcat, ts, g_spec, acc1, acc2,
    st1, st1_in, st2, st2_in, inv_s, colg, cols,
    gs, rs_src, rs_in, ag,
    load_sem, w_sem, halo_send, halo_recv, tp_send, tp_recv,
    all_send, all_recv,
):
    sp = lax.axis_index("sp")
    tp = lax.axis_index("tp")
    rows, edge, block = plan.rows, plan.edge, plan.block
    channels = value.shape[1]
    width = channels * 2
    chunks = channels // CHUNK
    size, freqs = plan.size, plan.freqs
    per = owners.per
    nxt = lax.rem(sp + 1, n)
    prv = lax.rem(sp + n - 1, n)
    has_prv = sp > 0
    has_nxt = sp < n - 1
    is_owner = (sp >= owners.first) & (sp < owners.first + owners.count)
    low_side = sp < n // 2

    def peer(d):
        return lax.rem(sp + d, n)

    barrier = pltpu.get_barrier_semaphore()

    pairs = [
        (value_h, value), (gate_h, gate), (taps_h, taps), (ft_h, ft), (own_h, own),
        (mats_h, mats), (go_h, go), (gain_h, gain), (shift_h, shift),
    ]
    loads = [
        pltpu.make_async_copy(a, b, load_sem.at[i]) for i, (a, b) in enumerate(pairs)
    ]
    for load in loads:
        load.start()

    def w_copy(c):
        part = pl.ds(pl.multiple_of(c * CHUNK, CHUNK), CHUNK)
        return pltpu.make_async_copy(w_h.at[part], w.at[part], w_sem.at[c])

    for c in range(chunks):
        w_copy(c).start()

    def greet(d, carry):
        pl.semaphore_signal(
            barrier, 1, device_id=(peer(d), tp), device_id_type=pl.DeviceIdType.MESH
        )
        return carry

    pl.semaphore_signal(
        barrier, 1, device_id=(sp, 1 - tp), device_id_type=pl.DeviceIdType.MESH
    )
    lax.fori_loop(1, n, greet, 0)

    def cut(c):
        return pl.ds(c * CHUNK, CHUNK)

    loads[0].wait()
    loads[1].wait()

    def gate_step(i, carry):
        part = pl.ds(pl.multiple_of(i * ALIGN, ALIGN), ALIGN)
        place = pl.ds(pl.multiple_of(i * ALIGN + edge, ALIGN), ALIGN)
        sig = sigmoid(gate[part].astype(F32))
        sig_s[part] = sig
        gw[place] = (value[part].astype(F32) * sig).astype(BF16)
        return carry

    lax.fori_loop(0, rows // ALIGN, gate_step, 0, unroll=4)

    def remote(src, dst, send, recv, device):
        return pltpu.make_async_remote_copy(
            src_ref=src, dst_ref=dst, send_sem=send, recv_sem=recv,
            device_id=device, device_id_type=pl.DeviceIdType.MESH,
        )

    def halo_pair(ref, k):
        return (
            remote(ref.at[pl.ds(rows, edge)], ref.at[pl.ds(0, edge)],
                   halo_send.at[k], halo_recv.at[k], (nxt, tp)),
            remote(ref.at[pl.ds(edge, edge)], ref.at[pl.ds(rows + edge, edge)],
                   halo_send.at[k + 1], halo_recv.at[k + 1], (prv, tp)),
        )

    def send_halo(pair):
        @pl.when(has_nxt)
        def _():
            pair[0].start()

        @pl.when(has_prv)
        def _():
            pair[1].start()

    def recv_prv(pair, ref):
        @pl.when(has_prv)
        def _():
            pair[0].wait_recv()

        @pl.when(sp == 0)
        def _():
            ref[pl.ds(0, edge)] = jnp.zeros((edge, channels), BF16)

    def recv_nxt(pair, ref):
        @pl.when(has_nxt)
        def _():
            pair[1].wait_recv()

        @pl.when(sp == n - 1)
        def _():
            ref[pl.ds(rows + edge, edge)] = jnp.zeros((edge, channels), BF16)

    def sent_halo(pair):
        @pl.when(has_nxt)
        def _():
            pair[0].wait_send()

        @pl.when(has_prv)
        def _():
            pair[1].wait_send()

    gw_halo = halo_pair(gw, 0)
    gc_halo = halo_pair(gcw, 2)

    pl.semaphore_wait(barrier, n)
    send_halo(gw_halo)

    for load in loads[2:7]:
        load.wait()

    tap = jnp.concatenate(
        [taps[...], jnp.zeros((plan.tap_rows - plan.kernel, channels), F32)], 0
    )
    tap_high = tap.astype(BF16)
    tap_low = (tap - tap_high.astype(F32)).astype(BF16)
    for k, part in enumerate((tap_high, tap_low, tap_high)):
        tcat[pl.ds(k * plan.tap_rows, plan.tap_rows)] = part

    def tap_step(_, carry):
        for c in range(chunks):
            ts[:, cut(c)] = dot(ft[...], tcat[:, cut(c)])
        return carry

    lax.fori_loop(0, 1, tap_step, 0)

    def mix(a, b):
        return lax.dot_general(a, b, (((1,), (1,)), ((), ())), preferred_element_type=F32)

    def mix_step(c, carry):
        part = pl.ds(pl.multiple_of(c * CHUNK, CHUNK), CHUNK)
        w_copy(c).wait()
        gm[:, part] = mix(go[...], w[part])
        return carry

    lax.fori_loop(0, chunks, mix_step, 0)

    def fold(x):
        out = x[:, :LANES]
        for k in range(1, x.shape[1] // LANES):
            out = out + x[:, k * LANES : (k + 1) * LANES]
        return out

    first_lanes = lax.broadcasted_iota(jnp.int32, (block, LANES), 1) < LANES // 2

    def conv_step(b):
        place = pl.ds(b * block, block)
        one = two = None
        for c in range(chunks):
            ta = ts[pl.ds(0, freqs), cut(c)]
            tb = ts[pl.ds(freqs, freqs), cut(c)]
            spec = dot(mats[pl.ds(0, size)], gw[pl.ds(b * block, size), cut(c)])
            g_spec[pl.ds(b * size, size), cut(c)] = spec
            re, im = spec[:freqs], spec[freqs:]
            prod = jnp.concatenate([re * ta + im * tb, re * tb - im * ta], 0).astype(BF16)
            out = dot(mats[pl.ds(plan.at_conv, block)], prod)
            conv[place, cut(c)] = out
            if c == 0:
                acc1[...] = fold(out)
                acc2[...] = fold(out * out)
            else:
                acc1[...] += fold(out)
                acc2[...] += fold(out * out)
        st1[place] = jnp.where(
            first_lanes,
            jnp.sum(acc1[...], 1, keepdims=True),
            jnp.sum(acc2[...], 1, keepdims=True),
        )

    def swap(src, dst, b, k):
        place = pl.ds(b * block, block)
        return remote(
            src.at[place], dst.at[place], tp_send.at[k], tp_recv.at[k], (sp, 1 - tp)
        )

    swap1 = [swap(st1, st1_in, b, b) for b in range(2)]
    swap2 = [swap(st2, st2_in, b, 2 + b) for b in range(2)]

    def conv_at(b):
        def step(_, carry):
            conv_step(b)
            return carry

        lax.fori_loop(0, 1, step, 0)

    recv_prv(gw_halo, gw)
    conv_at(0)
    swap1[0].start()
    recv_nxt(gw_halo, gw)
    conv_at(1)
    swap1[1].start()

    loads[7].wait()
    loads[8].wait()
    colg[...] = jnp.zeros_like(colg)
    cols[...] = jnp.zeros_like(cols)
    lanes = lax.broadcasted_iota(jnp.int32, (ALIGN, LANES), 1) < LANES // 2

    def norm_step(i, carry):
        part = pl.ds(pl.multiple_of(i * ALIGN, ALIGN), ALIGN)
        tot = (st1[part] + st1_in[part]) * (1.0 / width)
        mean = tot[:, :1]
        var = tot[:, LANES // 2 : LANES // 2 + 1] - mean * mean
        inv = lax.rsqrt(var + EPS)
        normed = (conv[part] - mean) * inv
        pre = normed * gain[...] + shift[...]
        sig = sigmoid(pre)
        gp = gm[part] * sig * (1.0 + pre * (1.0 - sig))
        gn = gp * gain[...]
        conv[part] = normed
        gm[part] = gn
        gx = gn * normed
        st2[part] = jnp.where(
            lanes,
            jnp.sum(fold(gn), 1, keepdims=True),
            jnp.sum(fold(gx), 1, keepdims=True),
        )
        inv_s[part] = jnp.broadcast_to(inv, (ALIGN, LANES))
        gpn = gp * normed
        colg[...] += gpn[:8] + gpn[8:]
        cols[...] += gp[:8] + gp[8:]
        return carry

    steps = block // ALIGN

    swap1[0].wait_recv()
    lax.fori_loop(0, steps, norm_step, 0, unroll=4)
    swap2[0].start()
    swap1[1].wait_recv()
    lax.fori_loop(steps, 2 * steps, norm_step, 0, unroll=4)
    swap2[1].start()

    rg = jnp.sum(colg[...], 0, keepdims=True)
    rsh = jnp.sum(cols[...], 0, keepdims=True)
    groups = channels // LANES
    gs[sp] = jnp.concatenate(
        [x[:, k * LANES : (k + 1) * LANES] for x in (rg, rsh) for k in range(groups)], 0
    ).astype(BF16)

    def send_gs(d, carry):
        remote(gs.at[sp], gs.at[sp], all_send.at[0], all_recv.at[0], (peer(d), tp)).start()
        return carry

    lax.fori_loop(1, n, send_gs, 0)

    def gc_step(i, carry):
        part = pl.ds(pl.multiple_of(i * ALIGN, ALIGN), ALIGN)
        place = pl.ds(pl.multiple_of(i * ALIGN + edge, ALIGN), ALIGN)
        tot = (st2[part] + st2_in[part]) * (1.0 / width)
        m1 = tot[:, :1]
        m2 = tot[:, LANES // 2 : LANES // 2 + 1]
        inv = inv_s[part][:, :1]
        gcw[place] = (inv * (gm[part] - m1 - conv[part] * m2)).astype(BF16)
        return carry

    swap2[0].wait_recv()
    lax.fori_loop(0, steps, gc_step, 0, unroll=4)
    swap2[1].wait_recv()
    lax.fori_loop(steps, 2 * steps, gc_step, 0, unroll=4)
    send_halo(gc_halo)

    slots = owners.count * per
    if slots > tiles:
        rs_src[pl.ds(tiles, slots - tiles)] = jnp.zeros((slots - tiles, ALIGN, LANES), BF16)

    def spec_step(_, carry):
        for c in range(chunks):
            dr = di = None
            for b in range(2):
                spec = dot(own[...], gcw[pl.ds(edge + b * block, block), cut(c)])
                re, im = spec[:freqs], spec[freqs:]
                hr = g_spec[pl.ds(b * size, freqs), cut(c)]
                hi = g_spec[pl.ds(b * size + freqs, freqs), cut(c)]
                r, i = hr * re + hi * im, hr * im - hi * re
                dr, di = (r, i) if b == 0 else (dr + r, di + i)
            prod = jnp.concatenate([dr, di], 0).astype(BF16)
            out = dot(mats[pl.ds(plan.at_lags, plan.tap_rows)], prod) * plan.lag_scale
            out = out.astype(BF16)
            for r in range(plan.tap_rows // ALIGN):
                for k in range(CHUNK // LANES):
                    rs_src[r * groups + c * (CHUNK // LANES) + k] = out[
                        r * ALIGN : (r + 1) * ALIGN, k * LANES : (k + 1) * LANES
                    ]
        return carry

    lax.fori_loop(0, 1, spec_step, 0)

    def send_rs(i, carry):
        o = jnp.where(low_side, owners.count - 1 - i, i)
        to = owners.first + o

        @pl.when(to != sp)
        def _():
            remote(rs_src.at[pl.ds(o * per, per)], rs_in.at[sp],
                   all_send.at[1], all_recv.at[1], (to, tp)).start()

        return carry

    lax.fori_loop(0, owners.count, send_rs, 0)

    recv_prv(gc_halo, gcw)
    recv_nxt(gc_halo, gcw)

    def out_step(_, carry):
        for c in range(chunks):
            ta = ts[pl.ds(0, freqs), cut(c)]
            tb = ts[pl.ds(freqs, freqs), cut(c)]
            for b in range(2):
                spec = dot(mats[pl.ds(0, size)], gcw[pl.ds(b * block, size), cut(c)])
                re, im = spec[:freqs], spec[freqs:]
                prod = jnp.concatenate([re * ta - im * tb, -(re * tb + im * ta)], 0).astype(BF16)
                out = dot(mats[pl.ds(plan.at_grad, block)], prod)
                place = pl.ds(b * block, block)
                sig = sig_s[place, cut(c)]
                left = out * sig
                dv[place, cut(c)] = left.astype(BF16)
                dg[place, cut(c)] = (
                    left * value[place, cut(c)].astype(F32) * (1.0 - sig)
                ).astype(BF16)
        return carry

    def settle(ref, count, sem):
        if count:
            part = ref.at[pl.ds(0, count)]
            pltpu.make_async_copy(part, part, sem).wait()

    lax.fori_loop(0, 1, out_step, 0)

    @pl.when(is_owner)
    def _():
        o = sp - owners.first
        rs_in[sp] = rs_src[pl.ds(o * per, per)]
        settle(rs_in, n - 1, all_recv.at[1])
        zero = jnp.zeros((per, ALIGN, LANES), F32)
        summed = lax.fori_loop(0, n, lambda i, t: t + rs_in[i].astype(F32), zero)
        ag[o] = summed.astype(BF16)

        def send_ag(i, carry):
            to = jnp.where(low_side, n - 1 - i, i)

            @pl.when(to != sp)
            def _():
                remote(ag.at[o], ag.at[o], all_send.at[2], all_recv.at[2], (to, tp)).start()

            return carry

        lax.fori_loop(0, n, send_ag, 0)

    settle(gs, n - 1, all_recv.at[0])
    small = lax.fori_loop(
        0, n, lambda i, t: t + gs[i].astype(F32), jnp.zeros(gs.shape[1:], F32)
    )
    dgs_o[...] = small * (1.0 / math.sqrt(total))

    sent_halo(gw_halo)
    sent_halo(gc_halo)
    for k in range(2):
        swap1[k].wait_send()
        swap2[k].wait_send()
    settle(gs, n - 1, all_send.at[0])

    @pl.when(is_owner)
    def _():
        settle(rs_in, owners.count - 1, all_send.at[1])
        settle(ag, owners.count - 1, all_recv.at[2])

    @pl.when(jnp.logical_not(is_owner))
    def _():
        settle(rs_in, owners.count, all_send.at[1])
        settle(ag, owners.count, all_recv.at[2])

    for t in range(tiles):
        r, k = t // groups, t % groups
        count = min(ALIGN, plan.kernel - r * ALIGN)
        dt_o[pl.ds(r * ALIGN, count), pl.ds(k * LANES, LANES)] = ag[t // per, t % per].astype(F32)[
            :count
        ]

    @pl.when(is_owner)
    def _():
        def sent(i, carry):
            pltpu.make_async_copy(ag.at[0], ag.at[0], all_send.at[2]).wait()
            return carry

        lax.fori_loop(0, n - 1, sent, 0)


def store(*refs):
    sources, targets, out_sem = refs[:4], refs[4:9], refs[9]
    groups = sources[3].shape[0] // 2
    views = list(sources[:3]) + [
        sources[3].at[pl.ds(0, groups)], sources[3].at[pl.ds(groups, groups)]
    ]
    copies = [
        pltpu.make_async_copy(a, b, out_sem.at[i]) for i, (a, b) in enumerate(zip(views, targets))
    ]
    for copy in copies:
        copy.start()
    for copy in copies:
        copy.wait()


def shards(n, value_in, gate_in, taps, gain, shift, w_out, grad_out):
    rows, channels = value_in.shape
    kernel = taps.shape[0]
    total = rows * n
    plan = Plan(rows, kernel, total)
    groups = channels // LANES
    tiles = plan.tap_rows // ALIGN * groups
    owners = Owners(n, tiles)
    per = owners.per
    model = grad_out.shape[1]
    mats = jnp.asarray(plan.mats, BF16)
    own = jnp.asarray(plan.own, BF16)
    ft = jnp.asarray(plan.taps, BF16)
    hbm = pl.BlockSpec(memory_space=pltpu.HBM)
    vmem = pl.BlockSpec(memory_space=pltpu.VMEM)
    size, block = plan.size, plan.block
    chunks = channels // CHUNK
    dma = pltpu.SemaphoreType.DMA
    results = pl.pallas_call(
        functools.partial(body, plan, n, tiles, owners, total),
        out_shape=(
            pltpu.VMEM((rows, channels), BF16),
            pltpu.VMEM((rows, channels), BF16),
            pltpu.VMEM((kernel, channels), F32),
            pltpu.VMEM((2 * groups, LANES), F32),
        ),
        in_specs=[hbm] * 10,
        out_specs=(vmem,) * 4,
        scratch_shapes=[
            pltpu.VMEM((rows, channels), BF16),
            pltpu.VMEM((rows, channels), BF16),
            pltpu.VMEM((kernel, channels), F32),
            pltpu.VMEM((1, channels), F32),
            pltpu.VMEM((1, channels), F32),
            pltpu.VMEM((channels, model), BF16),
            pltpu.VMEM((rows, model), BF16),
            pltpu.VMEM(plan.mats.shape, BF16),
            pltpu.VMEM(plan.own.shape, BF16),
            pltpu.VMEM(plan.taps.shape, BF16),
            pltpu.VMEM((rows, channels), F32),
            pltpu.VMEM((plan.wide, channels), BF16),
            pltpu.VMEM((rows, channels), F32),
            pltpu.VMEM((rows, channels), F32),
            pltpu.VMEM((plan.wide, channels), BF16),
            pltpu.VMEM((3 * plan.tap_rows, channels), BF16),
            pltpu.VMEM((size, channels), F32),
            pltpu.VMEM((2 * size, channels), F32),
            pltpu.VMEM((block, LANES), F32),
            pltpu.VMEM((block, LANES), F32),
            pltpu.VMEM((rows, LANES), F32),
            pltpu.VMEM((rows, LANES), F32),
            pltpu.VMEM((rows, LANES), F32),
            pltpu.VMEM((rows, LANES), F32),
            pltpu.VMEM((rows, LANES), F32),
            pltpu.VMEM((8, channels), F32),
            pltpu.VMEM((8, channels), F32),
            pltpu.VMEM((n, 2 * groups, LANES), BF16),
            pltpu.VMEM((owners.count * per, ALIGN, LANES), BF16),
            pltpu.VMEM((n, per, ALIGN, LANES), BF16),
            pltpu.VMEM((owners.count, per, ALIGN, LANES), BF16),
            dma((9,)), dma((chunks,)), dma((4,)), dma((4,)),
            dma((4,)), dma((4,)), dma((3,)), dma((3,)),
        ],
        compiler_params=pltpu.CompilerParams(
            collective_id=0, has_side_effects=True, vmem_limit_bytes=VMEM_GRANT
        ),
    )(
        *(
            pltpu.with_memory_space_constraint(x, pltpu.HBM)
            for x in (
                value_in, gate_in, taps, gain.reshape(1, -1), shift.reshape(1, -1), w_out,
                grad_out, mats, own, ft,
            )
        )
    )
    results = [pltpu.with_memory_space_constraint(x, pltpu.VMEM) for x in results]
    d_value, d_gate, d_taps, d_gain, d_shift = pl.pallas_call(
        store,
        out_shape=(
            jax.ShapeDtypeStruct((rows, channels), BF16),
            jax.ShapeDtypeStruct((rows, channels), BF16),
            jax.ShapeDtypeStruct((kernel, channels), F32),
            jax.ShapeDtypeStruct((groups, LANES), F32),
            jax.ShapeDtypeStruct((groups, LANES), F32),
        ),
        in_specs=[vmem] * 4,
        out_specs=(hbm,) * 5,
        scratch_shapes=[dma((5,))],
        compiler_params=pltpu.CompilerParams(vmem_limit_bytes=8 * 1024 * 1024),
    )(*results)
    return (d_value, d_gate, d_taps, d_gain.reshape(-1), d_shift.reshape(-1))


def solution(mesh):
    return jax.shard_map(
        functools.partial(shards, mesh.shape["sp"]),
        mesh=mesh,
        in_specs=(
            P("sp", "tp"),
            P("sp", "tp"),
            P(None, "tp"),
            P("tp"),
            P("tp"),
            P("tp", None),
            P("sp", None),
        ),
        out_specs=(P("sp", "tp"), P("sp", "tp"), P(None, "tp"), P("tp"), P("tp")),
        check_vma=False,
    )
```

```python
import functools
import math

import jax
import jax.numpy as jnp
import numpy as np
from jax import lax
from jax.experimental import pallas as pl
from jax.experimental.pallas import tpu as pltpu
from jax.sharding import PartitionSpec as P

EPS = 1e-05
ALIGN = 16
LANES = 128
CHUNK = 256
VMEM_GRANT = 48 * 1024 * 1024
F32 = jnp.float32
BF16 = jnp.bfloat16


class Plan:
    def __init__(self, rows, kernel, total):
        self.half = kernel // 2
        self.kernel = kernel
        self.rows = rows
        self.edge = -(-self.half // ALIGN) * ALIGN
        edge = self.edge
        self.block = rows // 2
        self.size = self.block + 2 * edge
        size = self.size
        self.freqs = size // 2
        self.wide = rows + 2 * edge
        omega = 2.0 * np.pi * (np.arange(self.freqs) + 0.5) / size

        def spectrum(times):
            angle = omega[:, None] * times[None, :]
            return np.concatenate([np.cos(angle), np.sin(angle)], 0)

        def inverse(times):
            angle = times[:, None] * omega[None, :]
            return np.concatenate([np.cos(angle), -np.sin(angle)], 1)

        own = np.arange(self.block)
        self.tap_rows = -(-kernel // ALIGN) * ALIGN
        lags = inverse(np.arange(self.tap_rows) - self.half)
        lags[kernel:] = 0.0
        self.mats = np.concatenate(
            [
                spectrum(np.arange(size)),
                inverse(own + edge - self.half),
                inverse(own + edge + self.half),
                lags,
            ],
            0,
        )
        self.at_conv = size
        self.at_grad = self.at_conv + self.block
        self.at_lags = self.at_grad + self.block
        self.own = spectrum(own + edge)
        taps = np.zeros((size, self.tap_rows))
        taps[:, :kernel] = spectrum(np.arange(kernel)) * (2.0 / size)
        high = taps.astype(jnp.bfloat16)
        low = taps - high.astype(np.float64)
        self.taps = np.concatenate([high.astype(np.float64), high.astype(np.float64), low], 1)
        self.lag_scale = 2.0 / size / math.sqrt(total)


class Owners:
    def __init__(self, n, tiles):
        self.count = max(1, min(n // 2, tiles))
        self.per = -(-tiles // self.count)
        self.first = (n - self.count) // 2


def dot(a, b):
    return jnp.dot(a, b, preferred_element_type=F32)


def sigmoid(x):
    return 0.5 * jnp.tanh(0.5 * x) + 0.5


def body(
    plan, n, tiles, owners, total,
    value_h, gate_h, taps_h, gain_h, shift_h, w_h, go_h, mats_h, own_h, ft_h,
    dv, dg, dt_o, dgs_o,
    value, gate, taps, gain, shift, w, go, mats, own, ft,
    sig_s, gw, conv, gm, gcw, tcat, ts, g_spec, dsp, acc1, acc2,
    st1, st1_in, st2, st2_in, inv_s, colg, cols,
    gs, rs_src, rs_in, ag,
    meet, load_sem, w_sem, halo_send, halo_recv, tp_send, tp_recv,
    all_send, all_recv,
):
    sp = lax.axis_index("sp")
    tp = lax.axis_index("tp")
    rows, edge, block = plan.rows, plan.edge, plan.block
    channels = value.shape[1]
    width = channels * 2
    chunks = channels // CHUNK
    size, freqs = plan.size, plan.freqs
    per = owners.per
    nxt = lax.rem(sp + 1, n)
    prv = lax.rem(sp + n - 1, n)
    has_prv = sp > 0
    has_nxt = sp < n - 1
    is_owner = (sp >= owners.first) & (sp < owners.first + owners.count)
    low_side = sp < n // 2
    crew = 1 << (max(n, 1).bit_length() // 2)
    crews = -(-n // crew)
    head = sp - lax.rem(sp, crew)
    is_head = (sp == head) & (tp == 1)

    def peer(d):
        return lax.rem(sp + d, n)

    barrier = pltpu.get_barrier_semaphore()

    pairs = [
        (value_h, value), (gate_h, gate), (taps_h, taps), (ft_h, ft), (own_h, own),
        (mats_h, mats), (go_h, go), (gain_h, gain), (shift_h, shift),
    ]
    loads = [
        pltpu.make_async_copy(a, b, load_sem.at[i]) for i, (a, b) in enumerate(pairs)
    ]
    for load in loads:
        load.start()

    def w_copy(c):
        part = pl.ds(pl.multiple_of(c * CHUNK, CHUNK), CHUNK)
        return pltpu.make_async_copy(w_h.at[part], w.at[part], w_sem.at[c])

    for c in range(chunks):
        w_copy(c).start()

    def tell(sem, s, t):
        pl.semaphore_signal(sem, 1, device_id=(s, t), device_id_type=pl.DeviceIdType.MESH)

    members = 2 * jnp.minimum(crew, n - head)

    def each_member(sem):
        def step(i, carry):
            s, t = head + i // 2, lax.rem(i, 2)

            @pl.when((s != sp) | (t != tp))
            def _():
                tell(sem, s, t)

            return carry

        lax.fori_loop(0, members, step, 0)

    def each_head(sem):
        def step(i, carry):
            @pl.when(i * crew != sp)
            def _():
                tell(sem, i * crew, 1)

            return carry

        lax.fori_loop(0, crews, step, 0)

    tell(barrier, sp, 1 - tp)

    @pl.when(has_prv)
    def _():
        tell(barrier, prv, tp)

    @pl.when(has_nxt)
    def _():
        tell(barrier, nxt, tp)

    @pl.when(is_head)
    def _():
        each_member(barrier)
        each_head(barrier)

    greeted = (
        1 + has_prv.astype(jnp.int32) + has_nxt.astype(jnp.int32)
        + jnp.where(is_head, crews - 1, 1)
    )

    def handshake_up():
        @pl.when(jnp.logical_not(is_head))
        def _():
            tell(meet.at[0], head, 1)

    def handshake_across():
        @pl.when(is_head)
        def _():
            pl.semaphore_wait(meet.at[0], members - 1)
            each_head(meet.at[1])

    def handshake_down():
        @pl.when(is_head)
        def _():
            if crews > 1:
                pl.semaphore_wait(meet.at[1], crews - 1)
            each_member(meet.at[2])

    def handshake_done():
        @pl.when(jnp.logical_not(is_head))
        def _():
            pl.semaphore_wait(meet.at[2], 1)

    def cut(c):
        return pl.ds(c * CHUNK, CHUNK)

    loads[0].wait()
    loads[1].wait()

    def gate_step(i, carry):
        part = pl.ds(pl.multiple_of(i * ALIGN, ALIGN), ALIGN)
        place = pl.ds(pl.multiple_of(i * ALIGN + edge, ALIGN), ALIGN)
        sig = sigmoid(gate[part].astype(F32))
        sig_s[part] = sig
        gw[place] = (value[part].astype(F32) * sig).astype(BF16)
        return carry

    lax.fori_loop(0, rows // ALIGN, gate_step, 0, unroll=4)

    def remote(src, dst, send, recv, device):
        return pltpu.make_async_remote_copy(
            src_ref=src, dst_ref=dst, send_sem=send, recv_sem=recv,
            device_id=device, device_id_type=pl.DeviceIdType.MESH,
        )

    def halo_pair(ref, k):
        return (
            remote(ref.at[pl.ds(rows, edge)], ref.at[pl.ds(0, edge)],
                   halo_send.at[k], halo_recv.at[k], (nxt, tp)),
            remote(ref.at[pl.ds(edge, edge)], ref.at[pl.ds(rows + edge, edge)],
                   halo_send.at[k + 1], halo_recv.at[k + 1], (prv, tp)),
        )

    def send_halo(pair):
        @pl.when(has_nxt)
        def _():
            pair[0].start()

        @pl.when(has_prv)
        def _():
            pair[1].start()

    def recv_prv(pair, ref):
        @pl.when(has_prv)
        def _():
            pair[0].wait_recv()

        @pl.when(sp == 0)
        def _():
            ref[pl.ds(0, edge)] = jnp.zeros((edge, channels), BF16)

    def recv_nxt(pair, ref):
        @pl.when(has_nxt)
        def _():
            pair[1].wait_recv()

        @pl.when(sp == n - 1)
        def _():
            ref[pl.ds(rows + edge, edge)] = jnp.zeros((edge, channels), BF16)

    def sent_halo(pair):
        @pl.when(has_nxt)
        def _():
            pair[0].wait_send()

        @pl.when(has_prv)
        def _():
            pair[1].wait_send()

    def settle(ref, count, sem):
        if count:
            part = ref.at[pl.ds(0, count)]
            pltpu.make_async_copy(part, part, sem).wait()

    gw_halo = halo_pair(gw, 0)
    gc_halo = halo_pair(gcw, 2)

    pl.semaphore_wait(barrier, greeted)
    send_halo(gw_halo)
    handshake_up()

    for load in loads[2:7]:
        load.wait()

    tap = jnp.concatenate(
        [taps[...], jnp.zeros((plan.tap_rows - plan.kernel, channels), F32)], 0
    )
    tap_high = tap.astype(BF16)
    tap_low = (tap - tap_high.astype(F32)).astype(BF16)
    for k, part in enumerate((tap_high, tap_low, tap_high)):
        tcat[pl.ds(k * plan.tap_rows, plan.tap_rows)] = part

    def tap_step(_, carry):
        for c in range(chunks):
            ts[:, cut(c)] = dot(ft[...], tcat[:, cut(c)])
        return carry

    lax.fori_loop(0, 1, tap_step, 0)

    def mix(a, b):
        return lax.dot_general(a, b, (((1,), (1,)), ((), ())), preferred_element_type=F32)

    def mix_step(c, carry):
        part = pl.ds(pl.multiple_of(c * CHUNK, CHUNK), CHUNK)
        w_copy(c).wait()
        gm[:, part] = mix(go[...], w[part])
        return carry

    early = chunks - chunks // 4
    lax.fori_loop(0, early, mix_step, 0)
    handshake_across()

    def fold(x):
        out = x[:, :LANES]
        for k in range(1, x.shape[1] // LANES):
            out = out + x[:, k * LANES : (k + 1) * LANES]
        return out

    first_lanes = lax.broadcasted_iota(jnp.int32, (block, LANES), 1) < LANES // 2

    def conv_step(b):
        place = pl.ds(b * block, block)
        one = two = None
        for c in range(chunks):
            ta = ts[pl.ds(0, freqs), cut(c)]
            tb = ts[pl.ds(freqs, freqs), cut(c)]
            spec = dot(mats[pl.ds(0, size)], gw[pl.ds(b * block, size), cut(c)])
            g_spec[pl.ds(b * size, size), cut(c)] = spec
            re, im = spec[:freqs], spec[freqs:]
            prod = jnp.concatenate([re * ta + im * tb, re * tb - im * ta], 0).astype(BF16)
            out = dot(mats[pl.ds(plan.at_conv, block)], prod)
            conv[place, cut(c)] = out
            if c == 0:
                acc1[...] = fold(out)
                acc2[...] = fold(out * out)
            else:
                acc1[...] += fold(out)
                acc2[...] += fold(out * out)
        st1[place] = jnp.where(
            first_lanes,
            jnp.sum(acc1[...], 1, keepdims=True),
            jnp.sum(acc2[...], 1, keepdims=True),
        )

    def swap(src, dst, b, k):
        place = pl.ds(b * block, block)
        return remote(
            src.at[place], dst.at[place], tp_send.at[k], tp_recv.at[k], (sp, 1 - tp)
        )

    swap1 = [swap(st1, st1_in, b, b) for b in range(2)]
    swap2 = [swap(st2, st2_in, b, 2 + b) for b in range(2)]

    def conv_at(b):
        def step(_, carry):
            conv_step(b)
            return carry

        lax.fori_loop(0, 1, step, 0)

    recv_prv(gw_halo, gw)
    conv_at(0)
    swap1[0].start()
    recv_nxt(gw_halo, gw)
    conv_at(1)
    swap1[1].start()
    handshake_down()
    lax.fori_loop(early, chunks, mix_step, 0)

    loads[7].wait()
    loads[8].wait()
    colg[...] = jnp.zeros_like(colg)
    cols[...] = jnp.zeros_like(cols)
    lanes = lax.broadcasted_iota(jnp.int32, (ALIGN, LANES), 1) < LANES // 2

    def norm_step(i, carry):
        part = pl.ds(pl.multiple_of(i * ALIGN, ALIGN), ALIGN)
        tot = (st1[part] + st1_in[part]) * (1.0 / width)
        mean = tot[:, :1]
        var = tot[:, LANES // 2 : LANES // 2 + 1] - mean * mean
        inv = lax.rsqrt(var + EPS)
        normed = (conv[part] - mean) * inv
        pre = normed * gain[...] + shift[...]
        sig = sigmoid(pre)
        gp = gm[part] * sig * (1.0 + pre * (1.0 - sig))
        gn = gp * gain[...]
        conv[part] = normed
        gm[part] = gn
        gx = gn * normed
        st2[part] = jnp.where(
            lanes,
            jnp.sum(fold(gn), 1, keepdims=True),
            jnp.sum(fold(gx), 1, keepdims=True),
        )
        inv_s[part] = jnp.broadcast_to(inv, (ALIGN, LANES))
        gpn = gp * normed
        colg[...] += gpn[:8] + gpn[8:]
        cols[...] += gp[:8] + gp[8:]
        return carry

    steps = block // ALIGN

    swap1[0].wait_recv()
    lax.fori_loop(0, steps, norm_step, 0, unroll=4)
    swap2[0].start()
    swap1[1].wait_recv()
    lax.fori_loop(steps, 2 * steps, norm_step, 0, unroll=4)
    swap2[1].start()

    rg = jnp.sum(colg[...], 0, keepdims=True)
    rsh = jnp.sum(cols[...], 0, keepdims=True)
    groups = channels // LANES
    gs[sp] = jnp.concatenate(
        [x[:, k * LANES : (k + 1) * LANES] for x in (rg, rsh) for k in range(groups)], 0
    ).astype(BF16)

    def send_gs(d, carry):
        remote(gs.at[sp], gs.at[sp], all_send.at[0], all_recv.at[0], (peer(d), tp)).start()
        return carry

    handshake_done()
    lax.fori_loop(1, n, send_gs, 0)

    def gc_step(i, carry):
        part = pl.ds(pl.multiple_of(i * ALIGN, ALIGN), ALIGN)
        place = pl.ds(pl.multiple_of(i * ALIGN + edge, ALIGN), ALIGN)
        tot = (st2[part] + st2_in[part]) * (1.0 / width)
        m1 = tot[:, :1]
        m2 = tot[:, LANES // 2 : LANES // 2 + 1]
        inv = inv_s[part][:, :1]
        gcw[place] = (inv * (gm[part] - m1 - conv[part] * m2)).astype(BF16)
        return carry

    slots = owners.count * per
    if slots > tiles:
        rs_src[pl.ds(tiles, slots - tiles)] = jnp.zeros((slots - tiles, ALIGN, LANES), BF16)
    tall = plan.tap_rows // ALIGN
    ready = tall * (CHUNK // LANES)

    def lag_part(b, c):
        spec = dot(own[...], gcw[pl.ds(edge + b * block, block), cut(c)])
        re, im = spec[:freqs], spec[freqs:]
        hr = g_spec[pl.ds(b * size, freqs), cut(c)]
        hi = g_spec[pl.ds(b * size + freqs, freqs), cut(c)]
        return hr * re + hi * im, hr * im - hi * re

    def send_rs(o):
        to = owners.first + o

        @pl.when(to != sp)
        def _():
            remote(rs_src.at[pl.ds(o * per, per)], rs_in.at[sp],
                   all_send.at[1], all_recv.at[1], (to, tp)).start()

    def spec_first(_, carry):
        for c in range(chunks):
            dr, di = lag_part(0, c)
            dsp[pl.ds(0, freqs), cut(c)] = dr
            dsp[pl.ds(freqs, freqs), cut(c)] = di
        return carry

    def spec_last(c):
        dr, di = lag_part(1, c)
        dr = dr + dsp[pl.ds(0, freqs), cut(c)]
        di = di + dsp[pl.ds(freqs, freqs), cut(c)]
        prod = jnp.concatenate([dr, di], 0).astype(BF16)
        out = dot(mats[pl.ds(plan.at_lags, plan.tap_rows)], prod) * plan.lag_scale
        out = out.astype(BF16)
        for r in range(tall):
            for k in range(CHUNK // LANES):
                rs_src[(c * (CHUNK // LANES) + k) * tall + r] = out[
                    r * ALIGN : (r + 1) * ALIGN, k * LANES : (k + 1) * LANES
                ]

    swap2[0].wait_recv()
    lax.fori_loop(0, steps, gc_step, 0, unroll=4)
    lax.fori_loop(0, 1, spec_first, 0)
    swap2[1].wait_recv()
    lax.fori_loop(steps, 2 * steps, gc_step, 0, unroll=4)

    def spec_phase(c0, count):
        for c in range(c0, c0 + count):
            spec_last(c)
        for o in range(owners.count):
            last = (min((o + 1) * per, tiles) - 1) // ready
            if c0 <= last < c0 + count:
                send_rs(o)

    group = 2 if chunks % 2 == 0 else 1
    for c0 in range(0, chunks, group):
        spec_phase(c0, group)
    send_halo(gc_halo)

    @pl.when(is_owner)
    def _():
        o = sp - owners.first
        rs_in[sp] = rs_src[pl.ds(o * per, per)]
        settle(rs_in, n - 1, all_recv.at[1])
        zero = jnp.zeros((per, ALIGN, LANES), F32)
        summed = lax.fori_loop(0, n, lambda i, t: t + rs_in[i].astype(F32), zero)
        ag[o] = summed.astype(BF16)

        def send_ag(i, carry):
            to = jnp.where(low_side, n - 1 - i, i)

            @pl.when(to != sp)
            def _():
                remote(ag.at[o], ag.at[o], all_send.at[2], all_recv.at[2], (to, tp)).start()

            return carry

        lax.fori_loop(0, n, send_ag, 0)

    recv_prv(gc_halo, gcw)
    recv_nxt(gc_halo, gcw)

    def out_step(_, carry):
        for c in range(chunks):
            ta = ts[pl.ds(0, freqs), cut(c)]
            tb = ts[pl.ds(freqs, freqs), cut(c)]
            for b in range(2):
                spec = dot(mats[pl.ds(0, size)], gcw[pl.ds(b * block, size), cut(c)])
                re, im = spec[:freqs], spec[freqs:]
                prod = jnp.concatenate([re * ta - im * tb, -(re * tb + im * ta)], 0).astype(BF16)
                out = dot(mats[pl.ds(plan.at_grad, block)], prod)
                place = pl.ds(b * block, block)
                sig = sig_s[place, cut(c)]
                left = out * sig
                dv[place, cut(c)] = left.astype(BF16)
                dg[place, cut(c)] = (
                    left * value[place, cut(c)].astype(F32) * (1.0 - sig)
                ).astype(BF16)
        return carry

    lax.fori_loop(0, 1, out_step, 0)

    settle(gs, n - 1, all_recv.at[0])
    small = lax.fori_loop(
        0, n, lambda i, t: t + gs[i].astype(F32), jnp.zeros(gs.shape[1:], F32)
    )
    dgs_o[...] = small * (1.0 / math.sqrt(total))

    sent_halo(gw_halo)
    sent_halo(gc_halo)
    for k in range(2):
        swap1[k].wait_send()
        swap2[k].wait_send()
    settle(gs, n - 1, all_send.at[0])

    @pl.when(is_owner)
    def _():
        settle(rs_in, owners.count - 1, all_send.at[1])
        settle(ag, owners.count - 1, all_recv.at[2])

    @pl.when(jnp.logical_not(is_owner))
    def _():
        settle(rs_in, owners.count, all_send.at[1])
        settle(ag, owners.count, all_recv.at[2])

    for t in range(tiles):
        k, r = t // tall, t % tall
        count = min(ALIGN, plan.kernel - r * ALIGN)
        dt_o[pl.ds(r * ALIGN, count), pl.ds(k * LANES, LANES)] = ag[t // per, t % per].astype(F32)[
            :count
        ]

    @pl.when(is_owner)
    def _():
        def sent(i, carry):
            pltpu.make_async_copy(ag.at[0], ag.at[0], all_send.at[2]).wait()
            return carry

        lax.fori_loop(0, n - 1, sent, 0)


def store(*refs):
    sources, targets, out_sem = refs[:4], refs[4:9], refs[9]
    groups = sources[3].shape[0] // 2
    views = list(sources[:3]) + [
        sources[3].at[pl.ds(0, groups)], sources[3].at[pl.ds(groups, groups)]
    ]
    copies = [
        pltpu.make_async_copy(a, b, out_sem.at[i]) for i, (a, b) in enumerate(zip(views, targets))
    ]
    for copy in copies:
        copy.start()
    for copy in copies:
        copy.wait()


def shards(n, value_in, gate_in, taps, gain, shift, w_out, grad_out):
    rows, channels = value_in.shape
    kernel = taps.shape[0]
    total = rows * n
    plan = Plan(rows, kernel, total)
    groups = channels // LANES
    tiles = plan.tap_rows // ALIGN * groups
    owners = Owners(n, tiles)
    per = owners.per
    model = grad_out.shape[1]
    mats = jnp.asarray(plan.mats, BF16)
    own = jnp.asarray(plan.own, BF16)
    ft = jnp.asarray(plan.taps, BF16)
    hbm = pl.BlockSpec(memory_space=pltpu.HBM)
    vmem = pl.BlockSpec(memory_space=pltpu.VMEM)
    size, block = plan.size, plan.block
    chunks = channels // CHUNK
    dma = pltpu.SemaphoreType.DMA
    results = pl.pallas_call(
        functools.partial(body, plan, n, tiles, owners, total),
        out_shape=(
            pltpu.VMEM((rows, channels), BF16),
            pltpu.VMEM((rows, channels), BF16),
            pltpu.VMEM((kernel, channels), F32),
            pltpu.VMEM((2 * groups, LANES), F32),
        ),
        in_specs=[hbm] * 10,
        out_specs=(vmem,) * 4,
        scratch_shapes=[
            pltpu.VMEM((rows, channels), BF16),
            pltpu.VMEM((rows, channels), BF16),
            pltpu.VMEM((kernel, channels), F32),
            pltpu.VMEM((1, channels), F32),
            pltpu.VMEM((1, channels), F32),
            pltpu.VMEM((channels, model), BF16),
            pltpu.VMEM((rows, model), BF16),
            pltpu.VMEM(plan.mats.shape, BF16),
            pltpu.VMEM(plan.own.shape, BF16),
            pltpu.VMEM(plan.taps.shape, BF16),
            pltpu.VMEM((rows, channels), F32),
            pltpu.VMEM((plan.wide, channels), BF16),
            pltpu.VMEM((rows, channels), F32),
            pltpu.VMEM((rows, channels), F32),
            pltpu.VMEM((plan.wide, channels), BF16),
            pltpu.VMEM((3 * plan.tap_rows, channels), BF16),
            pltpu.VMEM((size, channels), F32),
            pltpu.VMEM((2 * size, channels), F32),
            pltpu.VMEM((size, channels), F32),
            pltpu.VMEM((block, LANES), F32),
            pltpu.VMEM((block, LANES), F32),
            pltpu.VMEM((rows, LANES), F32),
            pltpu.VMEM((rows, LANES), F32),
            pltpu.VMEM((rows, LANES), F32),
            pltpu.VMEM((rows, LANES), F32),
            pltpu.VMEM((rows, LANES), F32),
            pltpu.VMEM((8, channels), F32),
            pltpu.VMEM((8, channels), F32),
            pltpu.VMEM((n, 2 * groups, LANES), BF16),
            pltpu.VMEM((owners.count * per, ALIGN, LANES), BF16),
            pltpu.VMEM((n, per, ALIGN, LANES), BF16),
            pltpu.VMEM((owners.count, per, ALIGN, LANES), BF16),
            pltpu.SemaphoreType.REGULAR((3,)),
            dma((9,)), dma((chunks,)), dma((4,)), dma((4,)),
            dma((4,)), dma((4,)), dma((3,)), dma((3,)),
        ],
        compiler_params=pltpu.CompilerParams(
            collective_id=0, has_side_effects=True, vmem_limit_bytes=VMEM_GRANT
        ),
    )(
        *(
            pltpu.with_memory_space_constraint(x, pltpu.HBM)
            for x in (
                value_in, gate_in, taps, gain.reshape(1, -1), shift.reshape(1, -1), w_out,
                grad_out, mats, own, ft,
            )
        )
    )
    results = [pltpu.with_memory_space_constraint(x, pltpu.VMEM) for x in results]
    d_value, d_gate, d_taps, d_gain, d_shift = pl.pallas_call(
        store,
        out_shape=(
            jax.ShapeDtypeStruct((rows, channels), BF16),
            jax.ShapeDtypeStruct((rows, channels), BF16),
            jax.ShapeDtypeStruct((kernel, channels), F32),
            jax.ShapeDtypeStruct((groups, LANES), F32),
            jax.ShapeDtypeStruct((groups, LANES), F32),
        ),
        in_specs=[vmem] * 4,
        out_specs=(hbm,) * 5,
        scratch_shapes=[dma((5,))],
        compiler_params=pltpu.CompilerParams(vmem_limit_bytes=8 * 1024 * 1024),
    )(*results)
    return (d_value, d_gate, d_taps, d_gain.reshape(-1), d_shift.reshape(-1))


def solution(mesh):
    return jax.shard_map(
        functools.partial(shards, mesh.shape["sp"]),
        mesh=mesh,
        in_specs=(
            P("sp", "tp"),
            P("sp", "tp"),
            P(None, "tp"),
            P("tp"),
            P("tp"),
            P("tp", None),
            P("sp", None),
        ),
        out_specs=(P("sp", "tp"), P("sp", "tp"), P(None, "tp"), P("tp"), P("tp")),
        check_vma=False,
    )
```

```python
import functools
import math

import jax
import jax.numpy as jnp
import numpy as np
from jax import lax
from jax.experimental import pallas as pl
from jax.experimental.pallas import tpu as pltpu
from jax.sharding import PartitionSpec as P

EPS = 1e-05
ALIGN = 16
LANES = 128
CHUNK = 256
VMEM_GRANT = 48 * 1024 * 1024
F32 = jnp.float32
BF16 = jnp.bfloat16


class Plan:
    def __init__(self, rows, kernel, total):
        self.half = kernel // 2
        self.kernel = kernel
        self.rows = rows
        self.edge = -(-self.half // ALIGN) * ALIGN
        edge = self.edge
        self.block = rows // 2
        self.size = self.block + 2 * edge
        size = self.size
        self.freqs = size // 2
        self.wide = rows + 2 * edge
        omega = 2.0 * np.pi * (np.arange(self.freqs) + 0.5) / size

        def spectrum(times):
            angle = omega[:, None] * times[None, :]
            return np.concatenate([np.cos(angle), np.sin(angle)], 0)

        def inverse(times):
            angle = times[:, None] * omega[None, :]
            return np.concatenate([np.cos(angle), -np.sin(angle)], 1)

        own = np.arange(self.block)
        self.tap_rows = -(-kernel // ALIGN) * ALIGN
        lags = inverse(np.arange(self.tap_rows) - self.half)
        lags[kernel:] = 0.0
        self.mats = np.concatenate(
            [
                spectrum(np.arange(size)),
                inverse(own + edge - self.half),
                inverse(own + edge + self.half),
                lags,
            ],
            0,
        )
        self.at_conv = size
        self.at_grad = self.at_conv + self.block
        self.at_lags = self.at_grad + self.block
        self.own = spectrum(own + edge)
        taps = np.zeros((size, self.tap_rows))
        taps[:, :kernel] = spectrum(np.arange(kernel)) * (2.0 / size)
        high = taps.astype(jnp.bfloat16)
        low = taps - high.astype(np.float64)
        self.taps = np.concatenate([high.astype(np.float64), high.astype(np.float64), low], 1)
        self.lag_scale = 2.0 / size / math.sqrt(total)


class Owners:
    def __init__(self, n, tiles):
        self.count = max(1, min(n // 2, tiles))
        self.per = -(-tiles // self.count)
        self.first = (n - self.count) // 2


def dot(a, b):
    return jnp.dot(a, b, preferred_element_type=F32)


def sigmoid(x):
    return 0.5 * jnp.tanh(0.5 * x) + 0.5


def body(
    plan, n, tiles, owners, total,
    value_h, gate_h, taps_h, gain_h, shift_h, w_h, go_h, mats_h, own_h, ft_h,
    dv, dg, dt_o, dgs_o,
    value, gate, taps, w, go, mats,
    sig_s, gw, conv, gm, gcw, tcat, ts, g_spec, spec_s, dsp, prod,
    st1, st1_in, st2, st2_in, inv_s, colg, cols, hgain, hshift,
    gs, rs_src, rs_in, ag, own, ft, gain, shift,
    meet, load_sem, w_sem, halo_send, halo_recv, tp_send, tp_recv,
    all_send, all_recv,
):
    sp = lax.axis_index("sp")
    tp = lax.axis_index("tp")
    rows, edge, block = plan.rows, plan.edge, plan.block
    channels = value.shape[1]
    width = channels * 2
    chunks = channels // CHUNK
    size, freqs = plan.size, plan.freqs
    per = owners.per
    nxt = lax.rem(sp + 1, n)
    prv = lax.rem(sp + n - 1, n)
    has_prv = sp > 0
    has_nxt = sp < n - 1
    is_owner = (sp >= owners.first) & (sp < owners.first + owners.count)
    low_side = sp < n // 2
    crew = 1 << (max(n, 1).bit_length() // 2)
    crews = -(-n // crew)
    head = sp - lax.rem(sp, crew)
    is_head = (sp == head) & (tp == 1)

    def peer(d):
        return lax.rem(sp + d, n)

    barrier = pltpu.get_barrier_semaphore()

    pairs = [
        (value_h, value), (gate_h, gate), (taps_h, taps), (ft_h, ft), (own_h, own),
        (mats_h, mats), (go_h, go), (gain_h, gain), (shift_h, shift),
    ]
    loads = [
        pltpu.make_async_copy(a, b, load_sem.at[i]) for i, (a, b) in enumerate(pairs)
    ]
    for load in loads:
        load.start()

    def w_copy(c):
        part = pl.ds(pl.multiple_of(c * CHUNK, CHUNK), CHUNK)
        return pltpu.make_async_copy(w_h.at[part], w.at[part], w_sem.at[c])

    for c in range(chunks):
        w_copy(c).start()

    def tell(sem, s, t):
        pl.semaphore_signal(sem, 1, device_id=(s, t), device_id_type=pl.DeviceIdType.MESH)

    members = 2 * jnp.minimum(crew, n - head)

    def each_member(sem):
        def step(i, carry):
            s, t = head + i // 2, lax.rem(i, 2)

            @pl.when((s != sp) | (t != tp))
            def _():
                tell(sem, s, t)

            return carry

        lax.fori_loop(0, members, step, 0)

    def each_head(sem):
        def step(i, carry):
            @pl.when(i * crew != sp)
            def _():
                tell(sem, i * crew, 1)

            return carry

        lax.fori_loop(0, crews, step, 0)

    tell(barrier, sp, 1 - tp)

    @pl.when(has_prv)
    def _():
        tell(barrier, prv, tp)

    @pl.when(has_nxt)
    def _():
        tell(barrier, nxt, tp)

    @pl.when(is_head)
    def _():
        each_member(barrier)
        each_head(barrier)

    greeted = (
        1 + has_prv.astype(jnp.int32) + has_nxt.astype(jnp.int32)
        + jnp.where(is_head, crews - 1, 1)
    )

    def handshake_up():
        @pl.when(jnp.logical_not(is_head))
        def _():
            tell(meet.at[0], head, 1)

    def handshake_across():
        @pl.when(is_head)
        def _():
            pl.semaphore_wait(meet.at[0], members - 1)
            each_head(meet.at[1])

    def handshake_down():
        @pl.when(is_head)
        def _():
            if crews > 1:
                pl.semaphore_wait(meet.at[1], crews - 1)
            each_member(meet.at[2])

    def handshake_done():
        @pl.when(jnp.logical_not(is_head))
        def _():
            pl.semaphore_wait(meet.at[2], 1)

    def cut(c):
        return pl.ds(c * CHUNK, CHUNK)

    loads[0].wait()
    loads[1].wait()

    def gate_step(i, carry):
        part = pl.ds(pl.multiple_of(i * ALIGN, ALIGN), ALIGN)
        place = pl.ds(pl.multiple_of(i * ALIGN + edge, ALIGN), ALIGN)
        sig = sigmoid(gate[part].astype(F32))
        sig_s[part] = sig
        gw[place] = (value[part].astype(F32) * sig).astype(BF16)
        return carry

    lax.fori_loop(0, rows // ALIGN, gate_step, 0, unroll=4)

    def remote(src, dst, send, recv, device):
        return pltpu.make_async_remote_copy(
            src_ref=src, dst_ref=dst, send_sem=send, recv_sem=recv,
            device_id=device, device_id_type=pl.DeviceIdType.MESH,
        )

    def halo_pair(ref, k):
        return (
            remote(ref.at[pl.ds(rows, edge)], ref.at[pl.ds(0, edge)],
                   halo_send.at[k], halo_recv.at[k], (nxt, tp)),
            remote(ref.at[pl.ds(edge, edge)], ref.at[pl.ds(rows + edge, edge)],
                   halo_send.at[k + 1], halo_recv.at[k + 1], (prv, tp)),
        )

    def send_halo(pair):
        @pl.when(has_nxt)
        def _():
            pair[0].start()

        @pl.when(has_prv)
        def _():
            pair[1].start()

    def recv_prv(pair, ref):
        @pl.when(has_prv)
        def _():
            pair[0].wait_recv()

        @pl.when(sp == 0)
        def _():
            ref[pl.ds(0, edge)] = jnp.zeros((edge, channels), BF16)

    def recv_nxt(pair, ref):
        @pl.when(has_nxt)
        def _():
            pair[1].wait_recv()

        @pl.when(sp == n - 1)
        def _():
            ref[pl.ds(rows + edge, edge)] = jnp.zeros((edge, channels), BF16)

    def sent_halo(pair):
        @pl.when(has_nxt)
        def _():
            pair[0].wait_send()

        @pl.when(has_prv)
        def _():
            pair[1].wait_send()

    def settle(ref, count, sem):
        if count:
            part = ref.at[pl.ds(0, count)]
            pltpu.make_async_copy(part, part, sem).wait()

    gw_halo = halo_pair(gw, 0)
    gc_halo = halo_pair(gcw, 2)

    pl.semaphore_wait(barrier, greeted)
    send_halo(gw_halo)
    handshake_up()

    for load in loads[2:7]:
        load.wait()

    tap = jnp.concatenate(
        [taps[...], jnp.zeros((plan.tap_rows - plan.kernel, channels), F32)], 0
    )
    tap_high = tap.astype(BF16)
    tap_low = (tap - tap_high.astype(F32)).astype(BF16)
    for k, part in enumerate((tap_high, tap_low, tap_high)):
        tcat[pl.ds(k * plan.tap_rows, plan.tap_rows)] = part

    def tap_step(_, carry):
        for c in range(chunks):
            ts[:, cut(c)] = dot(ft[...], tcat[:, cut(c)])
        return carry

    lax.fori_loop(0, 1, tap_step, 0)

    def mix(a, b):
        return lax.dot_general(a, b, (((1,), (1,)), ((), ())), preferred_element_type=F32)

    def mix_step(c, carry):
        part = pl.ds(pl.multiple_of(c * CHUNK, CHUNK), CHUNK)
        w_copy(c).wait()
        gm[:, part] = mix(go[...], w[part])
        return carry

    early = chunks - chunks // 4
    lax.fori_loop(0, early, mix_step, 0)
    handshake_across()

    def fold(x):
        out = x[:, :LANES]
        for k in range(1, x.shape[1] // LANES):
            out = out + x[:, k * LANES : (k + 1) * LANES]
        return out

    lanes = lax.broadcasted_iota(jnp.int32, (ALIGN, LANES), 1) < LANES // 2

    def multiply(spec, sign):
        for f in range(0, freqs, ALIGN):
            high, low = pl.ds(f, ALIGN), pl.ds(freqs + f, ALIGN)
            for c in range(chunks):
                re, im = spec[high, cut(c)], spec[low, cut(c)]
                ta, tb = ts[high, cut(c)], ts[low, cut(c)]
                prod[high, cut(c)] = (re * ta + sign * im * tb).astype(BF16)
                other = re * tb - sign * im * ta
                prod[low, cut(c)] = (sign * other).astype(BF16)

    def conv_step(b):
        start = b * block
        spec = g_spec.at[pl.ds(b * size, size)]
        spec[...] = dot(mats[pl.ds(0, size)], gw[pl.ds(start, size)])
        multiply(spec, 1.0)
        conv[pl.ds(start, block)] = dot(mats[pl.ds(plan.at_conv, block)], prod[...])
        for r in range(start, start + block, ALIGN):
            one = two = None
            for c in range(chunks):
                x = conv[pl.ds(r, ALIGN), cut(c)]
                p, q = fold(x), fold(x * x)
                one, two = (p, q) if c == 0 else (one + p, two + q)
            st1[pl.ds(r, ALIGN)] = jnp.where(
                lanes, jnp.sum(one, 1, keepdims=True), jnp.sum(two, 1, keepdims=True)
            )

    def swap(src, dst, b, k):
        place = pl.ds(b * block, block)
        return remote(
            src.at[place], dst.at[place], tp_send.at[k], tp_recv.at[k], (sp, 1 - tp)
        )

    swap1 = [swap(st1, st1_in, b, b) for b in range(2)]
    swap2 = [swap(st2, st2_in, b, 2 + b) for b in range(2)]

    def conv_at(b):
        def step(_, carry):
            conv_step(b)
            return carry

        lax.fori_loop(0, 1, step, 0)

    recv_prv(gw_halo, gw)
    conv_at(0)
    swap1[0].start()
    recv_nxt(gw_halo, gw)
    conv_at(1)
    swap1[1].start()
    handshake_down()
    lax.fori_loop(early, chunks, mix_step, 0)

    loads[7].wait()
    loads[8].wait()
    hgain[...] = jnp.broadcast_to(0.5 * gain[...], hgain.shape)
    hshift[...] = jnp.broadcast_to(0.5 * shift[...], hshift.shape)

    def twice(x):
        return jnp.concatenate([x, x], 0)

    def halves(x):
        return x[:8] + x[8:]

    def norm_at(b):
        total_g, total_s = [None] * chunks, [None] * chunks
        for r in range(b * block, (b + 1) * block, ALIGN):
            part = pl.ds(r, ALIGN)
            tot = (st1[part] + st1_in[part]) * (1.0 / width)
            mean = tot[:, :1]
            var = tot[:, LANES // 2 : LANES // 2 + 1] - mean * mean
            inv = lax.rsqrt(var + EPS)
            inv_s[part] = jnp.broadcast_to(inv, (ALIGN, LANES))
            one = two = None
            for c in range(chunks):
                hg = twice(hgain[:, cut(c)])
                normed = (conv[part, cut(c)] - mean) * inv
                half_pre = normed * hg + twice(hshift[:, cut(c)])
                th = jnp.tanh(half_pre)
                gp = gm[part, cut(c)] * (1.0 + th) * (1.0 + half_pre * (1.0 - th))
                gn = gp * hg
                gpn = gp * normed
                conv[part, cut(c)] = normed
                gm[part, cut(c)] = gn
                p, q = fold(gn), fold(gpn * hg)
                one, two = (p, q) if c == 0 else (one + p, two + q)
                g, h = halves(gpn), halves(gp)
                if total_g[c] is not None:
                    g, h = total_g[c] + g, total_s[c] + h
                total_g[c], total_s[c] = g, h
            st2[part] = jnp.where(
                lanes, jnp.sum(one, 1, keepdims=True), jnp.sum(two, 1, keepdims=True)
            )
        for c in range(chunks):
            if b == 0:
                colg[:, cut(c)] = total_g[c]
                cols[:, cut(c)] = total_s[c]
            else:
                colg[:, cut(c)] += total_g[c]
                cols[:, cut(c)] += total_s[c]

    swap1[0].wait_recv()
    norm_at(0)
    swap2[0].start()
    swap1[1].wait_recv()
    norm_at(1)
    swap2[1].start()

    rg = jnp.sum(colg[...], 0, keepdims=True)
    rsh = jnp.sum(cols[...], 0, keepdims=True)
    groups = channels // LANES
    gs[sp] = jnp.concatenate(
        [x[:, k * LANES : (k + 1) * LANES] for x in (rg, rsh) for k in range(groups)], 0
    ).astype(BF16)

    def send_gs(d, carry):
        remote(gs.at[sp], gs.at[sp], all_send.at[0], all_recv.at[0], (peer(d), tp)).start()
        return carry

    handshake_done()
    lax.fori_loop(1, n, send_gs, 0)

    def gc_at(b):
        for r in range(b * block, (b + 1) * block, ALIGN):
            part = pl.ds(r, ALIGN)
            tot = (st2[part] + st2_in[part]) * (1.0 / width)
            inv = inv_s[part]
            scaled = inv * tot
            m1 = scaled[:, :1]
            m2 = scaled[:, LANES // 2 : LANES // 2 + 1]
            inv = inv[:, :1]
            for c in range(chunks):
                gcw[pl.ds(r + edge, ALIGN), cut(c)] = (
                    inv * gm[part, cut(c)] - m1 - conv[part, cut(c)] * m2
                ).astype(BF16)

    slots = owners.count * per
    if slots > tiles:
        rs_src[pl.ds(tiles, slots - tiles)] = jnp.zeros((slots - tiles, ALIGN, LANES), BF16)
    tall = plan.tap_rows // ALIGN

    def lag_part(b, f, c):
        high, low = pl.ds(f, ALIGN), pl.ds(freqs + f, ALIGN)
        re, im = spec_s[high, cut(c)], spec_s[low, cut(c)]
        hr = g_spec[pl.ds(b * size + f, ALIGN), cut(c)]
        hi = g_spec[pl.ds(b * size + freqs + f, ALIGN), cut(c)]
        return high, low, hr * re + hi * im, hr * im - hi * re

    def send_rs(i, carry):
        o = jnp.where(low_side, owners.count - 1 - i, i)
        to = owners.first + o

        @pl.when(to != sp)
        def _():
            remote(rs_src.at[pl.ds(o * per, per)], rs_in.at[sp],
                   all_send.at[1], all_recv.at[1], (to, tp)).start()

        return carry

    def spec_first(_, carry):
        spec_s[...] = dot(own[...], gcw[pl.ds(edge, block)])
        for f in range(0, freqs, ALIGN):
            for c in range(chunks):
                high, low, dr, di = lag_part(0, f, c)
                dsp[high, cut(c)] = dr
                dsp[low, cut(c)] = di
        return carry

    def spec_last(_, carry):
        spec_s[...] = dot(own[...], gcw[pl.ds(edge + block, block)])
        for f in range(0, freqs, ALIGN):
            for c in range(chunks):
                high, low, dr, di = lag_part(1, f, c)
                prod[high, cut(c)] = (dr + dsp[high, cut(c)]).astype(BF16)
                prod[low, cut(c)] = (di + dsp[low, cut(c)]).astype(BF16)
        out = dot(mats[pl.ds(plan.at_lags, plan.tap_rows)], prod[...]) * plan.lag_scale
        out = out.astype(BF16)
        for r in range(tall):
            for k in range(groups):
                rs_src[k * tall + r] = out[
                    r * ALIGN : (r + 1) * ALIGN, k * LANES : (k + 1) * LANES
                ]
        return carry

    swap2[0].wait_recv()
    gc_at(0)
    lax.fori_loop(0, 1, spec_first, 0)
    swap2[1].wait_recv()
    gc_at(1)

    lax.fori_loop(0, 1, spec_last, 0)
    lax.fori_loop(0, owners.count, send_rs, 0)
    send_halo(gc_halo)

    @pl.when(is_owner)
    def _():
        o = sp - owners.first
        rs_in[sp] = rs_src[pl.ds(o * per, per)]
        settle(rs_in, n - 1, all_recv.at[1])
        zero = jnp.zeros((per, ALIGN, LANES), F32)
        summed = lax.fori_loop(0, n, lambda i, t: t + rs_in[i].astype(F32), zero)
        ag[o] = summed.astype(BF16)

        def send_ag(i, carry):
            to = jnp.where(low_side, n - 1 - i, i)

            @pl.when(to != sp)
            def _():
                remote(ag.at[o], ag.at[o], all_send.at[2], all_recv.at[2], (to, tp)).start()

            return carry

        lax.fori_loop(0, n, send_ag, 0)


    def out_step(b):
        start = b * block
        spec_s[...] = dot(mats[pl.ds(0, size)], gcw[pl.ds(start, size)])
        multiply(spec_s, -1.0)
        conv[pl.ds(start, block)] = dot(mats[pl.ds(plan.at_grad, block)], prod[...])
        for r in range(start, start + block, ALIGN):
            part = pl.ds(r, ALIGN)
            for c in range(chunks):
                sig = sig_s[part, cut(c)]
                left = conv[part, cut(c)] * sig
                dv[part, cut(c)] = left.astype(BF16)
                dg[part, cut(c)] = (
                    left * value[part, cut(c)].astype(F32) * (1.0 - sig)
                ).astype(BF16)

    def out_at(b):
        def step(_, carry):
            out_step(b)
            return carry

        lax.fori_loop(0, 1, step, 0)

    recv_prv(gc_halo, gcw)
    out_at(0)
    recv_nxt(gc_halo, gcw)
    out_at(1)

    settle(gs, n - 1, all_recv.at[0])
    small = lax.fori_loop(
        0, n, lambda i, t: t + gs[i].astype(F32), jnp.zeros(gs.shape[1:], F32)
    )
    dgs_o[...] = small * (0.5 / math.sqrt(total))

    sent_halo(gw_halo)
    sent_halo(gc_halo)
    for k in range(2):
        swap1[k].wait_send()
        swap2[k].wait_send()
    settle(gs, n - 1, all_send.at[0])

    @pl.when(is_owner)
    def _():
        settle(rs_in, owners.count - 1, all_send.at[1])
        settle(ag, owners.count - 1, all_recv.at[2])

    @pl.when(jnp.logical_not(is_owner))
    def _():
        settle(rs_in, owners.count, all_send.at[1])
        settle(ag, owners.count, all_recv.at[2])

    for t in range(tiles):
        k, r = t // tall, t % tall
        count = min(ALIGN, plan.kernel - r * ALIGN)
        dt_o[pl.ds(r * ALIGN, count), pl.ds(k * LANES, LANES)] = ag[t // per, t % per].astype(F32)[
            :count
        ]

    @pl.when(is_owner)
    def _():
        def sent(i, carry):
            pltpu.make_async_copy(ag.at[0], ag.at[0], all_send.at[2]).wait()
            return carry

        lax.fori_loop(0, n - 1, sent, 0)


def store(*refs):
    sources, targets, out_sem = refs[:4], refs[4:9], refs[9]
    groups = sources[3].shape[0] // 2
    views = list(sources[:3]) + [
        sources[3].at[pl.ds(0, groups)], sources[3].at[pl.ds(groups, groups)]
    ]
    copies = [
        pltpu.make_async_copy(a, b, out_sem.at[i]) for i, (a, b) in enumerate(zip(views, targets))
    ]
    for copy in copies:
        copy.start()
    for copy in copies:
        copy.wait()


def shards(n, value_in, gate_in, taps, gain, shift, w_out, grad_out):
    rows, channels = value_in.shape
    kernel = taps.shape[0]
    total = rows * n
    plan = Plan(rows, kernel, total)
    groups = channels // LANES
    tiles = plan.tap_rows // ALIGN * groups
    owners = Owners(n, tiles)
    per = owners.per
    model = grad_out.shape[1]
    mats = jnp.asarray(plan.mats, BF16)
    own = jnp.asarray(plan.own, BF16)
    ft = jnp.asarray(plan.taps, BF16)
    hbm = pl.BlockSpec(memory_space=pltpu.HBM)
    vmem = pl.BlockSpec(memory_space=pltpu.VMEM)
    size, block = plan.size, plan.block
    chunks = channels // CHUNK
    dma = pltpu.SemaphoreType.DMA
    results = pl.pallas_call(
        functools.partial(body, plan, n, tiles, owners, total),
        out_shape=(
            pltpu.VMEM((rows, channels), BF16),
            pltpu.VMEM((rows, channels), BF16),
            pltpu.VMEM((kernel, channels), F32),
            pltpu.VMEM((2 * groups, LANES), F32),
        ),
        in_specs=[hbm] * 10,
        out_specs=(vmem,) * 4,
        scratch_shapes=[
            pltpu.VMEM((rows, channels), BF16),
            pltpu.VMEM((rows, channels), BF16),
            pltpu.VMEM((kernel, channels), F32),
            pltpu.VMEM((channels, model), BF16),
            pltpu.VMEM((rows, model), BF16),
            pltpu.VMEM(plan.mats.shape, BF16),
            pltpu.VMEM((rows, channels), F32),
            pltpu.VMEM((plan.wide, channels), BF16),
            pltpu.VMEM((rows, channels), F32),
            pltpu.VMEM((rows, channels), F32),
            pltpu.VMEM((plan.wide, channels), BF16),
            pltpu.VMEM((3 * plan.tap_rows, channels), BF16),
            pltpu.VMEM((size, channels), F32),
            pltpu.VMEM((2 * size, channels), F32),
            pltpu.VMEM((size, channels), F32),
            pltpu.VMEM((size, channels), F32),
            pltpu.VMEM((size, channels), BF16),
            pltpu.VMEM((rows, LANES), F32),
            pltpu.VMEM((rows, LANES), F32),
            pltpu.VMEM((rows, LANES), F32),
            pltpu.VMEM((rows, LANES), F32),
            pltpu.VMEM((rows, LANES), F32),
            pltpu.VMEM((8, channels), F32),
            pltpu.VMEM((8, channels), F32),
            pltpu.VMEM((8, channels), F32),
            pltpu.VMEM((8, channels), F32),
            pltpu.VMEM((n, 2 * groups, LANES), BF16),
            pltpu.VMEM((owners.count * per, ALIGN, LANES), BF16),
            pltpu.VMEM((n, per, ALIGN, LANES), BF16),
            pltpu.VMEM((owners.count, per, ALIGN, LANES), BF16),
            pltpu.VMEM(plan.own.shape, BF16),
            pltpu.VMEM(plan.taps.shape, BF16),
            pltpu.VMEM((1, channels), F32),
            pltpu.VMEM((1, channels), F32),
            pltpu.SemaphoreType.REGULAR((3,)),
            dma((9,)), dma((chunks,)), dma((4,)), dma((4,)),
            dma((4,)), dma((4,)), dma((3,)), dma((3,)),
        ],
        compiler_params=pltpu.CompilerParams(
            collective_id=0, has_side_effects=True, vmem_limit_bytes=VMEM_GRANT
        ),
    )(
        *(
            pltpu.with_memory_space_constraint(x, pltpu.HBM)
            for x in (
                value_in, gate_in, taps, gain.reshape(1, -1), shift.reshape(1, -1), w_out,
                grad_out, mats, own, ft,
            )
        )
    )
    results = [pltpu.with_memory_space_constraint(x, pltpu.VMEM) for x in results]
    d_value, d_gate, d_taps, d_gain, d_shift = pl.pallas_call(
        store,
        out_shape=(
            jax.ShapeDtypeStruct((rows, channels), BF16),
            jax.ShapeDtypeStruct((rows, channels), BF16),
            jax.ShapeDtypeStruct((kernel, channels), F32),
            jax.ShapeDtypeStruct((groups, LANES), F32),
            jax.ShapeDtypeStruct((groups, LANES), F32),
        ),
        in_specs=[vmem] * 4,
        out_specs=(hbm,) * 5,
        scratch_shapes=[dma((5,))],
        compiler_params=pltpu.CompilerParams(vmem_limit_bytes=8 * 1024 * 1024),
    )(*results)
    return (d_value, d_gate, d_taps, d_gain.reshape(-1), d_shift.reshape(-1))


def solution(mesh):
    return jax.shard_map(
        functools.partial(shards, mesh.shape["sp"]),
        mesh=mesh,
        in_specs=(
            P("sp", "tp"),
            P("sp", "tp"),
            P(None, "tp"),
            P("tp"),
            P("tp"),
            P("tp", None),
            P("sp", None),
        ),
        out_specs=(P("sp", "tp"), P("sp", "tp"), P(None, "tp"), P("tp"), P("tp")),
        check_vma=False,
    )
```

```python
import functools
import math

import jax
import jax.numpy as jnp
import numpy as np
from jax import lax
from jax.experimental import pallas as pl
from jax.experimental.pallas import tpu as pltpu
from jax.sharding import PartitionSpec as P

EPS = 1e-05
ALIGN = 16
LANES = 128
CHUNK = 256
VMEM_GRANT = 48 * 1024 * 1024
F32 = jnp.float32
BF16 = jnp.bfloat16


class Plan:
    def __init__(self, rows, kernel, total):
        self.half = kernel // 2
        self.kernel = kernel
        self.rows = rows
        self.edge = -(-self.half // ALIGN) * ALIGN
        edge = self.edge
        self.block = rows // 2
        self.size = self.block + 2 * edge
        size = self.size
        self.freqs = size // 2
        self.wide = rows + 2 * edge
        omega = 2.0 * np.pi * (np.arange(self.freqs) + 0.5) / size

        def spectrum(times):
            angle = omega[:, None] * times[None, :]
            return np.concatenate([np.cos(angle), np.sin(angle)], 0)

        def inverse(times):
            angle = times[:, None] * omega[None, :]
            return np.concatenate([np.cos(angle), -np.sin(angle)], 1)

        own = np.arange(self.block)
        self.tap_rows = -(-kernel // ALIGN) * ALIGN
        lags = inverse(np.arange(self.tap_rows) - self.half)
        lags[kernel:] = 0.0
        self.mats = np.concatenate(
            [
                spectrum(np.arange(size)),
                inverse(own + edge - self.half),
                inverse(own + edge + self.half),
                lags,
            ],
            0,
        )
        self.at_conv = size
        self.at_grad = self.at_conv + self.block
        self.at_lags = self.at_grad + self.block
        self.own = spectrum(own + edge)
        taps = np.zeros((size, self.tap_rows))
        taps[:, :kernel] = spectrum(np.arange(kernel)) * (2.0 / size)
        high = taps.astype(jnp.bfloat16)
        low = taps - high.astype(np.float64)
        self.taps = np.concatenate([high.astype(np.float64), high.astype(np.float64), low], 1)
        self.lag_scale = 2.0 / size / math.sqrt(total)


class Owners:
    def __init__(self, n, tiles):
        self.count = max(1, min(n // 2, tiles))
        self.per = -(-tiles // self.count)
        self.first = (n - self.count) // 2


def dot(a, b):
    return jnp.dot(a, b, preferred_element_type=F32)


def sigmoid(x):
    return 0.5 * jnp.tanh(0.5 * x) + 0.5


def body(
    plan, n, tiles, owners, total,
    value_h, gate_h, taps_h, gain_h, shift_h, w_h, go_h, mats_h, own_h, ft_h,
    dv, dg, dt_o, dgs_o,
    value, gate, taps, w, go, mats,
    sig_s, gw, conv, gm, gcw, tcat, ts, g_spec, spec_s, dsp, prod,
    st1, st1_in, st2, st2_in, inv_s, colg, cols, hgain, hshift,
    gs, rs_src, rs_in, ag_src, ag, own, ft, gain, shift,
    meet, load_sem, w_sem, halo_send, halo_recv, tp_send, tp_recv,
    all_send, all_recv,
):
    sp = lax.axis_index("sp")
    tp = lax.axis_index("tp")
    rows, edge, block = plan.rows, plan.edge, plan.block
    channels = value.shape[1]
    width = channels * 2
    chunks = channels // CHUNK
    size, freqs = plan.size, plan.freqs
    per = owners.per
    nxt = lax.rem(sp + 1, n)
    prv = lax.rem(sp + n - 1, n)
    has_prv = sp > 0
    has_nxt = sp < n - 1
    is_owner = (sp >= owners.first) & (sp < owners.first + owners.count) & (tp == 1)
    low_side = sp < n // 2
    crew = 1 << (max(n, 1).bit_length() // 2)
    crews = -(-n // crew)
    head = sp - lax.rem(sp, crew)
    is_head = (sp == head) & (tp == 1)

    def peer(d):
        return lax.rem(sp + d, n)

    barrier = pltpu.get_barrier_semaphore()

    inner = pl.ds(edge, rows - 2 * edge)
    sides = [pl.ds(0, edge), pl.ds(rows - edge, edge)]
    pairs = [(h.at[part], v.at[part]) for h, v in ((value_h, value), (gate_h, gate)) for part in sides]
    pairs += [(h.at[inner], v.at[inner]) for h, v in ((value_h, value), (gate_h, gate))]
    pairs += [(taps_h, taps), (ft_h, ft), (go_h, go)]
    late = [(mats_h, mats), (own_h, own), (gain_h, gain), (shift_h, shift)]
    loads = [
        pltpu.make_async_copy(a, b, load_sem.at[i]) for i, (a, b) in enumerate(pairs + late)
    ]

    def w_copy(c):
        part = pl.ds(pl.multiple_of(c * CHUNK, CHUNK), CHUNK)
        return pltpu.make_async_copy(w_h.at[part], w.at[part], w_sem.at[c])

    for load in loads[: len(pairs)]:
        load.start()
    for c in range(chunks):
        w_copy(c).start()
    for load in loads[len(pairs):]:
        load.start()

    def tell(sem, s, t):
        pl.semaphore_signal(sem, 1, device_id=(s, t), device_id_type=pl.DeviceIdType.MESH)

    members = 2 * jnp.minimum(crew, n - head)

    def each_member(sem):
        def step(i, carry):
            s, t = head + i // 2, lax.rem(i, 2)

            @pl.when((s != sp) | (t != tp))
            def _():
                tell(sem, s, t)

            return carry

        lax.fori_loop(0, members, step, 0)

    def each_head(sem):
        def step(i, carry):
            @pl.when(i * crew != sp)
            def _():
                tell(sem, i * crew, 1)

            return carry

        lax.fori_loop(0, crews, step, 0)

    tell(barrier, sp, 1 - tp)

    @pl.when(has_prv)
    def _():
        tell(barrier, prv, tp)

    @pl.when(has_nxt)
    def _():
        tell(barrier, nxt, tp)

    @pl.when(is_head)
    def _():
        each_member(barrier)
        each_head(barrier)

    greeted = (
        1 + has_prv.astype(jnp.int32) + has_nxt.astype(jnp.int32)
        + jnp.where(is_head, crews - 1, 1)
    )

    def handshake_up():
        @pl.when(jnp.logical_not(is_head))
        def _():
            tell(meet.at[0], head, 1)

    def handshake_across():
        @pl.when(is_head)
        def _():
            pl.semaphore_wait(meet.at[0], members - 1)
            each_head(meet.at[1])

    def handshake_down():
        @pl.when(is_head)
        def _():
            if crews > 1:
                pl.semaphore_wait(meet.at[1], crews - 1)
            each_member(meet.at[2])

    def handshake_done():
        @pl.when(jnp.logical_not(is_head))
        def _():
            pl.semaphore_wait(meet.at[2], 1)

    def cut(c):
        return pl.ds(c * CHUNK, CHUNK)

    def gate_step(i, carry):
        part = pl.ds(pl.multiple_of(i * ALIGN, ALIGN), ALIGN)
        place = pl.ds(pl.multiple_of(i * ALIGN + edge, ALIGN), ALIGN)
        sig = sigmoid(gate[part].astype(F32))
        sig_s[part] = sig
        gw[place] = (value[part].astype(F32) * sig).astype(BF16)
        return carry

    def remote(src, dst, send, recv, device):
        return pltpu.make_async_remote_copy(
            src_ref=src, dst_ref=dst, send_sem=send, recv_sem=recv,
            device_id=device, device_id_type=pl.DeviceIdType.MESH,
        )

    def halo_pair(ref, k):
        return (
            remote(ref.at[pl.ds(rows, edge)], ref.at[pl.ds(0, edge)],
                   halo_send.at[k], halo_recv.at[k], (nxt, tp)),
            remote(ref.at[pl.ds(edge, edge)], ref.at[pl.ds(rows + edge, edge)],
                   halo_send.at[k + 1], halo_recv.at[k + 1], (prv, tp)),
        )

    def send_halo(pair):
        @pl.when(has_nxt)
        def _():
            pair[0].start()

        @pl.when(has_prv)
        def _():
            pair[1].start()

    def recv_prv(pair, ref):
        @pl.when(has_prv)
        def _():
            pair[0].wait_recv()

        @pl.when(sp == 0)
        def _():
            ref[pl.ds(0, edge)] = jnp.zeros((edge, channels), BF16)

    def recv_nxt(pair, ref):
        @pl.when(has_nxt)
        def _():
            pair[1].wait_recv()

        @pl.when(sp == n - 1)
        def _():
            ref[pl.ds(rows + edge, edge)] = jnp.zeros((edge, channels), BF16)

    def sent_halo(pair):
        @pl.when(has_nxt)
        def _():
            pair[0].wait_send()

        @pl.when(has_prv)
        def _():
            pair[1].wait_send()

    def settle(ref, count, sem):
        if count:
            part = ref.at[pl.ds(0, count)]
            pltpu.make_async_copy(part, part, sem).wait()

    gw_halo = halo_pair(gw, 0)
    gc_halo = halo_pair(gcw, 2)

    for load in loads[:4]:
        load.wait()
    sided = edge // ALIGN
    for r in range(sided):
        gate_step(r, 0)
        gate_step(rows // ALIGN - 1 - r, 0)
    pl.semaphore_wait(barrier, greeted)
    send_halo(gw_halo)
    handshake_up()
    loads[4].wait()
    loads[5].wait()
    lax.fori_loop(sided, rows // ALIGN - sided, gate_step, 0, unroll=7)
    loads[6].wait()
    loads[7].wait()

    tap = jnp.concatenate(
        [taps[...], jnp.zeros((plan.tap_rows - plan.kernel, channels), F32)], 0
    )
    tap_high = tap.astype(BF16)
    tap_low = (tap - tap_high.astype(F32)).astype(BF16)
    for k, part in enumerate((tap_high, tap_low, tap_high)):
        tcat[pl.ds(k * plan.tap_rows, plan.tap_rows)] = part

    def tap_step(_, carry):
        for c in range(chunks):
            ts[:, cut(c)] = dot(ft[...], tcat[:, cut(c)])
        return carry

    lax.fori_loop(0, 1, tap_step, 0)

    def mix(a, b):
        return lax.dot_general(a, b, (((1,), (1,)), ((), ())), preferred_element_type=F32)

    def mix_step(c, carry):
        part = pl.ds(pl.multiple_of(c * CHUNK, CHUNK), CHUNK)
        w_copy(c).wait()
        gm[:, part] = mix(go[...], w[part])
        return carry

    loads[8].wait()
    lax.fori_loop(0, chunks, mix_step, 0)
    handshake_across()
    loads[9].wait()

    def fold(x):
        out = x[:, :LANES]
        for k in range(1, x.shape[1] // LANES):
            out = out + x[:, k * LANES : (k + 1) * LANES]
        return out

    lanes = lax.broadcasted_iota(jnp.int32, (ALIGN, LANES), 1) < LANES // 2

    def multiply(spec, sign):
        for f in range(0, freqs, ALIGN):
            high, low = pl.ds(f, ALIGN), pl.ds(freqs + f, ALIGN)
            for c in range(chunks):
                re, im = spec[high, cut(c)], spec[low, cut(c)]
                ta, tb = ts[high, cut(c)], ts[low, cut(c)]
                prod[high, cut(c)] = (re * ta + sign * im * tb).astype(BF16)
                other = re * tb - sign * im * ta
                prod[low, cut(c)] = (sign * other).astype(BF16)

    def conv_step(b):
        start = b * block
        spec = g_spec.at[pl.ds(b * size, size)]
        spec[...] = dot(mats[pl.ds(0, size)], gw[pl.ds(start, size)])
        multiply(spec, 1.0)
        conv[pl.ds(start, block)] = dot(mats[pl.ds(plan.at_conv, block)], prod[...])
        for r in range(start, start + block, ALIGN):
            one = two = None
            for c in range(chunks):
                x = conv[pl.ds(r, ALIGN), cut(c)]
                p, q = fold(x), fold(x * x)
                one, two = (p, q) if c == 0 else (one + p, two + q)
            st1[pl.ds(r, ALIGN)] = jnp.where(
                lanes, jnp.sum(one, 1, keepdims=True), jnp.sum(two, 1, keepdims=True)
            )

    def swap(src, dst, b, k):
        place = pl.ds(b * block, block)
        return remote(
            src.at[place], dst.at[place], tp_send.at[k], tp_recv.at[k], (sp, 1 - tp)
        )

    swap1 = [swap(st1, st1_in, b, b) for b in range(2)]
    swap2 = [swap(st2, st2_in, b, 2 + b) for b in range(2)]

    def conv_at(b):
        def step(_, carry):
            conv_step(b)
            return carry

        lax.fori_loop(0, 1, step, 0)

    recv_prv(gw_halo, gw)
    conv_at(0)
    swap1[0].start()
    recv_nxt(gw_halo, gw)
    conv_at(1)
    swap1[1].start()
    handshake_down()
    for load in loads[10:]:
        load.wait()
    hgain[...] = jnp.broadcast_to(0.5 * gain[...], hgain.shape)
    hshift[...] = jnp.broadcast_to(0.5 * shift[...], hshift.shape)

    def twice(x):
        return jnp.concatenate([x, x], 0)

    def halves(x):
        return x[:8] + x[8:]

    def norm_at(b):
        total_g, total_s = [None] * chunks, [None] * chunks
        for r in range(b * block, (b + 1) * block, ALIGN):
            part = pl.ds(r, ALIGN)
            tot = (st1[part] + st1_in[part]) * (1.0 / width)
            mean = tot[:, :1]
            var = tot[:, LANES // 2 : LANES // 2 + 1] - mean * mean
            inv = lax.rsqrt(var + EPS)
            inv_s[part] = jnp.broadcast_to(inv, (ALIGN, LANES))
            one = two = None
            for c in range(chunks):
                hg = twice(hgain[:, cut(c)])
                normed = (conv[part, cut(c)] - mean) * inv
                half_pre = normed * hg + twice(hshift[:, cut(c)])
                th = jnp.tanh(half_pre)
                gp = gm[part, cut(c)] * (1.0 + th) * (1.0 + half_pre * (1.0 - th))
                gn = gp * hg
                gpn = gp * normed
                conv[part, cut(c)] = normed
                gm[part, cut(c)] = gn
                p, q = fold(gn), fold(gpn * hg)
                one, two = (p, q) if c == 0 else (one + p, two + q)
                g, h = halves(gpn), halves(gp)
                if total_g[c] is not None:
                    g, h = total_g[c] + g, total_s[c] + h
                total_g[c], total_s[c] = g, h
            st2[part] = jnp.where(
                lanes, jnp.sum(one, 1, keepdims=True), jnp.sum(two, 1, keepdims=True)
            )
        for c in range(chunks):
            if b == 0:
                colg[:, cut(c)] = total_g[c]
                cols[:, cut(c)] = total_s[c]
            else:
                colg[:, cut(c)] += total_g[c]
                cols[:, cut(c)] += total_s[c]

    swap1[0].wait_recv()
    norm_at(0)
    swap2[0].start()
    swap1[1].wait_recv()
    norm_at(1)
    swap2[1].start()

    rg = jnp.sum(colg[...], 0, keepdims=True)
    rsh = jnp.sum(cols[...], 0, keepdims=True)
    groups = channels // LANES
    gs[sp] = jnp.concatenate(
        [x[:, k * LANES : (k + 1) * LANES] for x in (rg, rsh) for k in range(groups)], 0
    ).astype(BF16)

    def send_gs(d, carry):
        remote(gs.at[sp], gs.at[sp], all_send.at[0], all_recv.at[0], (peer(d), tp)).start()
        return carry

    handshake_done()
    lax.fori_loop(1, n, send_gs, 0)

    def gc_at(b):
        for r in range(b * block, (b + 1) * block, ALIGN):
            part = pl.ds(r, ALIGN)
            tot = (st2[part] + st2_in[part]) * (1.0 / width)
            inv = inv_s[part]
            scaled = inv * tot
            m1 = scaled[:, :1]
            m2 = scaled[:, LANES // 2 : LANES // 2 + 1]
            inv = inv[:, :1]
            for c in range(chunks):
                gcw[pl.ds(r + edge, ALIGN), cut(c)] = (
                    inv * gm[part, cut(c)] - m1 - conv[part, cut(c)] * m2
                ).astype(BF16)

    slots = owners.count * per
    if slots > tiles:
        rs_src[pl.ds(tiles, slots - tiles)] = jnp.zeros((slots - tiles, ALIGN, LANES), BF16)
    tall = plan.tap_rows // ALIGN

    def lag_part(b, f, c):
        high, low = pl.ds(f, ALIGN), pl.ds(freqs + f, ALIGN)
        re, im = spec_s[high, cut(c)], spec_s[low, cut(c)]
        hr = g_spec[pl.ds(b * size + f, ALIGN), cut(c)]
        hi = g_spec[pl.ds(b * size + freqs + f, ALIGN), cut(c)]
        return high, low, hr * re + hi * im, hr * im - hi * re

    def send_rs(i, carry):
        o = jnp.where(low_side, owners.count - 1 - i, i)
        to = owners.first + o

        @pl.when((to != sp) | (tp != 1))
        def _():
            remote(rs_src.at[pl.ds(o * per, per)], rs_in.at[2 * sp + tp],
                   all_send.at[1], all_recv.at[1], (to, 1)).start()

        return carry

    def spec_first(_, carry):
        spec_s[...] = dot(own[...], gcw[pl.ds(edge, block)])
        for f in range(0, freqs, ALIGN):
            for c in range(chunks):
                high, low, dr, di = lag_part(0, f, c)
                dsp[high, cut(c)] = dr
                dsp[low, cut(c)] = di
        return carry

    def spec_last(_, carry):
        spec_s[...] = dot(own[...], gcw[pl.ds(edge + block, block)])
        for f in range(0, freqs, ALIGN):
            for c in range(chunks):
                high, low, dr, di = lag_part(1, f, c)
                prod[high, cut(c)] = (dr + dsp[high, cut(c)]).astype(BF16)
                prod[low, cut(c)] = (di + dsp[low, cut(c)]).astype(BF16)
        out = dot(mats[pl.ds(plan.at_lags, plan.tap_rows)], prod[...]) * plan.lag_scale
        out = out.astype(BF16)
        for r in range(tall):
            for k in range(groups):
                rs_src[k * tall + r] = out[
                    r * ALIGN : (r + 1) * ALIGN, k * LANES : (k + 1) * LANES
                ]
        return carry

    swap2[0].wait_recv()
    gc_at(0)
    lax.fori_loop(0, 1, spec_first, 0)
    swap2[1].wait_recv()
    gc_at(1)

    lax.fori_loop(0, 1, spec_last, 0)
    lax.fori_loop(0, owners.count, send_rs, 0)
    send_halo(gc_halo)

    @pl.when(is_owner)
    def _():
        o = sp - owners.first
        rs_in[2 * sp + 1] = rs_src[pl.ds(o * per, per)]
        settle(rs_in, 2 * n - 1, all_recv.at[1])
        zero = jnp.zeros((2, per, ALIGN, LANES), F32)
        summed = lax.fori_loop(
            0, n, lambda i, t: t + rs_in[pl.ds(2 * i, 2)].astype(F32), zero, unroll=4
        )
        ag_src[...] = summed.astype(BF16)
        ag[o] = ag_src[1]

        def send_ag(i, carry):
            for t in range(2):
                @pl.when((i != sp) | (t != 1))
                def _():
                    remote(ag_src.at[t], ag.at[o],
                           all_send.at[2], all_recv.at[2], (i, t)).start()

            return carry

        lax.fori_loop(0, n, send_ag, 0)

    def out_step(b):
        start = b * block
        spec_s[...] = dot(mats[pl.ds(0, size)], gcw[pl.ds(start, size)])
        multiply(spec_s, -1.0)
        conv[pl.ds(start, block)] = dot(mats[pl.ds(plan.at_grad, block)], prod[...])
        for r in range(start, start + block, ALIGN):
            part = pl.ds(r, ALIGN)
            for c in range(chunks):
                sig = sig_s[part, cut(c)]
                left = conv[part, cut(c)] * sig
                dv[part, cut(c)] = left.astype(BF16)
                dg[part, cut(c)] = (
                    left * value[part, cut(c)].astype(F32) * (1.0 - sig)
                ).astype(BF16)

    def out_at(b):
        def step(_, carry):
            out_step(b)
            return carry

        lax.fori_loop(0, 1, step, 0)

    recv_prv(gc_halo, gcw)
    out_at(0)
    recv_nxt(gc_halo, gcw)
    out_at(1)

    settle(gs, n - 1, all_recv.at[0])
    small = lax.fori_loop(
        0, n, lambda i, t: t + gs[i].astype(F32), jnp.zeros(gs.shape[1:], F32)
    )
    dgs_o[...] = small * (0.5 / math.sqrt(total))

    sent_halo(gw_halo)
    sent_halo(gc_halo)
    for k in range(2):
        swap1[k].wait_send()
        swap2[k].wait_send()
    settle(gs, n - 1, all_send.at[0])

    @pl.when(is_owner)
    def _():
        settle(rs_in, owners.count - 1, all_send.at[1])
        settle(ag, owners.count - 1, all_recv.at[2])

    @pl.when(jnp.logical_not(is_owner))
    def _():
        settle(rs_in, owners.count, all_send.at[1])
        settle(ag, owners.count, all_recv.at[2])

    for t in range(tiles):
        k, r = t // tall, t % tall
        count = min(ALIGN, plan.kernel - r * ALIGN)
        dt_o[pl.ds(r * ALIGN, count), pl.ds(k * LANES, LANES)] = ag[t // per, t % per].astype(F32)[
            :count
        ]

    @pl.when(is_owner)
    def _():
        settle(rs_in, 2 * n - 1, all_send.at[2])


def store(*refs):
    sources, targets, out_sem = refs[:4], refs[4:9], refs[9]
    groups = sources[3].shape[0] // 2
    views = list(sources[:3]) + [
        sources[3].at[pl.ds(0, groups)], sources[3].at[pl.ds(groups, groups)]
    ]
    copies = [
        pltpu.make_async_copy(a, b, out_sem.at[i]) for i, (a, b) in enumerate(zip(views, targets))
    ]
    for copy in copies:
        copy.start()
    for copy in copies:
        copy.wait()


def shards(n, value_in, gate_in, taps, gain, shift, w_out, grad_out):
    rows, channels = value_in.shape
    kernel = taps.shape[0]
    total = rows * n
    plan = Plan(rows, kernel, total)
    groups = channels // LANES
    tiles = plan.tap_rows // ALIGN * groups
    owners = Owners(n, tiles)
    per = owners.per
    model = grad_out.shape[1]
    mats = jnp.asarray(plan.mats, BF16)
    own = jnp.asarray(plan.own, BF16)
    ft = jnp.asarray(plan.taps, BF16)
    hbm = pl.BlockSpec(memory_space=pltpu.HBM)
    vmem = pl.BlockSpec(memory_space=pltpu.VMEM)
    size, block = plan.size, plan.block
    chunks = channels // CHUNK
    dma = pltpu.SemaphoreType.DMA
    results = pl.pallas_call(
        functools.partial(body, plan, n, tiles, owners, total),
        out_shape=(
            pltpu.VMEM((rows, channels), BF16),
            pltpu.VMEM((rows, channels), BF16),
            pltpu.VMEM((kernel, channels), F32),
            pltpu.VMEM((2 * groups, LANES), F32),
        ),
        in_specs=[hbm] * 10,
        out_specs=(vmem,) * 4,
        scratch_shapes=[
            pltpu.VMEM((rows, channels), BF16),
            pltpu.VMEM((rows, channels), BF16),
            pltpu.VMEM((kernel, channels), F32),
            pltpu.VMEM((channels, model), BF16),
            pltpu.VMEM((rows, model), BF16),
            pltpu.VMEM(plan.mats.shape, BF16),
            pltpu.VMEM((rows, channels), F32),
            pltpu.VMEM((plan.wide, channels), BF16),
            pltpu.VMEM((rows, channels), F32),
            pltpu.VMEM((rows, channels), F32),
            pltpu.VMEM((plan.wide, channels), BF16),
            pltpu.VMEM((3 * plan.tap_rows, channels), BF16),
            pltpu.VMEM((size, channels), F32),
            pltpu.VMEM((2 * size, channels), F32),
            pltpu.VMEM((size, channels), F32),
            pltpu.VMEM((size, channels), F32),
            pltpu.VMEM((size, channels), BF16),
            pltpu.VMEM((rows, LANES), F32),
            pltpu.VMEM((rows, LANES), F32),
            pltpu.VMEM((rows, LANES), F32),
            pltpu.VMEM((rows, LANES), F32),
            pltpu.VMEM((rows, LANES), F32),
            pltpu.VMEM((8, channels), F32),
            pltpu.VMEM((8, channels), F32),
            pltpu.VMEM((8, channels), F32),
            pltpu.VMEM((8, channels), F32),
            pltpu.VMEM((n, 2 * groups, LANES), BF16),
            pltpu.VMEM((owners.count * per, ALIGN, LANES), BF16),
            pltpu.VMEM((2 * n, per, ALIGN, LANES), BF16),
            pltpu.VMEM((2, per, ALIGN, LANES), BF16),
            pltpu.VMEM((owners.count, per, ALIGN, LANES), BF16),
            pltpu.VMEM(plan.own.shape, BF16),
            pltpu.VMEM(plan.taps.shape, BF16),
            pltpu.VMEM((1, channels), F32),
            pltpu.VMEM((1, channels), F32),
            pltpu.SemaphoreType.REGULAR((3,)),
            dma((13,)), dma((chunks,)), dma((4,)), dma((4,)),
            dma((4,)), dma((4,)), dma((3,)), dma((3,)),
        ],
        compiler_params=pltpu.CompilerParams(
            collective_id=0, has_side_effects=True, vmem_limit_bytes=VMEM_GRANT
        ),
    )(
        *(
            pltpu.with_memory_space_constraint(x, pltpu.HBM)
            for x in (
                value_in, gate_in, taps, gain.reshape(1, -1), shift.reshape(1, -1), w_out,
                grad_out, mats, own, ft,
            )
        )
    )
    results = [pltpu.with_memory_space_constraint(x, pltpu.VMEM) for x in results]
    d_value, d_gate, d_taps, d_gain, d_shift = pl.pallas_call(
        store,
        out_shape=(
            jax.ShapeDtypeStruct((rows, channels), BF16),
            jax.ShapeDtypeStruct((rows, channels), BF16),
            jax.ShapeDtypeStruct((kernel, channels), F32),
            jax.ShapeDtypeStruct((groups, LANES), F32),
            jax.ShapeDtypeStruct((groups, LANES), F32),
        ),
        in_specs=[vmem] * 4,
        out_specs=(hbm,) * 5,
        scratch_shapes=[dma((5,))],
        compiler_params=pltpu.CompilerParams(vmem_limit_bytes=8 * 1024 * 1024),
    )(*results)
    return (d_value, d_gate, d_taps, d_gain.reshape(-1), d_shift.reshape(-1))


def solution(mesh):
    return jax.shard_map(
        functools.partial(shards, mesh.shape["sp"]),
        mesh=mesh,
        in_specs=(
            P("sp", "tp"),
            P("sp", "tp"),
            P(None, "tp"),
            P("tp"),
            P("tp"),
            P("tp", None),
            P("sp", None),
        ),
        out_specs=(P("sp", "tp"), P("sp", "tp"), P(None, "tp"), P("tp"), P("tp")),
        check_vma=False,
    )
```

```python
import functools
import math

import jax
import jax.numpy as jnp
import numpy as np
from jax import lax
from jax.experimental import pallas as pl
from jax.experimental.pallas import tpu as pltpu
from jax.sharding import PartitionSpec as P

EPS = 1e-05
ALIGN = 16
LANES = 128
CHUNK = 256
VMEM_GRANT = 48 * 1024 * 1024
F32 = jnp.float32
BF16 = jnp.bfloat16


class Plan:
    def __init__(self, rows, kernel, total):
        self.half = half = kernel // 2
        self.kernel = kernel
        self.rows = rows
        self.edge = edge = -(-half // ALIGN) * ALIGN
        self.side = side = 4 * edge
        self.inner = rows - 2 * edge
        self.wide = rows + 2 * edge
        self.tap_rows = -(-kernel // ALIGN) * ALIGN

        def omega(size):
            return 2.0 * np.pi * (np.arange(size // 2) + 0.5) / size

        def spectrum(size, times):
            angle = omega(size)[:, None] * times[None, :]
            return np.concatenate([np.cos(angle), np.sin(angle)], 0)

        def inverse(size, times):
            angle = times[:, None] * omega(size)[None, :]
            return np.concatenate([np.cos(angle), -np.sin(angle)], 1)

        def lags(size):
            out = inverse(size, np.arange(self.tap_rows) - half)
            out[kernel:] = 0.0
            return out

        main = np.arange(self.inner) + edge
        top = np.arange(edge) + edge
        low = np.arange(edge) + side - 2 * edge
        self.main = np.concatenate(
            [
                spectrum(rows, np.arange(rows)), inverse(rows, main - half),
                inverse(rows, main + half), lags(rows),
            ],
            0,
        )
        self.at_conv = rows
        self.at_grad = self.at_conv + self.inner
        self.at_lags = self.at_grad + self.inner
        self.edges = np.concatenate(
            [spectrum(side, np.arange(side))]
            + [inverse(side, part + shift) for shift in (-half, half) for part in (top, low)]
            + [lags(side)],
            0,
        )
        self.edge_conv = side
        self.edge_grad = side + 2 * edge
        self.edge_lags = side + 4 * edge
        self.own = spectrum(rows, main)
        self.own_edges = np.concatenate([spectrum(side, top), spectrum(side, low)], 0)
        taps = np.zeros((rows + side, self.tap_rows))
        times = np.arange(kernel)
        taps[:rows, :kernel] = spectrum(rows, times) * (2.0 / rows)
        taps[rows:, :kernel] = spectrum(side, times) * (2.0 / side)
        high = taps.astype(jnp.bfloat16)
        low_part = taps - high.astype(np.float64)
        self.taps = np.concatenate([high.astype(np.float64), high.astype(np.float64), low_part], 1)
        self.lag_scale = [2.0 / size / math.sqrt(total) for size in (rows, side)]


class Owners:
    def __init__(self, n, tiles):
        self.count = max(1, min(n // 2, tiles))
        self.per = -(-tiles // self.count)
        self.first = (n - self.count) // 2


def dot(a, b):
    return jnp.dot(a, b, preferred_element_type=F32)


def sigmoid(x):
    return 0.5 * jnp.tanh(0.5 * x) + 0.5


def body(
    plan, n, tiles, owners, total,
    value_h, gate_h, taps_h, gain_h, shift_h, w_h, go_h, mats_h, emats_h, own_h, eown_h, ft_h,
    dv, dg, dt_o, dgs_o,
    value, gate, taps, w, go, mats, emats, own, eown,
    sig_s, gw, conv, gm, gcw, tcat, ts, g_spec, spec_s, prod, lag_s,
    st1, st1_in, st2, st2_in, inv_s, colg, cols, hgain, hshift,
    gs, rs_src, rs_in, ag_src, ag, ft, gain, shift,
    meet, load_sem, w_sem, halo_send, halo_recv, tp_send, tp_recv,
    all_send, all_recv,
):
    sp = lax.axis_index("sp")
    tp = lax.axis_index("tp")
    rows, edge, side, inner_rows = plan.rows, plan.edge, plan.side, plan.inner
    channels = value.shape[1]
    width = channels * 2
    chunks = channels // CHUNK
    per = owners.per
    nxt = lax.rem(sp + 1, n)
    prv = lax.rem(sp + n - 1, n)
    has_prv = sp > 0
    has_nxt = sp < n - 1
    is_owner = (sp >= owners.first) & (sp < owners.first + owners.count) & (tp == 1)
    low_side = sp < n // 2
    crew = 1 << (max(n, 1).bit_length() // 2)
    crews = -(-n // crew)
    head = sp - lax.rem(sp, crew)
    is_head = (sp == head) & (tp == 1)

    def peer(d):
        return lax.rem(sp + d, n)

    barrier = pltpu.get_barrier_semaphore()

    inner = pl.ds(edge, rows - 2 * edge)
    sides = [pl.ds(0, edge), pl.ds(rows - edge, edge)]
    pairs = [(h.at[part], v.at[part]) for h, v in ((value_h, value), (gate_h, gate)) for part in sides]
    pairs += [(h.at[inner], v.at[inner]) for h, v in ((value_h, value), (gate_h, gate))]
    pairs += [(taps_h, taps), (ft_h, ft), (mats_h, mats), (go_h, go)]
    late = [
        (emats_h, emats), (own_h, own), (eown_h, eown), (gain_h, gain), (shift_h, shift),
    ]
    loads = [
        pltpu.make_async_copy(a, b, load_sem.at[i]) for i, (a, b) in enumerate(pairs + late)
    ]

    def w_copy(c):
        part = pl.ds(pl.multiple_of(c * CHUNK, CHUNK), CHUNK)
        return pltpu.make_async_copy(w_h.at[part], w.at[part], w_sem.at[c])

    def tell(sem, s, t):
        pl.semaphore_signal(sem, 1, device_id=(s, t), device_id_type=pl.DeviceIdType.MESH)

    members = 2 * jnp.minimum(crew, n - head)

    def each_member(sem):
        def step(i, carry):
            s, t = head + i // 2, lax.rem(i, 2)

            @pl.when((s != sp) | (t != tp))
            def _():
                tell(sem, s, t)

            return carry

        lax.fori_loop(0, members, step, 0)

    def each_head(sem):
        def step(i, carry):
            @pl.when(i * crew != sp)
            def _():
                tell(sem, i * crew, 1)

            return carry

        lax.fori_loop(0, crews, step, 0)

    tell(barrier, sp, 1 - tp)

    @pl.when(has_prv)
    def _():
        tell(barrier, prv, tp)

    @pl.when(has_nxt)
    def _():
        tell(barrier, nxt, tp)

    @pl.when(is_head)
    def _():
        each_member(barrier)
        each_head(barrier)

    for load in loads[: len(pairs)]:
        load.start()
    for c in range(chunks):
        w_copy(c).start()
    for load in loads[len(pairs):]:
        load.start()

    greeted = (
        1 + has_prv.astype(jnp.int32) + has_nxt.astype(jnp.int32)
        + jnp.where(is_head, crews - 1, 1)
    )

    def handshake_up():
        @pl.when(jnp.logical_not(is_head))
        def _():
            tell(meet.at[0], head, 1)

    def handshake_across():
        @pl.when(is_head)
        def _():
            pl.semaphore_wait(meet.at[0], members - 1)
            each_head(meet.at[1])

    def handshake_down():
        @pl.when(is_head)
        def _():
            if crews > 1:
                pl.semaphore_wait(meet.at[1], crews - 1)
            each_member(meet.at[2])

    def handshake_done():
        @pl.when(jnp.logical_not(is_head))
        def _():
            pl.semaphore_wait(meet.at[2], 1)

    def cut(c):
        return pl.ds(c * CHUNK, CHUNK)

    def gate_step(i, carry):
        part = pl.ds(pl.multiple_of(i * ALIGN, ALIGN), ALIGN)
        place = pl.ds(pl.multiple_of(i * ALIGN + edge, ALIGN), ALIGN)
        sig = sigmoid(gate[part].astype(F32))
        sig_s[part] = sig
        gw[place] = (value[part].astype(F32) * sig).astype(BF16)
        return carry

    def remote(src, dst, send, recv, device):
        return pltpu.make_async_remote_copy(
            src_ref=src, dst_ref=dst, send_sem=send, recv_sem=recv,
            device_id=device, device_id_type=pl.DeviceIdType.MESH,
        )

    def halo_pair(ref, k):
        return (
            remote(ref.at[pl.ds(rows, edge)], ref.at[pl.ds(0, edge)],
                   halo_send.at[k], halo_recv.at[k], (nxt, tp)),
            remote(ref.at[pl.ds(edge, edge)], ref.at[pl.ds(rows + edge, edge)],
                   halo_send.at[k + 1], halo_recv.at[k + 1], (prv, tp)),
        )

    def send_halo(pair):
        @pl.when(has_nxt)
        def _():
            pair[0].start()

        @pl.when(has_prv)
        def _():
            pair[1].start()

    def recv_prv(pair, ref):
        @pl.when(has_prv)
        def _():
            pair[0].wait_recv()

        @pl.when(sp == 0)
        def _():
            ref[pl.ds(0, edge)] = jnp.zeros((edge, channels), BF16)

    def recv_nxt(pair, ref):
        @pl.when(has_nxt)
        def _():
            pair[1].wait_recv()

        @pl.when(sp == n - 1)
        def _():
            ref[pl.ds(rows + edge, edge)] = jnp.zeros((edge, channels), BF16)

    def sent_halo(pair):
        @pl.when(has_nxt)
        def _():
            pair[0].wait_send()

        @pl.when(has_prv)
        def _():
            pair[1].wait_send()

    def settle(ref, count, sem):
        if count:
            part = ref.at[pl.ds(0, count)]
            pltpu.make_async_copy(part, part, sem).wait()

    gw_halo = halo_pair(gw, 0)
    gc_halo = halo_pair(gcw, 2)

    for load in loads[:4]:
        load.wait()
    sided = edge // ALIGN
    for r in range(sided):
        gate_step(r, 0)
        gate_step(rows // ALIGN - 1 - r, 0)
    pl.semaphore_wait(barrier, greeted)
    send_halo(gw_halo)
    handshake_up()
    loads[4].wait()
    loads[5].wait()
    lax.fori_loop(sided, rows // ALIGN - sided, gate_step, 0, unroll=7)
    loads[6].wait()
    loads[7].wait()

    tap = jnp.concatenate(
        [taps[...], jnp.zeros((plan.tap_rows - plan.kernel, channels), F32)], 0
    )
    tap_high = tap.astype(BF16)
    tap_low = (tap - tap_high.astype(F32)).astype(BF16)
    for k, part in enumerate((tap_high, tap_low, tap_high)):
        tcat[pl.ds(k * plan.tap_rows, plan.tap_rows)] = part

    def tap_step(_, carry):
        for c in range(chunks):
            ts[:, cut(c)] = dot(ft[...], tcat[:, cut(c)])
        return carry

    lax.fori_loop(0, 1, tap_step, 0)

    def mix(a, b):
        return lax.dot_general(a, b, (((1,), (1,)), ((), ())), preferred_element_type=F32)

    def mix_step(c, carry):
        part = pl.ds(pl.multiple_of(c * CHUNK, CHUNK), CHUNK)
        w_copy(c).wait()
        gm[:, part] = mix(go[...], w[part])
        return carry

    def fold(x):
        out = x[:, :LANES]
        for k in range(1, x.shape[1] // LANES):
            out = out + x[:, k * LANES : (k + 1) * LANES]
        return out

    lanes = lax.broadcasted_iota(jnp.int32, (ALIGN, LANES), 1) < LANES // 2

    def multiply(at, size, tap_at, sign, source):
        freqs = size // 2
        for f in range(0, freqs, ALIGN):
            high, low = pl.ds(at + f, ALIGN), pl.ds(at + freqs + f, ALIGN)
            for c in range(chunks):
                re, im = source[high, cut(c)], source[low, cut(c)]
                ta = ts[pl.ds(tap_at + f, ALIGN), cut(c)]
                tb = ts[pl.ds(tap_at + freqs + f, ALIGN), cut(c)]
                prod[high, cut(c)] = (re * ta + sign * im * tb).astype(BF16)
                other = re * tb - sign * im * ta
                prod[low, cut(c)] = (sign * other).astype(BF16)

    def slot(r):
        return r - edge if edge <= r < rows - edge else (r + inner_rows if r < edge else r)

    main_rows = list(range(edge, rows - edge, ALIGN))
    middle = len(main_rows) // 2
    first_rows, second_rows = main_rows[:middle], main_rows[middle:]
    edge_rows = list(range(0, edge, ALIGN)) + list(range(rows - edge, rows, ALIGN))

    def stats(picked):
        for r in picked:
            one = two = None
            for c in range(chunks):
                x = conv[pl.ds(r, ALIGN), cut(c)]
                p, q = fold(x), fold(x * x)
                one, two = (p, q) if c == 0 else (one + p, two + q)
            st1[pl.ds(slot(r), ALIGN)] = jnp.where(
                lanes, jnp.sum(one, 1, keepdims=True), jnp.sum(two, 1, keepdims=True)
            )

    def transform_main(source, target, at, sign):
        target[pl.ds(0, rows)] = dot(mats[pl.ds(0, rows)], source[pl.ds(edge, rows)])
        multiply(0, rows, 0, sign, target)
        conv[pl.ds(edge, inner_rows)] = dot(mats[pl.ds(at, inner_rows)], prod[pl.ds(0, rows)])

    def transform_edge(e, source, target, at, sign):
        place = rows + e * side
        window = source[pl.ds(e * (plan.wide - side), side)]
        target[pl.ds(place, side)] = dot(emats[pl.ds(0, side)], window)
        multiply(place, side, rows, sign, target)
        conv[pl.ds(e * (rows - edge), edge)] = dot(
            emats[pl.ds(at + e * edge, edge)], prod[pl.ds(place, side)]
        )

    def swap(src, dst, start, count, k):
        place = pl.ds(start, count)
        return remote(
            src.at[place], dst.at[place], tp_send.at[k], tp_recv.at[k], (sp, 1 - tp)
        )

    cutoff = middle * ALIGN
    swap1 = [
        swap(st1, st1_in, 0, inner_rows, 0), swap(st1, st1_in, inner_rows, 2 * edge, 1)
    ]
    swap2 = [
        swap(st2, st2_in, 0, cutoff, 2), swap(st2, st2_in, cutoff, inner_rows - cutoff, 3),
        swap(st2, st2_in, inner_rows, 2 * edge, 4),
    ]

    def conv_main_phase():
        transform_main(gw, g_spec, plan.at_conv, 1.0)
        stats(main_rows)

    def conv_edge_phase():
        transform_edge(0, gw, g_spec, plan.edge_conv, 1.0)
        transform_edge(1, gw, g_spec, plan.edge_conv, 1.0)
        stats(edge_rows)

    loads[8].wait()
    conv_main_phase()
    swap1[0].start()
    loads[9].wait()
    lax.fori_loop(0, chunks, mix_step, 0)
    handshake_across()
    for load in loads[10:]:
        load.wait()
    recv_prv(gw_halo, gw)
    recv_nxt(gw_halo, gw)
    conv_edge_phase()
    swap1[1].start()
    handshake_down()
    hgain[...] = jnp.broadcast_to(0.5 * gain[...], hgain.shape)
    hshift[...] = jnp.broadcast_to(0.5 * shift[...], hshift.shape)

    def twice(x):
        return jnp.concatenate([x, x], 0)

    def halves(x):
        return x[:8] + x[8:]

    def norm_at(picked, opening):
        total_g, total_s = [None] * chunks, [None] * chunks
        for r in picked:
            part, place = pl.ds(r, ALIGN), pl.ds(slot(r), ALIGN)
            tot = (st1[place] + st1_in[place]) * (1.0 / width)
            mean = tot[:, :1]
            var = tot[:, LANES // 2 : LANES // 2 + 1] - mean * mean
            inv = lax.rsqrt(var + EPS)
            inv_s[place] = jnp.broadcast_to(inv, (ALIGN, LANES))
            one = two = None
            for c in range(chunks):
                hg = twice(hgain[:, cut(c)])
                normed = (conv[part, cut(c)] - mean) * inv
                half_pre = normed * hg + twice(hshift[:, cut(c)])
                th = jnp.tanh(half_pre)
                gp = gm[part, cut(c)] * (1.0 + th) * (1.0 + half_pre * (1.0 - th))
                gn = gp * hg
                gpn = gp * normed
                conv[part, cut(c)] = normed
                gm[part, cut(c)] = gn
                p, q = fold(gn), fold(gpn * hg)
                one, two = (p, q) if c == 0 else (one + p, two + q)
                g, h = halves(gpn), halves(gp)
                if total_g[c] is not None:
                    g, h = total_g[c] + g, total_s[c] + h
                total_g[c], total_s[c] = g, h
            st2[place] = jnp.where(
                lanes, jnp.sum(one, 1, keepdims=True), jnp.sum(two, 1, keepdims=True)
            )
        for c in range(chunks):
            if opening:
                colg[:, cut(c)] = total_g[c]
                cols[:, cut(c)] = total_s[c]
            else:
                colg[:, cut(c)] += total_g[c]
                cols[:, cut(c)] += total_s[c]

    swap1[0].wait_recv()
    norm_at(first_rows, True)
    swap2[0].start()
    norm_at(second_rows, False)
    swap2[1].start()
    swap1[1].wait_recv()
    norm_at(edge_rows, False)
    swap2[2].start()

    rg = jnp.sum(colg[...], 0, keepdims=True)
    rsh = jnp.sum(cols[...], 0, keepdims=True)
    groups = channels // LANES
    gs[sp] = jnp.concatenate(
        [x[:, k * LANES : (k + 1) * LANES] for x in (rg, rsh) for k in range(groups)], 0
    ).astype(BF16)

    def send_gs(d, carry):
        remote(gs.at[sp], gs.at[sp], all_send.at[0], all_recv.at[0], (peer(d), tp)).start()
        return carry

    handshake_done()
    lax.fori_loop(1, n, send_gs, 0)

    def gc_at(picked):
        for r in picked:
            part, place = pl.ds(r, ALIGN), pl.ds(slot(r), ALIGN)
            tot = (st2[place] + st2_in[place]) * (1.0 / width)
            inv = inv_s[place]
            scaled = inv * tot
            m1 = scaled[:, :1]
            m2 = scaled[:, LANES // 2 : LANES // 2 + 1]
            inv = inv[:, :1]
            for c in range(chunks):
                gcw[pl.ds(r + edge, ALIGN), cut(c)] = (
                    inv * gm[part, cut(c)] - m1 - conv[part, cut(c)] * m2
                ).astype(BF16)

    slots = owners.count * per
    if slots > tiles:
        rs_src[pl.ds(tiles, slots - tiles)] = jnp.zeros((slots - tiles, ALIGN, LANES), BF16)
    tall = plan.tap_rows // ALIGN

    def lag_part(at, size, f, c):
        high, low = pl.ds(at + f, ALIGN), pl.ds(at + size // 2 + f, ALIGN)
        re, im = spec_s[high, cut(c)], spec_s[low, cut(c)]
        hr, hi = g_spec[high, cut(c)], g_spec[low, cut(c)]
        return hr * re + hi * im, hr * im - hi * re

    def send_rs(i, carry):
        o = jnp.where(low_side, owners.count - 1 - i, i)
        to = owners.first + o

        @pl.when((to != sp) | (tp != 1))
        def _():
            remote(rs_src.at[pl.ds(o * per, per)], rs_in.at[2 * sp + tp],
                   all_send.at[1], all_recv.at[1], (to, 1)).start()

        return carry

    def spec_main_phase():
        spec_s[pl.ds(0, rows)] = dot(own[...], gcw[pl.ds(2 * edge, inner_rows)])
        for f in range(0, rows // 2, ALIGN):
            for c in range(chunks):
                dr, di = lag_part(0, rows, f, c)
                prod[pl.ds(f, ALIGN), cut(c)] = dr.astype(BF16)
                prod[pl.ds(rows // 2 + f, ALIGN), cut(c)] = di.astype(BF16)
        lag_s[...] = (
            dot(mats[pl.ds(plan.at_lags, plan.tap_rows)], prod[pl.ds(0, rows)])
            * plan.lag_scale[0]
        )

    def spec_edge_phase():
        for e in range(2):
            spec_s[pl.ds(rows + e * side, side)] = dot(
                eown[pl.ds(e * side, side)], gcw[pl.ds(edge + e * (rows - edge), edge)]
            )
        for f in range(0, side // 2, ALIGN):
            for c in range(chunks):
                r0, i0 = lag_part(rows, side, f, c)
                r1, i1 = lag_part(rows + side, side, f, c)
                prod[pl.ds(rows + f, ALIGN), cut(c)] = (r0 + r1).astype(BF16)
                prod[pl.ds(rows + side // 2 + f, ALIGN), cut(c)] = (i0 + i1).astype(BF16)
        out = lag_s[...] + plan.lag_scale[1] * dot(
            emats[pl.ds(plan.edge_lags, plan.tap_rows)], prod[pl.ds(rows, side)]
        )
        out = out.astype(BF16)
        for r in range(tall):
            for k in range(groups):
                rs_src[k * tall + r] = out[
                    r * ALIGN : (r + 1) * ALIGN, k * LANES : (k + 1) * LANES
                ]

    swap2[0].wait_recv()
    gc_at(first_rows)
    swap2[1].wait_recv()
    gc_at(second_rows)
    spec_main_phase()
    swap2[2].wait_recv()
    gc_at(edge_rows)
    spec_edge_phase()
    lax.fori_loop(0, owners.count, send_rs, 0)
    send_halo(gc_halo)

    def sum_phase():
        @pl.when(is_owner)
        def _():
            o = sp - owners.first
            rs_in[2 * sp + 1] = rs_src[pl.ds(o * per, per)]
            settle(rs_in, 2 * n - 1, all_recv.at[1])
            zero = jnp.zeros((2, per, ALIGN, LANES), F32)
            summed = lax.fori_loop(
                0, n, lambda i, t: t + rs_in[pl.ds(2 * i, 2)].astype(F32), zero, unroll=4
            )
            ag_src[...] = summed.astype(BF16)
            ag[o] = ag_src[1]

    def gather_phase(first, count):
        @pl.when(is_owner)
        def _():
            o = sp - owners.first

            def send_ag(i, carry):
                for t in range(2):
                    @pl.when((i != sp) | (t != 1))
                    def _():
                        remote(ag_src.at[t], ag.at[o],
                               all_send.at[2], all_recv.at[2], (i, t)).start()

                return carry

            lax.fori_loop(first, first + count, send_ag, 0)

    def finish(picked):
        for r in picked:
            part = pl.ds(r, ALIGN)
            for c in range(chunks):
                sig = sig_s[part, cut(c)]
                left = conv[part, cut(c)] * sig
                dv[part, cut(c)] = left.astype(BF16)
                dg[part, cut(c)] = (
                    left * value[part, cut(c)].astype(F32) * (1.0 - sig)
                ).astype(BF16)

    def out_main_phase():
        transform_main(gcw, spec_s, plan.at_grad, -1.0)
        finish(main_rows)

    def out_edge_phase():
        transform_edge(0, gcw, spec_s, plan.edge_grad, -1.0)
        transform_edge(1, gcw, spec_s, plan.edge_grad, -1.0)
        finish(edge_rows)

    out_main_phase()
    sum_phase()
    gather_phase(0, 1)
    gather_phase(1, n - 1)
    recv_prv(gc_halo, gcw)
    recv_nxt(gc_halo, gcw)
    out_edge_phase()
    settle(gs, n - 1, all_recv.at[0])
    small = lax.fori_loop(
        0, n, lambda i, t: t + gs[i].astype(F32), jnp.zeros(gs.shape[1:], F32)
    )
    dgs_o[...] = small * (0.5 / math.sqrt(total))

    sent_halo(gw_halo)
    sent_halo(gc_halo)
    for each in swap1 + swap2:
        each.wait_send()
    settle(gs, n - 1, all_send.at[0])

    @pl.when(is_owner)
    def _():
        settle(rs_in, owners.count - 1, all_send.at[1])
        settle(ag, owners.count - 1, all_recv.at[2])

    @pl.when(jnp.logical_not(is_owner))
    def _():
        settle(rs_in, owners.count, all_send.at[1])
        settle(ag, owners.count, all_recv.at[2])

    for t in range(tiles):
        k, r = t // tall, t % tall
        count = min(ALIGN, plan.kernel - r * ALIGN)
        dt_o[pl.ds(r * ALIGN, count), pl.ds(k * LANES, LANES)] = ag[t // per, t % per].astype(F32)[
            :count
        ]

    @pl.when(is_owner)
    def _():
        settle(rs_in, 2 * n - 1, all_send.at[2])


def store(*refs):
    sources, targets, out_sem = refs[:4], refs[4:9], refs[9]
    groups = sources[3].shape[0] // 2
    views = list(sources[:3]) + [
        sources[3].at[pl.ds(0, groups)], sources[3].at[pl.ds(groups, groups)]
    ]
    copies = [
        pltpu.make_async_copy(a, b, out_sem.at[i]) for i, (a, b) in enumerate(zip(views, targets))
    ]
    for copy in copies:
        copy.start()
    for copy in copies:
        copy.wait()


def shards(n, value_in, gate_in, taps, gain, shift, w_out, grad_out):
    rows, channels = value_in.shape
    kernel = taps.shape[0]
    total = rows * n
    plan = Plan(rows, kernel, total)
    groups = channels // LANES
    tiles = plan.tap_rows // ALIGN * groups
    owners = Owners(n, tiles)
    per = owners.per
    model = grad_out.shape[1]
    mats = jnp.asarray(plan.main, BF16)
    emats = jnp.asarray(plan.edges, BF16)
    own = jnp.asarray(plan.own, BF16)
    eown = jnp.asarray(plan.own_edges, BF16)
    ft = jnp.asarray(plan.taps, BF16)
    hbm = pl.BlockSpec(memory_space=pltpu.HBM)
    vmem = pl.BlockSpec(memory_space=pltpu.VMEM)
    both = rows + 2 * plan.side
    chunks = channels // CHUNK
    dma = pltpu.SemaphoreType.DMA
    results = pl.pallas_call(
        functools.partial(body, plan, n, tiles, owners, total),
        out_shape=(
            pltpu.VMEM((rows, channels), BF16),
            pltpu.VMEM((rows, channels), BF16),
            pltpu.VMEM((kernel, channels), F32),
            pltpu.VMEM((2 * groups, LANES), F32),
        ),
        in_specs=[hbm] * 12,
        out_specs=(vmem,) * 4,
        scratch_shapes=[
            pltpu.VMEM((rows, channels), BF16),
            pltpu.VMEM((rows, channels), BF16),
            pltpu.VMEM((kernel, channels), F32),
            pltpu.VMEM((channels, model), BF16),
            pltpu.VMEM((rows, model), BF16),
            pltpu.VMEM(plan.main.shape, BF16),
            pltpu.VMEM(plan.edges.shape, BF16),
            pltpu.VMEM(plan.own.shape, BF16),
            pltpu.VMEM(plan.own_edges.shape, BF16),
            pltpu.VMEM((rows, channels), F32),
            pltpu.VMEM((plan.wide, channels), BF16),
            pltpu.VMEM((rows, channels), F32),
            pltpu.VMEM((rows, channels), F32),
            pltpu.VMEM((plan.wide, channels), BF16),
            pltpu.VMEM((3 * plan.tap_rows, channels), BF16),
            pltpu.VMEM((rows + plan.side, channels), F32),
            pltpu.VMEM((both, channels), F32),
            pltpu.VMEM((both, channels), F32),
            pltpu.VMEM((both, channels), BF16),
            pltpu.VMEM((plan.tap_rows, channels), F32),
            pltpu.VMEM((rows, LANES), F32),
            pltpu.VMEM((rows, LANES), F32),
            pltpu.VMEM((rows, LANES), F32),
            pltpu.VMEM((rows, LANES), F32),
            pltpu.VMEM((rows, LANES), F32),
            pltpu.VMEM((8, channels), F32),
            pltpu.VMEM((8, channels), F32),
            pltpu.VMEM((8, channels), F32),
            pltpu.VMEM((8, channels), F32),
            pltpu.VMEM((n, 2 * groups, LANES), BF16),
            pltpu.VMEM((owners.count * per, ALIGN, LANES), BF16),
            pltpu.VMEM((2 * n, per, ALIGN, LANES), BF16),
            pltpu.VMEM((2, per, ALIGN, LANES), BF16),
            pltpu.VMEM((owners.count, per, ALIGN, LANES), BF16),
            pltpu.VMEM(plan.taps.shape, BF16),
            pltpu.VMEM((1, channels), F32),
            pltpu.VMEM((1, channels), F32),
            pltpu.SemaphoreType.REGULAR((3,)),
            dma((15,)), dma((chunks,)), dma((4,)), dma((4,)),
            dma((5,)), dma((5,)), dma((3,)), dma((3,)),
        ],
        compiler_params=pltpu.CompilerParams(
            collective_id=0, has_side_effects=True, vmem_limit_bytes=VMEM_GRANT
        ),
    )(
        *(
            pltpu.with_memory_space_constraint(x, pltpu.HBM)
            for x in (
                value_in, gate_in, taps, gain.reshape(1, -1), shift.reshape(1, -1), w_out,
                grad_out, mats, emats, own, eown, ft,
            )
        )
    )
    results = [pltpu.with_memory_space_constraint(x, pltpu.VMEM) for x in results]
    d_value, d_gate, d_taps, d_gain, d_shift = pl.pallas_call(
        store,
        out_shape=(
            jax.ShapeDtypeStruct((rows, channels), BF16),
            jax.ShapeDtypeStruct((rows, channels), BF16),
            jax.ShapeDtypeStruct((kernel, channels), F32),
            jax.ShapeDtypeStruct((groups, LANES), F32),
            jax.ShapeDtypeStruct((groups, LANES), F32),
        ),
        in_specs=[vmem] * 4,
        out_specs=(hbm,) * 5,
        scratch_shapes=[dma((5,))],
        compiler_params=pltpu.CompilerParams(vmem_limit_bytes=8 * 1024 * 1024),
    )(*results)
    return (d_value, d_gate, d_taps, d_gain.reshape(-1), d_shift.reshape(-1))


def solution(mesh):
    return jax.shard_map(
        functools.partial(shards, mesh.shape["sp"]),
        mesh=mesh,
        in_specs=(
            P("sp", "tp"),
            P("sp", "tp"),
            P(None, "tp"),
            P("tp"),
            P("tp"),
            P("tp", None),
            P("sp", None),
        ),
        out_specs=(P("sp", "tp"), P("sp", "tp"), P(None, "tp"), P("tp"), P("tp")),
        check_vma=False,
    )
```

```python
import functools
import math

import jax
import jax.numpy as jnp
import numpy as np
from jax import lax
from jax.experimental import pallas as pl
from jax.experimental.pallas import tpu as pltpu
from jax.sharding import PartitionSpec as P

EPS = 1e-05
ALIGN = 16
LANES = 128
CHUNK = 256
VMEM_GRANT = 48 * 1024 * 1024
F32 = jnp.float32
BF16 = jnp.bfloat16


class Plan:
    def __init__(self, rows, kernel, total):
        self.half = half = kernel // 2
        self.kernel = kernel
        self.rows = rows
        self.edge = edge = -(-half // ALIGN) * ALIGN
        self.side = side = 4 * edge
        self.inner = rows - 2 * edge
        self.wide = rows + 2 * edge
        self.tap_rows = -(-kernel // ALIGN) * ALIGN

        def omega(size):
            return 2.0 * np.pi * (np.arange(size // 2) + 0.5) / size

        def spectrum(size, times):
            angle = omega(size)[:, None] * times[None, :]
            return np.concatenate([np.cos(angle), np.sin(angle)], 0)

        def inverse(size, times):
            angle = times[:, None] * omega(size)[None, :]
            return np.concatenate([np.cos(angle), -np.sin(angle)], 1)

        def lags(size):
            out = inverse(size, np.arange(self.tap_rows) - half)
            out[kernel:] = 0.0
            return out

        main = np.arange(self.inner) + edge
        top = np.arange(edge) + edge
        low = np.arange(edge) + side - 2 * edge
        self.main = np.concatenate(
            [
                spectrum(rows, np.arange(rows)), inverse(rows, main - half),
                inverse(rows, main + half), lags(rows),
            ],
            0,
        )
        self.at_conv = rows
        self.at_grad = self.at_conv + self.inner
        self.at_lags = self.at_grad + self.inner
        self.edges = np.concatenate(
            [spectrum(side, np.arange(side))]
            + [inverse(side, part + shift) for shift in (-half, half) for part in (top, low)]
            + [lags(side)],
            0,
        )
        self.edge_conv = side
        self.edge_grad = side + 2 * edge
        self.edge_lags = side + 4 * edge
        self.own = spectrum(rows, main)
        self.own_edges = np.concatenate([spectrum(side, top), spectrum(side, low)], 0)
        taps = np.zeros((rows + side, self.tap_rows))
        times = np.arange(kernel)
        taps[:rows, :kernel] = spectrum(rows, times) * (2.0 / rows)
        taps[rows:, :kernel] = spectrum(side, times) * (2.0 / side)
        high = taps.astype(jnp.bfloat16)
        low_part = taps - high.astype(np.float64)
        self.taps = np.concatenate([high.astype(np.float64), high.astype(np.float64), low_part], 1)
        self.lag_scale = [2.0 / size / math.sqrt(total) for size in (rows, side)]


class Owners:
    def __init__(self, n, tiles):
        self.count = max(1, min(n // 2, tiles))
        self.per = -(-tiles // self.count)
        self.first = (n - self.count) // 2


def dot(a, b):
    return jnp.dot(a, b, preferred_element_type=F32)


def sigmoid(x):
    return 0.5 * jnp.tanh(0.5 * x) + 0.5


def body(
    plan, n, tiles, owners, total,
    value_h, gate_h, taps_h, gain_h, shift_h, w_h, go_h, mats_h, emats_h, own_h, eown_h, ft_h,
    dv, dg, dt_o, dgs_o,
    value, gate, taps, w, go, mats, emats, own, eown,
    sig_s, gw, conv, gm, gcw, tcat, ts, g_spec, spec_s, prod, lag_s,
    st1, st1_in, st2, st2_in, inv_s, colg, cols, hgain, hshift,
    gs, rs_src, rs_in, ag_src, ag, ft, gain, shift,
    meet, load_sem, w_sem, halo_send, halo_recv, tp_send, tp_recv,
    all_send, all_recv,
):
    sp = lax.axis_index("sp")
    tp = lax.axis_index("tp")
    rows, edge, side, inner_rows = plan.rows, plan.edge, plan.side, plan.inner
    channels = value.shape[1]
    width = channels * 2
    chunks = channels // CHUNK
    per = owners.per
    nxt = lax.rem(sp + 1, n)
    prv = lax.rem(sp + n - 1, n)
    has_prv = sp > 0
    has_nxt = sp < n - 1
    is_owner = (sp >= owners.first) & (sp < owners.first + owners.count) & (tp == 1)
    low_side = sp < n // 2
    crew = 1 << (max(n, 1).bit_length() // 2)
    crews = -(-n // crew)
    head = sp - lax.rem(sp, crew)
    is_head = (sp == head) & (tp == 1)

    def peer(d):
        return lax.rem(sp + d, n)

    barrier = pltpu.get_barrier_semaphore()

    inner = pl.ds(edge, rows - 2 * edge)
    sides = [pl.ds(0, edge), pl.ds(rows - edge, edge)]
    pairs = [(h.at[part], v.at[part]) for h, v in ((value_h, value), (gate_h, gate)) for part in sides]
    pairs += [(h.at[inner], v.at[inner]) for h, v in ((value_h, value), (gate_h, gate))]
    pairs += [(taps_h, taps), (ft_h, ft), (mats_h, mats), (go_h, go)]
    late = [
        (emats_h, emats), (own_h, own), (eown_h, eown), (gain_h, gain), (shift_h, shift),
    ]
    loads = [
        pltpu.make_async_copy(a, b, load_sem.at[i]) for i, (a, b) in enumerate(pairs + late)
    ]

    def w_copy(c):
        part = pl.ds(pl.multiple_of(c * CHUNK, CHUNK), CHUNK)
        return pltpu.make_async_copy(w_h.at[part], w.at[part], w_sem.at[c])

    def tell(sem, s, t):
        pl.semaphore_signal(sem, 1, device_id=(s, t), device_id_type=pl.DeviceIdType.MESH)

    members = 2 * jnp.minimum(crew, n - head)

    def each_member(sem):
        def step(i, carry):
            s, t = head + i // 2, lax.rem(i, 2)

            @pl.when((s != sp) | (t != tp))
            def _():
                tell(sem, s, t)

            return carry

        lax.fori_loop(0, members, step, 0)

    def each_head(sem):
        def step(i, carry):
            @pl.when(i * crew != sp)
            def _():
                tell(sem, i * crew, 1)

            return carry

        lax.fori_loop(0, crews, step, 0)

    tell(barrier, sp, 1 - tp)

    @pl.when(has_prv)
    def _():
        tell(barrier, prv, tp)

    @pl.when(has_nxt)
    def _():
        tell(barrier, nxt, tp)

    @pl.when(is_head)
    def _():
        each_member(barrier)
        each_head(barrier)

    for load in loads[: len(pairs)]:
        load.start()
    for c in range(chunks):
        w_copy(c).start()
    for load in loads[len(pairs):]:
        load.start()

    greeted = (
        1 + has_prv.astype(jnp.int32) + has_nxt.astype(jnp.int32)
        + jnp.where(is_head, crews - 1, 1)
    )

    def handshake_up():
        @pl.when(jnp.logical_not(is_head))
        def _():
            tell(meet.at[0], head, 1)

    def handshake_across():
        @pl.when(is_head)
        def _():
            pl.semaphore_wait(meet.at[0], members - 1)
            each_head(meet.at[1])

    def handshake_down():
        @pl.when(is_head)
        def _():
            if crews > 1:
                pl.semaphore_wait(meet.at[1], crews - 1)
            each_member(meet.at[2])

    def handshake_done():
        @pl.when(jnp.logical_not(is_head))
        def _():
            pl.semaphore_wait(meet.at[2], 1)

    def cut(c):
        return pl.ds(c * CHUNK, CHUNK)

    def gate_step(i, carry):
        part = pl.ds(pl.multiple_of(i * ALIGN, ALIGN), ALIGN)
        place = pl.ds(pl.multiple_of(i * ALIGN + edge, ALIGN), ALIGN)
        sig = sigmoid(gate[part].astype(F32))
        sig_s[part] = sig
        gw[place] = (value[part].astype(F32) * sig).astype(BF16)
        return carry

    def remote(src, dst, send, recv, device):
        return pltpu.make_async_remote_copy(
            src_ref=src, dst_ref=dst, send_sem=send, recv_sem=recv,
            device_id=device, device_id_type=pl.DeviceIdType.MESH,
        )

    def halo_pair(ref, k):
        return (
            remote(ref.at[pl.ds(rows, edge)], ref.at[pl.ds(0, edge)],
                   halo_send.at[k], halo_recv.at[k], (nxt, tp)),
            remote(ref.at[pl.ds(edge, edge)], ref.at[pl.ds(rows + edge, edge)],
                   halo_send.at[k + 1], halo_recv.at[k + 1], (prv, tp)),
        )

    def send_halo(pair):
        @pl.when(has_nxt)
        def _():
            pair[0].start()

        @pl.when(has_prv)
        def _():
            pair[1].start()

    def recv_prv(pair, ref):
        @pl.when(has_prv)
        def _():
            pair[0].wait_recv()

        @pl.when(sp == 0)
        def _():
            ref[pl.ds(0, edge)] = jnp.zeros((edge, channels), BF16)

    def recv_nxt(pair, ref):
        @pl.when(has_nxt)
        def _():
            pair[1].wait_recv()

        @pl.when(sp == n - 1)
        def _():
            ref[pl.ds(rows + edge, edge)] = jnp.zeros((edge, channels), BF16)

    def sent_halo(pair):
        @pl.when(has_nxt)
        def _():
            pair[0].wait_send()

        @pl.when(has_prv)
        def _():
            pair[1].wait_send()

    def settle(ref, count, sem):
        if count:
            part = ref.at[pl.ds(0, count)]
            pltpu.make_async_copy(part, part, sem).wait()

    gw_halo = halo_pair(gw, 0)
    gc_halo = halo_pair(gcw, 2)

    for load in loads[:4]:
        load.wait()
    sided = edge // ALIGN
    for r in range(sided):
        gate_step(r, 0)
        gate_step(rows // ALIGN - 1 - r, 0)
    pl.semaphore_wait(barrier, greeted)
    send_halo(gw_halo)
    handshake_up()
    loads[4].wait()
    loads[5].wait()
    lax.fori_loop(sided, rows // ALIGN - sided, gate_step, 0, unroll=7)
    loads[6].wait()
    loads[7].wait()

    tap = jnp.concatenate(
        [taps[...], jnp.zeros((plan.tap_rows - plan.kernel, channels), F32)], 0
    )
    tap_high = tap.astype(BF16)
    tap_low = (tap - tap_high.astype(F32)).astype(BF16)
    for k, part in enumerate((tap_high, tap_low, tap_high)):
        tcat[pl.ds(k * plan.tap_rows, plan.tap_rows)] = part

    def tap_step(_, carry):
        for c in range(chunks):
            ts[:, cut(c)] = dot(ft[...], tcat[:, cut(c)])
        return carry

    lax.fori_loop(0, 1, tap_step, 0)

    def mix(a, b):
        return lax.dot_general(a, b, (((1,), (1,)), ((), ())), preferred_element_type=F32)

    def mix_step(c, carry):
        part = pl.ds(pl.multiple_of(c * CHUNK, CHUNK), CHUNK)
        w_copy(c).wait()
        gm[:, part] = mix(go[...], w[part])
        return carry

    def fold(x):
        out = x[:, :LANES]
        for k in range(1, x.shape[1] // LANES):
            out = out + x[:, k * LANES : (k + 1) * LANES]
        return out

    lanes = lax.broadcasted_iota(jnp.int32, (ALIGN, LANES), 1) < LANES // 2

    def multiply(at, size, tap_at, sign, source):
        freqs = size // 2
        for f in range(0, freqs, ALIGN):
            high, low = pl.ds(at + f, ALIGN), pl.ds(at + freqs + f, ALIGN)
            for c in range(chunks):
                re, im = source[high, cut(c)], source[low, cut(c)]
                ta = ts[pl.ds(tap_at + f, ALIGN), cut(c)]
                tb = ts[pl.ds(tap_at + freqs + f, ALIGN), cut(c)]
                prod[high, cut(c)] = (re * ta + sign * im * tb).astype(BF16)
                other = re * tb - sign * im * ta
                prod[low, cut(c)] = (sign * other).astype(BF16)

    def slot(r):
        return r - edge if edge <= r < rows - edge else (r + inner_rows if r < edge else r)

    main_rows = list(range(edge, rows - edge, ALIGN))
    middle = len(main_rows) // 2
    first_rows, second_rows = main_rows[:middle], main_rows[middle:]
    edge_rows = list(range(0, edge, ALIGN)) + list(range(rows - edge, rows, ALIGN))

    def stats(picked):
        for r in picked:
            one = two = None
            for c in range(chunks):
                x = conv[pl.ds(r, ALIGN), cut(c)]
                p, q = fold(x), fold(x * x)
                one, two = (p, q) if c == 0 else (one + p, two + q)
            st1[pl.ds(slot(r), ALIGN)] = jnp.where(
                lanes, jnp.sum(one, 1, keepdims=True), jnp.sum(two, 1, keepdims=True)
            )

    def transform_main(source, target, at, sign):
        target[pl.ds(0, rows)] = dot(mats[pl.ds(0, rows)], source[pl.ds(edge, rows)])
        multiply(0, rows, 0, sign, target)
        conv[pl.ds(edge, inner_rows)] = dot(mats[pl.ds(at, inner_rows)], prod[pl.ds(0, rows)])

    def transform_edges(source, target, at, sign):
        for e in range(2):
            window = source[pl.ds(e * (plan.wide - side), side)]
            target[pl.ds(rows + e * side, side)] = dot(emats[pl.ds(0, side)], window)
        for e in range(2):
            multiply(rows + e * side, side, rows, sign, target)
        for e in range(2):
            conv[pl.ds(e * (rows - edge), edge)] = dot(
                emats[pl.ds(at + e * edge, edge)], prod[pl.ds(rows + e * side, side)]
            )

    def swap(src, dst, start, count, k):
        place = pl.ds(start, count)
        return remote(
            src.at[place], dst.at[place], tp_send.at[k], tp_recv.at[k], (sp, 1 - tp)
        )

    cutoff = middle * ALIGN
    swap1 = [
        swap(st1, st1_in, 0, inner_rows, 0), swap(st1, st1_in, inner_rows, 2 * edge, 1)
    ]
    swap2 = [
        swap(st2, st2_in, 0, cutoff, 2), swap(st2, st2_in, cutoff, inner_rows - cutoff, 3),
        swap(st2, st2_in, inner_rows, 2 * edge, 4),
    ]

    def conv_main_phase():
        transform_main(gw, g_spec, plan.at_conv, 1.0)
        stats(main_rows)

    def conv_edge_phase():
        transform_edges(gw, g_spec, plan.edge_conv, 1.0)
        stats(edge_rows)

    loads[8].wait()
    conv_main_phase()
    swap1[0].start()
    handshake_across()
    loads[9].wait()
    lax.fori_loop(0, chunks, mix_step, 0)
    for load in loads[10:]:
        load.wait()
    hgain[...] = jnp.broadcast_to(0.5 * gain[...], hgain.shape)
    hshift[...] = jnp.broadcast_to(0.5 * shift[...], hshift.shape)

    def twice(x):
        return jnp.concatenate([x, x], 0)

    def halves(x):
        return x[:8] + x[8:]

    def norm_at(picked, opening):
        total_g, total_s = [None] * chunks, [None] * chunks
        for r in picked:
            part, place = pl.ds(r, ALIGN), pl.ds(slot(r), ALIGN)
            tot = (st1[place] + st1_in[place]) * (1.0 / width)
            mean = tot[:, :1]
            var = tot[:, LANES // 2 : LANES // 2 + 1] - mean * mean
            inv = lax.rsqrt(var + EPS)
            inv_s[place] = jnp.broadcast_to(inv, (ALIGN, LANES))
            one = two = None
            for c in range(chunks):
                hg = twice(hgain[:, cut(c)])
                normed = (conv[part, cut(c)] - mean) * inv
                half_pre = normed * hg + twice(hshift[:, cut(c)])
                th = jnp.tanh(half_pre)
                gp = gm[part, cut(c)] * (1.0 + th) * (1.0 + half_pre * (1.0 - th))
                gn = gp * hg
                gpn = gp * normed
                conv[part, cut(c)] = normed
                gm[part, cut(c)] = gn
                p, q = fold(gn), fold(gpn * hg)
                one, two = (p, q) if c == 0 else (one + p, two + q)
                g, h = halves(gpn), halves(gp)
                if total_g[c] is not None:
                    g, h = total_g[c] + g, total_s[c] + h
                total_g[c], total_s[c] = g, h
            st2[place] = jnp.where(
                lanes, jnp.sum(one, 1, keepdims=True), jnp.sum(two, 1, keepdims=True)
            )
        for c in range(chunks):
            if opening:
                colg[:, cut(c)] = total_g[c]
                cols[:, cut(c)] = total_s[c]
            else:
                colg[:, cut(c)] += total_g[c]
                cols[:, cut(c)] += total_s[c]

    def gc_at(picked):
        for r in picked:
            part, place = pl.ds(r, ALIGN), pl.ds(slot(r), ALIGN)
            tot = (st2[place] + st2_in[place]) * (1.0 / width)
            inv = inv_s[place]
            scaled = inv * tot
            m1 = scaled[:, :1]
            m2 = scaled[:, LANES // 2 : LANES // 2 + 1]
            inv = inv[:, :1]
            for c in range(chunks):
                gcw[pl.ds(r + edge, ALIGN), cut(c)] = (
                    inv * gm[part, cut(c)] - m1 - conv[part, cut(c)] * m2
                ).astype(BF16)

    swap1[0].wait_recv()
    norm_at(first_rows, True)
    swap2[0].start()
    recv_prv(gw_halo, gw)
    recv_nxt(gw_halo, gw)
    conv_edge_phase()
    swap1[1].start()
    handshake_down()
    norm_at(second_rows, False)
    swap2[1].start()
    swap2[0].wait_recv()
    gc_at(first_rows)
    swap1[1].wait_recv()
    norm_at(edge_rows, False)
    swap2[2].start()

    rg = jnp.sum(colg[...], 0, keepdims=True)
    rsh = jnp.sum(cols[...], 0, keepdims=True)
    groups = channels // LANES
    gs[sp] = jnp.concatenate(
        [x[:, k * LANES : (k + 1) * LANES] for x in (rg, rsh) for k in range(groups)], 0
    ).astype(BF16)

    def send_gs(d, carry):
        remote(gs.at[sp], gs.at[sp], all_send.at[0], all_recv.at[0], (peer(d), tp)).start()
        return carry

    handshake_done()
    lax.fori_loop(1, n, send_gs, 0)

    slots = owners.count * per
    if slots > tiles:
        rs_src[pl.ds(tiles, slots - tiles)] = jnp.zeros((slots - tiles, ALIGN, LANES), BF16)
    tall = plan.tap_rows // ALIGN

    def lag_part(at, size, f, c):
        high, low = pl.ds(at + f, ALIGN), pl.ds(at + size // 2 + f, ALIGN)
        re, im = spec_s[high, cut(c)], spec_s[low, cut(c)]
        hr, hi = g_spec[high, cut(c)], g_spec[low, cut(c)]
        return hr * re + hi * im, hr * im - hi * re

    def send_rs(i, carry):
        o = jnp.where(low_side, owners.count - 1 - i, i)
        to = owners.first + o

        @pl.when((to != sp) | (tp != 1))
        def _():
            remote(rs_src.at[pl.ds(o * per, per)], rs_in.at[2 * sp + tp],
                   all_send.at[1], all_recv.at[1], (to, 1)).start()

        return carry

    def spec_main_phase():
        spec_s[pl.ds(0, rows)] = dot(own[...], gcw[pl.ds(2 * edge, inner_rows)])
        for f in range(0, rows // 2, ALIGN):
            for c in range(chunks):
                dr, di = lag_part(0, rows, f, c)
                prod[pl.ds(f, ALIGN), cut(c)] = dr.astype(BF16)
                prod[pl.ds(rows // 2 + f, ALIGN), cut(c)] = di.astype(BF16)
        lag_s[...] = (
            dot(mats[pl.ds(plan.at_lags, plan.tap_rows)], prod[pl.ds(0, rows)])
            * plan.lag_scale[0]
        )

    def spec_edge_phase():
        for e in range(2):
            spec_s[pl.ds(rows + e * side, side)] = dot(
                eown[pl.ds(e * side, side)], gcw[pl.ds(edge + e * (rows - edge), edge)]
            )
        for f in range(0, side // 2, ALIGN):
            for c in range(chunks):
                r0, i0 = lag_part(rows, side, f, c)
                r1, i1 = lag_part(rows + side, side, f, c)
                prod[pl.ds(rows + f, ALIGN), cut(c)] = (r0 + r1).astype(BF16)
                prod[pl.ds(rows + side // 2 + f, ALIGN), cut(c)] = (i0 + i1).astype(BF16)
        out = lag_s[...] + plan.lag_scale[1] * dot(
            emats[pl.ds(plan.edge_lags, plan.tap_rows)], prod[pl.ds(rows, side)]
        )
        out = out.astype(BF16)
        for r in range(tall):
            for k in range(groups):
                rs_src[k * tall + r] = out[
                    r * ALIGN : (r + 1) * ALIGN, k * LANES : (k + 1) * LANES
                ]

    swap2[1].wait_recv()
    gc_at(second_rows)
    spec_main_phase()
    swap2[2].wait_recv()
    gc_at(edge_rows)
    spec_edge_phase()
    lax.fori_loop(0, owners.count, send_rs, 0)
    send_halo(gc_halo)

    def sum_phase():
        @pl.when(is_owner)
        def _():
            o = sp - owners.first
            rs_in[2 * sp + 1] = rs_src[pl.ds(o * per, per)]
            settle(rs_in, 2 * n - 1, all_recv.at[1])
            zero = jnp.zeros((2, per, ALIGN, LANES), F32)
            summed = lax.fori_loop(
                0, n, lambda i, t: t + rs_in[pl.ds(2 * i, 2)].astype(F32), zero, unroll=4
            )
            ag_src[...] = summed.astype(BF16)
            ag[o] = ag_src[1]

    def gather_phase(first, count):
        @pl.when(is_owner)
        def _():
            o = sp - owners.first

            def send_ag(i, carry):
                for t in range(2):
                    @pl.when((i != sp) | (t != 1))
                    def _():
                        remote(ag_src.at[t], ag.at[o],
                               all_send.at[2], all_recv.at[2], (i, t)).start()

                return carry

            lax.fori_loop(first, first + count, send_ag, 0)

    def finish(picked):
        for r in picked:
            part = pl.ds(r, ALIGN)
            for c in range(chunks):
                sig = sig_s[part, cut(c)]
                left = conv[part, cut(c)] * sig
                dv[part, cut(c)] = left.astype(BF16)
                dg[part, cut(c)] = (
                    left * value[part, cut(c)].astype(F32) * (1.0 - sig)
                ).astype(BF16)

    def out_main_phase():
        transform_main(gcw, spec_s, plan.at_grad, -1.0)
        finish(main_rows)

    def out_edge_phase():
        transform_edges(gcw, spec_s, plan.edge_grad, -1.0)
        finish(edge_rows)

    out_main_phase()
    sum_phase()
    gather_phase(0, 1)
    gather_phase(1, n - 1)
    recv_prv(gc_halo, gcw)
    recv_nxt(gc_halo, gcw)
    out_edge_phase()
    settle(gs, n - 1, all_recv.at[0])
    small = lax.fori_loop(
        0, n, lambda i, t: t + gs[i].astype(F32), jnp.zeros(gs.shape[1:], F32)
    )
    dgs_o[...] = small * (0.5 / math.sqrt(total))

    sent_halo(gw_halo)
    sent_halo(gc_halo)
    for each in swap1 + swap2:
        each.wait_send()
    settle(gs, n - 1, all_send.at[0])

    @pl.when(is_owner)
    def _():
        settle(rs_in, owners.count - 1, all_send.at[1])
        settle(ag, owners.count - 1, all_recv.at[2])

    @pl.when(jnp.logical_not(is_owner))
    def _():
        settle(rs_in, owners.count, all_send.at[1])
        settle(ag, owners.count, all_recv.at[2])

    for t in range(tiles):
        k, r = t // tall, t % tall
        count = min(ALIGN, plan.kernel - r * ALIGN)
        dt_o[pl.ds(r * ALIGN, count), pl.ds(k * LANES, LANES)] = ag[t // per, t % per].astype(F32)[
            :count
        ]

    @pl.when(is_owner)
    def _():
        settle(rs_in, 2 * n - 1, all_send.at[2])


def store(*refs):
    sources, targets, out_sem = refs[:4], refs[4:9], refs[9]
    groups = sources[3].shape[0] // 2
    views = list(sources[:3]) + [
        sources[3].at[pl.ds(0, groups)], sources[3].at[pl.ds(groups, groups)]
    ]
    copies = [
        pltpu.make_async_copy(a, b, out_sem.at[i]) for i, (a, b) in enumerate(zip(views, targets))
    ]
    for copy in copies:
        copy.start()
    for copy in copies:
        copy.wait()


def shards(n, value_in, gate_in, taps, gain, shift, w_out, grad_out):
    rows, channels = value_in.shape
    kernel = taps.shape[0]
    total = rows * n
    plan = Plan(rows, kernel, total)
    groups = channels // LANES
    tiles = plan.tap_rows // ALIGN * groups
    owners = Owners(n, tiles)
    per = owners.per
    model = grad_out.shape[1]
    mats = jnp.asarray(plan.main, BF16)
    emats = jnp.asarray(plan.edges, BF16)
    own = jnp.asarray(plan.own, BF16)
    eown = jnp.asarray(plan.own_edges, BF16)
    ft = jnp.asarray(plan.taps, BF16)
    hbm = pl.BlockSpec(memory_space=pltpu.HBM)
    vmem = pl.BlockSpec(memory_space=pltpu.VMEM)
    both = rows + 2 * plan.side
    chunks = channels // CHUNK
    dma = pltpu.SemaphoreType.DMA
    results = pl.pallas_call(
        functools.partial(body, plan, n, tiles, owners, total),
        out_shape=(
            pltpu.VMEM((rows, channels), BF16),
            pltpu.VMEM((rows, channels), BF16),
            pltpu.VMEM((kernel, channels), F32),
            pltpu.VMEM((2 * groups, LANES), F32),
        ),
        in_specs=[hbm] * 12,
        out_specs=(vmem,) * 4,
        scratch_shapes=[
            pltpu.VMEM((rows, channels), BF16),
            pltpu.VMEM((rows, channels), BF16),
            pltpu.VMEM((kernel, channels), F32),
            pltpu.VMEM((channels, model), BF16),
            pltpu.VMEM((rows, model), BF16),
            pltpu.VMEM(plan.main.shape, BF16),
            pltpu.VMEM(plan.edges.shape, BF16),
            pltpu.VMEM(plan.own.shape, BF16),
            pltpu.VMEM(plan.own_edges.shape, BF16),
            pltpu.VMEM((rows, channels), F32),
            pltpu.VMEM((plan.wide, channels), BF16),
            pltpu.VMEM((rows, channels), F32),
            pltpu.VMEM((rows, channels), F32),
            pltpu.VMEM((plan.wide, channels), BF16),
            pltpu.VMEM((3 * plan.tap_rows, channels), BF16),
            pltpu.VMEM((rows + plan.side, channels), F32),
            pltpu.VMEM((both, channels), F32),
            pltpu.VMEM((both, channels), F32),
            pltpu.VMEM((both, channels), BF16),
            pltpu.VMEM((plan.tap_rows, channels), F32),
            pltpu.VMEM((rows, LANES), F32),
            pltpu.VMEM((rows, LANES), F32),
            pltpu.VMEM((rows, LANES), F32),
            pltpu.VMEM((rows, LANES), F32),
            pltpu.VMEM((rows, LANES), F32),
            pltpu.VMEM((8, channels), F32),
            pltpu.VMEM((8, channels), F32),
            pltpu.VMEM((8, channels), F32),
            pltpu.VMEM((8, channels), F32),
            pltpu.VMEM((n, 2 * groups, LANES), BF16),
            pltpu.VMEM((owners.count * per, ALIGN, LANES), BF16),
            pltpu.VMEM((2 * n, per, ALIGN, LANES), BF16),
            pltpu.VMEM((2, per, ALIGN, LANES), BF16),
            pltpu.VMEM((owners.count, per, ALIGN, LANES), BF16),
            pltpu.VMEM(plan.taps.shape, BF16),
            pltpu.VMEM((1, channels), F32),
            pltpu.VMEM((1, channels), F32),
            pltpu.SemaphoreType.REGULAR((3,)),
            dma((15,)), dma((chunks,)), dma((4,)), dma((4,)),
            dma((5,)), dma((5,)), dma((3,)), dma((3,)),
        ],
        compiler_params=pltpu.CompilerParams(
            collective_id=0, has_side_effects=True, vmem_limit_bytes=VMEM_GRANT
        ),
    )(
        *(
            pltpu.with_memory_space_constraint(x, pltpu.HBM)
            for x in (
                value_in, gate_in, taps, gain.reshape(1, -1), shift.reshape(1, -1), w_out,
                grad_out, mats, emats, own, eown, ft,
            )
        )
    )
    results = [pltpu.with_memory_space_constraint(x, pltpu.VMEM) for x in results]
    d_value, d_gate, d_taps, d_gain, d_shift = pl.pallas_call(
        store,
        out_shape=(
            jax.ShapeDtypeStruct((rows, channels), BF16),
            jax.ShapeDtypeStruct((rows, channels), BF16),
            jax.ShapeDtypeStruct((kernel, channels), F32),
            jax.ShapeDtypeStruct((groups, LANES), F32),
            jax.ShapeDtypeStruct((groups, LANES), F32),
        ),
        in_specs=[vmem] * 4,
        out_specs=(hbm,) * 5,
        scratch_shapes=[dma((5,))],
        compiler_params=pltpu.CompilerParams(vmem_limit_bytes=8 * 1024 * 1024),
    )(*results)
    return (d_value, d_gate, d_taps, d_gain.reshape(-1), d_shift.reshape(-1))


def solution(mesh):
    return jax.shard_map(
        functools.partial(shards, mesh.shape["sp"]),
        mesh=mesh,
        in_specs=(
            P("sp", "tp"),
            P("sp", "tp"),
            P(None, "tp"),
            P("tp"),
            P("tp"),
            P("tp", None),
            P("sp", None),
        ),
        out_specs=(P("sp", "tp"), P("sp", "tp"), P(None, "tp"), P("tp"), P("tp")),
        check_vma=False,
    )
```

```python
import functools
import math

import jax
import jax.numpy as jnp
import numpy as np
from jax import lax
from jax.experimental import pallas as pl
from jax.experimental.pallas import tpu as pltpu
from jax.sharding import PartitionSpec as P

EPS = 1e-05
ALIGN = 16
LANES = 128
CHUNK = 256
VMEM_GRANT = 48 * 1024 * 1024
F32 = jnp.float32
BF16 = jnp.bfloat16


class Plan:
    def __init__(self, rows, kernel, total):
        self.half = half = kernel // 2
        self.kernel = kernel
        self.rows = rows
        self.edge = edge = -(-half // ALIGN) * ALIGN
        self.side = side = 4 * edge
        self.inner = rows - 2 * edge
        self.wide = rows + 2 * edge
        self.tap_rows = -(-kernel // ALIGN) * ALIGN

        def omega(size):
            return 2.0 * np.pi * (np.arange(size // 2) + 0.5) / size

        def spectrum(size, times):
            angle = omega(size)[:, None] * times[None, :]
            return np.concatenate([np.cos(angle), np.sin(angle)], 0)

        def inverse(size, times):
            angle = times[:, None] * omega(size)[None, :]
            return np.concatenate([np.cos(angle), -np.sin(angle)], 1)

        def lags(size):
            out = inverse(size, np.arange(self.tap_rows) - half)
            out[kernel:] = 0.0
            return out

        main = np.arange(self.inner) + edge
        top = np.arange(edge) + edge
        low = np.arange(edge) + side - 2 * edge
        self.main = np.concatenate(
            [
                spectrum(rows, np.arange(rows)), inverse(rows, main - half),
                inverse(rows, main + half), lags(rows),
            ],
            0,
        )
        self.at_conv = rows
        self.at_grad = self.at_conv + self.inner
        self.at_lags = self.at_grad + self.inner
        self.edges = np.concatenate(
            [spectrum(side, np.arange(side))]
            + [inverse(side, part + shift) for shift in (-half, half) for part in (top, low)]
            + [lags(side)],
            0,
        )
        self.edge_conv = side
        self.edge_grad = side + 2 * edge
        self.edge_lags = side + 4 * edge
        self.own = spectrum(rows, main)
        self.own_edges = np.concatenate([spectrum(side, top), spectrum(side, low)], 0)
        taps = np.zeros((rows + side, self.tap_rows))
        times = np.arange(kernel)
        taps[:rows, :kernel] = spectrum(rows, times) * (2.0 / rows)
        taps[rows:, :kernel] = spectrum(side, times) * (2.0 / side)
        high = taps.astype(jnp.bfloat16)
        low_part = taps - high.astype(np.float64)
        self.taps = np.concatenate([high.astype(np.float64), high.astype(np.float64), low_part], 1)
        self.lag_scale = [2.0 / size / math.sqrt(total) for size in (rows, side)]


class Owners:
    def __init__(self, n, tiles):
        self.count = max(1, min(n // 2, tiles))
        self.per = -(-tiles // self.count)
        self.first = max(0, (n - self.count) // 2 - 1)


def dot(a, b):
    return jnp.dot(a, b, preferred_element_type=F32)


def sigmoid(x):
    return 0.5 * jnp.tanh(0.5 * x) + 0.5


def body(
    plan, n, tiles, owners, total,
    value_h, gate_h, taps_h, gain_h, shift_h, w_h, go_h, mats_h, emats_h, own_h, eown_h, ft_h,
    dv, dg, dt_o, dgs_o,
    value, gate, taps, w, go, mats, emats, own, eown,
    sig_s, gw, conv, gm, gcw, tcat, ts, g_spec, spec_s, prod, lag_s,
    st1, st1_in, st2, st2_in, inv_s, colg, cols, hgain, hshift,
    gs, rs_src, rs_in, ag_src, ag, ft, gain, shift,
    meet, load_sem, w_sem, halo_send, halo_recv, tp_send, tp_recv,
    all_send, all_recv,
):
    sp = lax.axis_index("sp")
    tp = lax.axis_index("tp")
    rows, edge, side, inner_rows = plan.rows, plan.edge, plan.side, plan.inner
    channels = value.shape[1]
    width = channels * 2
    chunks = channels // CHUNK
    per = owners.per
    nxt = lax.rem(sp + 1, n)
    prv = lax.rem(sp + n - 1, n)
    has_prv = sp > 0
    has_nxt = sp < n - 1
    is_owner = (sp >= owners.first) & (sp < owners.first + owners.count) & (tp == 1)
    low_side = sp < n // 2
    crew = 1 << (max(n, 1).bit_length() // 2)
    crews = -(-n // crew)
    head = sp - lax.rem(sp, crew)
    is_head = (sp == head) & (tp == 1)

    def peer(d):
        return lax.rem(sp + d, n)

    barrier = pltpu.get_barrier_semaphore()

    inner = pl.ds(edge, rows - 2 * edge)
    sides = [pl.ds(0, edge), pl.ds(rows - edge, edge)]
    pairs = [(h.at[part], v.at[part]) for h, v in ((value_h, value), (gate_h, gate)) for part in sides]
    pairs += [(taps_h, taps), (ft_h, ft)]
    pairs += [(h.at[inner], v.at[inner]) for h, v in ((value_h, value), (gate_h, gate))]
    pairs += [(mats_h, mats), (go_h, go)]
    late = [
        (emats_h, emats), (own_h, own), (eown_h, eown), (gain_h, gain), (shift_h, shift),
    ]
    loads = [
        pltpu.make_async_copy(a, b, load_sem.at[i]) for i, (a, b) in enumerate(pairs + late)
    ]

    def w_copy(c):
        part = pl.ds(pl.multiple_of(c * CHUNK, CHUNK), CHUNK)
        return pltpu.make_async_copy(w_h.at[part], w.at[part], w_sem.at[c])

    def tell(sem, s, t):
        pl.semaphore_signal(sem, 1, device_id=(s, t), device_id_type=pl.DeviceIdType.MESH)

    members = 2 * jnp.minimum(crew, n - head)

    def each_member(sem):
        def step(i, carry):
            s, t = head + i // 2, lax.rem(i, 2)

            @pl.when((s != sp) | (t != tp))
            def _():
                tell(sem, s, t)

            return carry

        lax.fori_loop(0, members, step, 0)

    def each_head(sem):
        def step(i, carry):
            @pl.when(i * crew != sp)
            def _():
                tell(sem, i * crew, 1)

            return carry

        lax.fori_loop(0, crews, step, 0)

    tell(barrier, sp, 1 - tp)

    @pl.when(has_prv)
    def _():
        tell(barrier, prv, tp)

    @pl.when(has_nxt)
    def _():
        tell(barrier, nxt, tp)

    @pl.when(is_head)
    def _():
        each_member(barrier)
        each_head(barrier)

    for load in loads[: len(pairs)]:
        load.start()

    greeted = (
        1 + has_prv.astype(jnp.int32) + has_nxt.astype(jnp.int32)
        + jnp.where(is_head, crews - 1, 1)
    )

    def handshake_up():
        @pl.when(jnp.logical_not(is_head))
        def _():
            tell(meet.at[0], head, 1)

    def handshake_across():
        @pl.when(is_head)
        def _():
            pl.semaphore_wait(meet.at[0], members - 1)
            each_head(meet.at[1])

    def handshake_down():
        @pl.when(is_head)
        def _():
            if crews > 1:
                pl.semaphore_wait(meet.at[1], crews - 1)
            each_member(meet.at[2])

    def handshake_done():
        @pl.when(jnp.logical_not(is_head))
        def _():
            pl.semaphore_wait(meet.at[2], 1)

    def cut(c):
        return pl.ds(c * CHUNK, CHUNK)

    def gate_step(i, carry):
        part = pl.ds(pl.multiple_of(i * ALIGN, ALIGN), ALIGN)
        place = pl.ds(pl.multiple_of(i * ALIGN + edge, ALIGN), ALIGN)
        sig = sigmoid(gate[part].astype(F32))
        sig_s[part] = sig
        gw[place] = (value[part].astype(F32) * sig).astype(BF16)
        return carry

    def remote(src, dst, send, recv, device):
        return pltpu.make_async_remote_copy(
            src_ref=src, dst_ref=dst, send_sem=send, recv_sem=recv,
            device_id=device, device_id_type=pl.DeviceIdType.MESH,
        )

    def halo_pair(ref, k):
        return (
            remote(ref.at[pl.ds(rows, edge)], ref.at[pl.ds(0, edge)],
                   halo_send.at[k], halo_recv.at[k], (nxt, tp)),
            remote(ref.at[pl.ds(edge, edge)], ref.at[pl.ds(rows + edge, edge)],
                   halo_send.at[k + 1], halo_recv.at[k + 1], (prv, tp)),
        )

    def send_halo(pair):
        @pl.when(has_nxt)
        def _():
            pair[0].start()

        @pl.when(has_prv)
        def _():
            pair[1].start()

    def recv_prv(pair, ref):
        @pl.when(has_prv)
        def _():
            pair[0].wait_recv()

        @pl.when(sp == 0)
        def _():
            ref[pl.ds(0, edge)] = jnp.zeros((edge, channels), BF16)

    def recv_nxt(pair, ref):
        @pl.when(has_nxt)
        def _():
            pair[1].wait_recv()

        @pl.when(sp == n - 1)
        def _():
            ref[pl.ds(rows + edge, edge)] = jnp.zeros((edge, channels), BF16)

    def sent_halo(pair):
        @pl.when(has_nxt)
        def _():
            pair[0].wait_send()

        @pl.when(has_prv)
        def _():
            pair[1].wait_send()

    def settle(ref, count, sem):
        if count:
            part = ref.at[pl.ds(0, count)]
            pltpu.make_async_copy(part, part, sem).wait()

    gw_halo = halo_pair(gw, 0)
    gc_halo = halo_pair(gcw, 2)

    for load in loads[:4]:
        load.wait()
    for c in range(chunks):
        w_copy(c).start()
    for load in loads[len(pairs):]:
        load.start()
    sided = edge // ALIGN
    for r in range(sided):
        gate_step(r, 0)
        gate_step(rows // ALIGN - 1 - r, 0)
    pl.semaphore_wait(barrier, greeted)
    send_halo(gw_halo)
    handshake_up()
    loads[4].wait()
    loads[5].wait()

    tap = jnp.concatenate(
        [taps[...], jnp.zeros((plan.tap_rows - plan.kernel, channels), F32)], 0
    )
    tap_high = tap.astype(BF16)
    tap_low = (tap - tap_high.astype(F32)).astype(BF16)
    for k, part in enumerate((tap_high, tap_low, tap_high)):
        tcat[pl.ds(k * plan.tap_rows, plan.tap_rows)] = part

    def tap_phase():
        for c in range(chunks):
            ts[:, cut(c)] = dot(ft[...], tcat[:, cut(c)])

    tap_phase()
    loads[6].wait()
    loads[7].wait()
    lax.fori_loop(sided, rows // ALIGN - sided, gate_step, 0, unroll=7)

    def mix(a, b):
        return lax.dot_general(a, b, (((1,), (1,)), ((), ())), preferred_element_type=F32)

    def mix_step(c, carry):
        part = pl.ds(pl.multiple_of(c * CHUNK, CHUNK), CHUNK)
        w_copy(c).wait()
        gm[:, part] = mix(go[...], w[part])
        return carry

    def fold(x):
        out = x[:, :LANES]
        for k in range(1, x.shape[1] // LANES):
            out = out + x[:, k * LANES : (k + 1) * LANES]
        return out

    lanes = lax.broadcasted_iota(jnp.int32, (ALIGN, LANES), 1) < LANES // 2

    def multiply(at, size, tap_at, sign, source):
        freqs = size // 2
        for f in range(0, freqs, ALIGN):
            high, low = pl.ds(at + f, ALIGN), pl.ds(at + freqs + f, ALIGN)
            for c in range(chunks):
                re, im = source[high, cut(c)], source[low, cut(c)]
                ta = ts[pl.ds(tap_at + f, ALIGN), cut(c)]
                tb = ts[pl.ds(tap_at + freqs + f, ALIGN), cut(c)]
                prod[high, cut(c)] = (re * ta + sign * im * tb).astype(BF16)
                other = re * tb - sign * im * ta
                prod[low, cut(c)] = (sign * other).astype(BF16)

    def slot(r):
        return r - edge if edge <= r < rows - edge else (r + inner_rows if r < edge else r)

    main_rows = list(range(edge, rows - edge, ALIGN))
    middle = len(main_rows) // 2
    first_rows, second_rows = main_rows[:middle], main_rows[middle:]
    edge_rows = list(range(0, edge, ALIGN)) + list(range(rows - edge, rows, ALIGN))

    def stats(picked):
        for r in picked:
            one = two = None
            for c in range(chunks):
                x = conv[pl.ds(r, ALIGN), cut(c)]
                p, q = fold(x), fold(x * x)
                one, two = (p, q) if c == 0 else (one + p, two + q)
            st1[pl.ds(slot(r), ALIGN)] = jnp.where(
                lanes, jnp.sum(one, 1, keepdims=True), jnp.sum(two, 1, keepdims=True)
            )

    def transform_main(source, target, at, sign):
        target[pl.ds(0, rows)] = dot(mats[pl.ds(0, rows)], source[pl.ds(edge, rows)])
        multiply(0, rows, 0, sign, target)
        conv[pl.ds(edge, inner_rows)] = dot(mats[pl.ds(at, inner_rows)], prod[pl.ds(0, rows)])

    def transform_edges(source, target, at, sign):
        for e in range(2):
            window = source[pl.ds(e * (plan.wide - side), side)]
            target[pl.ds(rows + e * side, side)] = dot(emats[pl.ds(0, side)], window)
        for e in range(2):
            multiply(rows + e * side, side, rows, sign, target)
        for e in range(2):
            conv[pl.ds(e * (rows - edge), edge)] = dot(
                emats[pl.ds(at + e * edge, edge)], prod[pl.ds(rows + e * side, side)]
            )

    def swap(src, dst, start, count, k):
        place = pl.ds(start, count)
        return remote(
            src.at[place], dst.at[place], tp_send.at[k], tp_recv.at[k], (sp, 1 - tp)
        )

    cutoff = middle * ALIGN
    swap1 = [
        swap(st1, st1_in, 0, inner_rows, 0), swap(st1, st1_in, inner_rows, 2 * edge, 1)
    ]
    swap2 = [
        swap(st2, st2_in, 0, cutoff, 2), swap(st2, st2_in, cutoff, inner_rows - cutoff, 3),
        swap(st2, st2_in, inner_rows, 2 * edge, 4),
    ]

    def conv_main_phase():
        transform_main(gw, g_spec, plan.at_conv, 1.0)
        stats(main_rows)

    def conv_edge_phase():
        transform_edges(gw, g_spec, plan.edge_conv, 1.0)
        stats(edge_rows)

    loads[8].wait()
    conv_main_phase()
    swap1[0].start()
    handshake_across()
    loads[9].wait()
    lax.fori_loop(0, chunks, mix_step, 0)
    for load in loads[10:]:
        load.wait()
    hgain[...] = jnp.broadcast_to(0.5 * gain[...], hgain.shape)
    hshift[...] = jnp.broadcast_to(0.5 * shift[...], hshift.shape)

    def twice(x):
        return jnp.concatenate([x, x], 0)

    def halves(x):
        return x[:8] + x[8:]

    def norm_at(picked, opening):
        total_g, total_s = [None] * chunks, [None] * chunks
        for r in picked:
            part, place = pl.ds(r, ALIGN), pl.ds(slot(r), ALIGN)
            tot = (st1[place] + st1_in[place]) * (1.0 / width)
            mean = tot[:, :1]
            var = tot[:, LANES // 2 : LANES // 2 + 1] - mean * mean
            inv = lax.rsqrt(var + EPS)
            inv_s[place] = jnp.broadcast_to(inv, (ALIGN, LANES))
            one = two = None
            for c in range(chunks):
                hg = twice(hgain[:, cut(c)])
                normed = (conv[part, cut(c)] - mean) * inv
                half_pre = normed * hg + twice(hshift[:, cut(c)])
                th = jnp.tanh(half_pre)
                gp = gm[part, cut(c)] * (1.0 + th) * (1.0 + half_pre * (1.0 - th))
                gn = gp * hg
                gpn = gp * normed
                conv[part, cut(c)] = normed
                gm[part, cut(c)] = gn
                p, q = fold(gn), fold(gpn * hg)
                one, two = (p, q) if c == 0 else (one + p, two + q)
                g, h = halves(gpn), halves(gp)
                if total_g[c] is not None:
                    g, h = total_g[c] + g, total_s[c] + h
                total_g[c], total_s[c] = g, h
            st2[place] = jnp.where(
                lanes, jnp.sum(one, 1, keepdims=True), jnp.sum(two, 1, keepdims=True)
            )
        for c in range(chunks):
            if opening:
                colg[:, cut(c)] = total_g[c]
                cols[:, cut(c)] = total_s[c]
            else:
                colg[:, cut(c)] += total_g[c]
                cols[:, cut(c)] += total_s[c]

    def gc_at(picked):
        for r in picked:
            part, place = pl.ds(r, ALIGN), pl.ds(slot(r), ALIGN)
            tot = (st2[place] + st2_in[place]) * (1.0 / width)
            inv = inv_s[place]
            scaled = inv * tot
            m1 = scaled[:, :1]
            m2 = scaled[:, LANES // 2 : LANES // 2 + 1]
            inv = inv[:, :1]
            for c in range(chunks):
                gcw[pl.ds(r + edge, ALIGN), cut(c)] = (
                    inv * gm[part, cut(c)] - m1 - conv[part, cut(c)] * m2
                ).astype(BF16)

    swap1[0].wait_recv()
    norm_at(first_rows, True)
    swap2[0].start()
    recv_prv(gw_halo, gw)
    recv_nxt(gw_halo, gw)
    conv_edge_phase()
    swap1[1].start()
    handshake_down()
    norm_at(second_rows, False)
    swap2[1].start()
    swap2[0].wait_recv()
    gc_at(first_rows)
    swap1[1].wait_recv()
    norm_at(edge_rows, False)
    swap2[2].start()

    rg = jnp.sum(colg[...], 0, keepdims=True)
    rsh = jnp.sum(cols[...], 0, keepdims=True)
    groups = channels // LANES
    gs[sp] = jnp.concatenate(
        [x[:, k * LANES : (k + 1) * LANES] for x in (rg, rsh) for k in range(groups)], 0
    ).astype(BF16)

    def send_gs(d, carry):
        remote(gs.at[sp], gs.at[sp], all_send.at[0], all_recv.at[0], (peer(d), tp)).start()
        return carry

    handshake_done()
    lax.fori_loop(1, n, send_gs, 0)

    slots = owners.count * per
    if slots > tiles:
        rs_src[pl.ds(tiles, slots - tiles)] = jnp.zeros((slots - tiles, ALIGN, LANES), BF16)
    tall = plan.tap_rows // ALIGN

    def lag_part(at, size, f, c):
        high, low = pl.ds(at + f, ALIGN), pl.ds(at + size // 2 + f, ALIGN)
        re, im = spec_s[high, cut(c)], spec_s[low, cut(c)]
        hr, hi = g_spec[high, cut(c)], g_spec[low, cut(c)]
        return hr * re + hi * im, hr * im - hi * re

    def send_rs(i, carry):
        o = jnp.where(low_side, owners.count - 1 - i, i)
        to = owners.first + o

        @pl.when((to != sp) | (tp != 1))
        def _():
            remote(rs_src.at[pl.ds(o * per, per)], rs_in.at[2 * sp + tp],
                   all_send.at[1], all_recv.at[1], (to, 1)).start()

        return carry

    def spec_main_phase():
        spec_s[pl.ds(0, rows)] = dot(own[...], gcw[pl.ds(2 * edge, inner_rows)])
        for f in range(0, rows // 2, ALIGN):
            for c in range(chunks):
                dr, di = lag_part(0, rows, f, c)
                prod[pl.ds(f, ALIGN), cut(c)] = dr.astype(BF16)
                prod[pl.ds(rows // 2 + f, ALIGN), cut(c)] = di.astype(BF16)
        lag_s[...] = (
            dot(mats[pl.ds(plan.at_lags, plan.tap_rows)], prod[pl.ds(0, rows)])
            * plan.lag_scale[0]
        )

    def spec_edge_phase():
        for e in range(2):
            spec_s[pl.ds(rows + e * side, side)] = dot(
                eown[pl.ds(e * side, side)], gcw[pl.ds(edge + e * (rows - edge), edge)]
            )
        for f in range(0, side // 2, ALIGN):
            for c in range(chunks):
                r0, i0 = lag_part(rows, side, f, c)
                r1, i1 = lag_part(rows + side, side, f, c)
                prod[pl.ds(rows + f, ALIGN), cut(c)] = (r0 + r1).astype(BF16)
                prod[pl.ds(rows + side // 2 + f, ALIGN), cut(c)] = (i0 + i1).astype(BF16)
        out = lag_s[...] + plan.lag_scale[1] * dot(
            emats[pl.ds(plan.edge_lags, plan.tap_rows)], prod[pl.ds(rows, side)]
        )
        out = out.astype(BF16)
        for r in range(tall):
            for k in range(groups):
                rs_src[k * tall + r] = out[
                    r * ALIGN : (r + 1) * ALIGN, k * LANES : (k + 1) * LANES
                ]

    swap2[1].wait_recv()
    gc_at(second_rows)
    spec_main_phase()
    swap2[2].wait_recv()
    gc_at(edge_rows)
    spec_edge_phase()
    lax.fori_loop(0, owners.count, send_rs, 0)
    send_halo(gc_halo)

    def sum_phase():
        @pl.when(is_owner)
        def _():
            o = sp - owners.first
            rs_in[2 * sp + 1] = rs_src[pl.ds(o * per, per)]
            settle(rs_in, 2 * n - 1, all_recv.at[1])
            zero = jnp.zeros((2, per, ALIGN, LANES), F32)
            summed = lax.fori_loop(
                0, n, lambda i, t: t + rs_in[pl.ds(2 * i, 2)].astype(F32), zero, unroll=4
            )
            ag_src[...] = summed.astype(BF16)
            ag[o] = ag_src[1]

    def gather_phase(first, count):
        @pl.when(is_owner)
        def _():
            o = sp - owners.first

            def send_ag(i, carry):
                for t in range(2):
                    @pl.when((i != sp) | (t != 1))
                    def _():
                        remote(ag_src.at[t], ag.at[o],
                               all_send.at[2], all_recv.at[2], (i, t)).start()

                return carry

            lax.fori_loop(first, first + count, send_ag, 0)

    def finish(picked):
        for r in picked:
            part = pl.ds(r, ALIGN)
            for c in range(chunks):
                sig = sig_s[part, cut(c)]
                left = conv[part, cut(c)] * sig
                dv[part, cut(c)] = left.astype(BF16)
                dg[part, cut(c)] = (
                    left * value[part, cut(c)].astype(F32) * (1.0 - sig)
                ).astype(BF16)

    def out_main_phase():
        transform_main(gcw, spec_s, plan.at_grad, -1.0)
        finish(main_rows)

    def out_edge_phase():
        transform_edges(gcw, spec_s, plan.edge_grad, -1.0)
        finish(edge_rows)

    out_main_phase()
    sum_phase()
    gather_phase(0, 1)
    gather_phase(1, n - 1)
    recv_prv(gc_halo, gcw)
    recv_nxt(gc_halo, gcw)
    out_edge_phase()
    settle(gs, n - 1, all_recv.at[0])
    small = lax.fori_loop(
        0, n, lambda i, t: t + gs[i].astype(F32), jnp.zeros(gs.shape[1:], F32)
    )
    dgs_o[...] = small * (0.5 / math.sqrt(total))

    sent_halo(gw_halo)
    sent_halo(gc_halo)
    for each in swap1 + swap2:
        each.wait_send()
    settle(gs, n - 1, all_send.at[0])

    @pl.when(is_owner)
    def _():
        settle(rs_in, owners.count - 1, all_send.at[1])
        settle(ag, owners.count - 1, all_recv.at[2])

    @pl.when(jnp.logical_not(is_owner))
    def _():
        settle(rs_in, owners.count, all_send.at[1])
        settle(ag, owners.count, all_recv.at[2])

    for t in range(tiles):
        k, r = t // tall, t % tall
        count = min(ALIGN, plan.kernel - r * ALIGN)
        dt_o[pl.ds(r * ALIGN, count), pl.ds(k * LANES, LANES)] = ag[t // per, t % per].astype(F32)[
            :count
        ]

    @pl.when(is_owner)
    def _():
        settle(rs_in, 2 * n - 1, all_send.at[2])


def store(*refs):
    sources, targets, out_sem = refs[:4], refs[4:9], refs[9]
    groups = sources[3].shape[0] // 2
    views = list(sources[:3]) + [
        sources[3].at[pl.ds(0, groups)], sources[3].at[pl.ds(groups, groups)]
    ]
    copies = [
        pltpu.make_async_copy(a, b, out_sem.at[i]) for i, (a, b) in enumerate(zip(views, targets))
    ]
    for copy in copies:
        copy.start()
    for copy in copies:
        copy.wait()


def shards(n, value_in, gate_in, taps, gain, shift, w_out, grad_out):
    rows, channels = value_in.shape
    kernel = taps.shape[0]
    total = rows * n
    plan = Plan(rows, kernel, total)
    groups = channels // LANES
    tiles = plan.tap_rows // ALIGN * groups
    owners = Owners(n, tiles)
    per = owners.per
    model = grad_out.shape[1]
    mats = jnp.asarray(plan.main, BF16)
    emats = jnp.asarray(plan.edges, BF16)
    own = jnp.asarray(plan.own, BF16)
    eown = jnp.asarray(plan.own_edges, BF16)
    ft = jnp.asarray(plan.taps, BF16)
    hbm = pl.BlockSpec(memory_space=pltpu.HBM)
    vmem = pl.BlockSpec(memory_space=pltpu.VMEM)
    both = rows + 2 * plan.side
    chunks = channels // CHUNK
    dma = pltpu.SemaphoreType.DMA
    results = pl.pallas_call(
        functools.partial(body, plan, n, tiles, owners, total),
        out_shape=(
            pltpu.VMEM((rows, channels), BF16),
            pltpu.VMEM((rows, channels), BF16),
            pltpu.VMEM((kernel, channels), F32),
            pltpu.VMEM((2 * groups, LANES), F32),
        ),
        in_specs=[hbm] * 12,
        out_specs=(vmem,) * 4,
        scratch_shapes=[
            pltpu.VMEM((rows, channels), BF16),
            pltpu.VMEM((rows, channels), BF16),
            pltpu.VMEM((kernel, channels), F32),
            pltpu.VMEM((channels, model), BF16),
            pltpu.VMEM((rows, model), BF16),
            pltpu.VMEM(plan.main.shape, BF16),
            pltpu.VMEM(plan.edges.shape, BF16),
            pltpu.VMEM(plan.own.shape, BF16),
            pltpu.VMEM(plan.own_edges.shape, BF16),
            pltpu.VMEM((rows, channels), F32),
            pltpu.VMEM((plan.wide, channels), BF16),
            pltpu.VMEM((rows, channels), F32),
            pltpu.VMEM((rows, channels), F32),
            pltpu.VMEM((plan.wide, channels), BF16),
            pltpu.VMEM((3 * plan.tap_rows, channels), BF16),
            pltpu.VMEM((rows + plan.side, channels), F32),
            pltpu.VMEM((both, channels), F32),
            pltpu.VMEM((both, channels), F32),
            pltpu.VMEM((both, channels), BF16),
            pltpu.VMEM((plan.tap_rows, channels), F32),
            pltpu.VMEM((rows, LANES), F32),
            pltpu.VMEM((rows, LANES), F32),
            pltpu.VMEM((rows, LANES), F32),
            pltpu.VMEM((rows, LANES), F32),
            pltpu.VMEM((rows, LANES), F32),
            pltpu.VMEM((8, channels), F32),
            pltpu.VMEM((8, channels), F32),
            pltpu.VMEM((8, channels), F32),
            pltpu.VMEM((8, channels), F32),
            pltpu.VMEM((n, 2 * groups, LANES), BF16),
            pltpu.VMEM((owners.count * per, ALIGN, LANES), BF16),
            pltpu.VMEM((2 * n, per, ALIGN, LANES), BF16),
            pltpu.VMEM((2, per, ALIGN, LANES), BF16),
            pltpu.VMEM((owners.count, per, ALIGN, LANES), BF16),
            pltpu.VMEM(plan.taps.shape, BF16),
            pltpu.VMEM((1, channels), F32),
            pltpu.VMEM((1, channels), F32),
            pltpu.SemaphoreType.REGULAR((3,)),
            dma((15,)), dma((chunks,)), dma((4,)), dma((4,)),
            dma((5,)), dma((5,)), dma((3,)), dma((3,)),
        ],
        compiler_params=pltpu.CompilerParams(
            collective_id=0, has_side_effects=True, vmem_limit_bytes=VMEM_GRANT
        ),
    )(
        *(
            pltpu.with_memory_space_constraint(x, pltpu.HBM)
            for x in (
                value_in, gate_in, taps, gain.reshape(1, -1), shift.reshape(1, -1), w_out,
                grad_out, mats, emats, own, eown, ft,
            )
        )
    )
    results = [pltpu.with_memory_space_constraint(x, pltpu.VMEM) for x in results]
    d_value, d_gate, d_taps, d_gain, d_shift = pl.pallas_call(
        store,
        out_shape=(
            jax.ShapeDtypeStruct((rows, channels), BF16),
            jax.ShapeDtypeStruct((rows, channels), BF16),
            jax.ShapeDtypeStruct((kernel, channels), F32),
            jax.ShapeDtypeStruct((groups, LANES), F32),
            jax.ShapeDtypeStruct((groups, LANES), F32),
        ),
        in_specs=[vmem] * 4,
        out_specs=(hbm,) * 5,
        scratch_shapes=[dma((5,))],
        compiler_params=pltpu.CompilerParams(vmem_limit_bytes=8 * 1024 * 1024),
    )(*results)
    return (d_value, d_gate, d_taps, d_gain.reshape(-1), d_shift.reshape(-1))


def solution(mesh):
    return jax.shard_map(
        functools.partial(shards, mesh.shape["sp"]),
        mesh=mesh,
        in_specs=(
            P("sp", "tp"),
            P("sp", "tp"),
            P(None, "tp"),
            P("tp"),
            P("tp"),
            P("tp", None),
            P("sp", None),
        ),
        out_specs=(P("sp", "tp"), P("sp", "tp"), P(None, "tp"), P("tp"), P("tp")),
        check_vma=False,
    )
```

```python
import functools
import math

import jax
import jax.numpy as jnp
import numpy as np
from jax import lax
from jax.experimental import pallas as pl
from jax.experimental.pallas import tpu as pltpu
from jax.sharding import PartitionSpec as P

EPS = 1e-05
ALIGN = 16
LANES = 128
CHUNK = 256
VMEM_GRANT = 48 * 1024 * 1024
F32 = jnp.float32
BF16 = jnp.bfloat16


class Plan:
    def __init__(self, rows, kernel, total):
        self.half = half = kernel // 2
        self.kernel = kernel
        self.rows = rows
        self.edge = edge = -(-half // ALIGN) * ALIGN
        self.side = side = 4 * edge
        self.inner = rows - 2 * edge
        self.wide = rows + 2 * edge
        self.tap_rows = -(-kernel // ALIGN) * ALIGN

        def omega(size):
            return 2.0 * np.pi * (np.arange(size // 2) + 0.5) / size

        def spectrum(size, times):
            angle = omega(size)[:, None] * times[None, :]
            return np.concatenate([np.cos(angle), np.sin(angle)], 0)

        def inverse(size, times):
            angle = times[:, None] * omega(size)[None, :]
            return np.concatenate([np.cos(angle), -np.sin(angle)], 1)

        def lags(size):
            out = inverse(size, np.arange(self.tap_rows) - half)
            out[kernel:] = 0.0
            return out

        main = np.arange(self.inner) + edge
        top = np.arange(edge) + edge
        low = np.arange(edge) + side - 2 * edge
        self.main = np.concatenate(
            [
                spectrum(rows, np.arange(rows)), inverse(rows, main - half),
                inverse(rows, main + half), lags(rows),
            ],
            0,
        )
        self.at_conv = rows
        self.at_grad = self.at_conv + self.inner
        self.at_lags = self.at_grad + self.inner
        self.edges = np.concatenate(
            [spectrum(side, np.arange(side))]
            + [inverse(side, part + shift) for shift in (-half, half) for part in (top, low)]
            + [lags(side)],
            0,
        )
        self.edge_conv = side
        self.edge_grad = side + 2 * edge
        self.edge_lags = side + 4 * edge
        self.own = spectrum(rows, main)
        self.own_edges = np.concatenate([spectrum(side, top), spectrum(side, low)], 0)
        taps = np.zeros((rows + side, self.tap_rows))
        times = np.arange(kernel)
        taps[:rows, :kernel] = spectrum(rows, times) * (2.0 / rows)
        taps[rows:, :kernel] = spectrum(side, times) * (2.0 / side)
        high = taps.astype(jnp.bfloat16)
        low_part = taps - high.astype(np.float64)
        self.taps = np.concatenate([high.astype(np.float64), high.astype(np.float64), low_part], 1)
        self.lag_scale = [2.0 / size / math.sqrt(total) for size in (rows, side)]


class Owners:
    def __init__(self, n, tiles):
        self.count = max(1, min(n // 2, tiles))
        self.per = -(-tiles // self.count)
        self.first = max(0, (n - self.count) // 2 - 1)


def dot(a, b):
    return jnp.dot(a, b, preferred_element_type=F32)


def sigmoid(x):
    return 0.5 * jnp.tanh(0.5 * x) + 0.5


def body(
    plan, n, tiles, owners, total,
    value_h, gate_h, taps_h, gain_h, shift_h, w_h, go_h, mats_h, emats_h, own_h, eown_h, ft_h,
    dv, dg, dt_o, dgs_o,
    value, gate, taps, w, go, mats, emats, own, eown,
    sig_s, gw, conv, gm, gcw, tcat, ts, g_spec, spec_s, prod, lag_s,
    st1, st1_in, st2, st2_in, inv_s, colg, cols, hgain, hshift,
    gs, rs_src, rs_in, ag_src, ag, ft, gain, shift,
    meet, load_sem, w_sem, halo_send, halo_recv, tp_send, tp_recv,
    all_send, all_recv,
):
    sp = lax.axis_index("sp")
    tp = lax.axis_index("tp")
    rows, edge, side, inner_rows = plan.rows, plan.edge, plan.side, plan.inner
    channels = value.shape[1]
    width = channels * 2
    chunks = channels // CHUNK
    per = owners.per
    nxt = lax.rem(sp + 1, n)
    prv = lax.rem(sp + n - 1, n)
    has_prv = sp > 0
    has_nxt = sp < n - 1
    is_owner = (sp >= owners.first) & (sp < owners.first + owners.count) & (tp == 1)
    low_side = sp < n // 2
    crew = 1 << (max(n, 1).bit_length() // 2)
    crews = -(-n // crew)
    head = sp - lax.rem(sp, crew)
    is_head = (sp == head) & (tp == 1)

    def peer(d):
        return lax.rem(sp + d, n)

    barrier = pltpu.get_barrier_semaphore()

    inner = pl.ds(edge, rows - 2 * edge)
    sides = [pl.ds(0, edge), pl.ds(rows - edge, edge)]
    pairs = [(h.at[part], v.at[part]) for h, v in ((value_h, value), (gate_h, gate)) for part in sides]
    pairs += [(taps_h, taps), (ft_h, ft)]
    pairs += [(h.at[inner], v.at[inner]) for h, v in ((value_h, value), (gate_h, gate))]
    pairs += [(mats_h, mats), (go_h, go)]
    late = [
        (emats_h, emats), (own_h, own), (eown_h, eown), (gain_h, gain), (shift_h, shift),
    ]
    loads = [
        pltpu.make_async_copy(a, b, load_sem.at[i]) for i, (a, b) in enumerate(pairs + late)
    ]

    def w_copy(c):
        part = pl.ds(pl.multiple_of(c * CHUNK, CHUNK), CHUNK)
        return pltpu.make_async_copy(w_h.at[part], w.at[part], w_sem.at[c])

    def tell(sem, s, t):
        pl.semaphore_signal(sem, 1, device_id=(s, t), device_id_type=pl.DeviceIdType.MESH)

    members = 2 * jnp.minimum(crew, n - head)

    def each_member(sem):
        def step(i, carry):
            s, t = head + i // 2, lax.rem(i, 2)

            @pl.when((s != sp) | (t != tp))
            def _():
                tell(sem, s, t)

            return carry

        lax.fori_loop(0, members, step, 0)

    def each_head(sem):
        def step(i, carry):
            @pl.when(i * crew != sp)
            def _():
                tell(sem, i * crew, 1)

            return carry

        lax.fori_loop(0, crews, step, 0)

    tell(barrier, sp, 1 - tp)

    @pl.when(has_prv)
    def _():
        tell(barrier, prv, tp)

    @pl.when(has_nxt)
    def _():
        tell(barrier, nxt, tp)

    @pl.when(is_head)
    def _():
        each_member(barrier)
        each_head(barrier)

    for load in loads[: len(pairs)]:
        load.start()

    greeted = (
        1 + has_prv.astype(jnp.int32) + has_nxt.astype(jnp.int32)
        + jnp.where(is_head, crews - 1, 1)
    )

    def handshake_up():
        @pl.when(jnp.logical_not(is_head))
        def _():
            tell(meet.at[0], head, 1)

    def handshake_across():
        @pl.when(is_head)
        def _():
            pl.semaphore_wait(meet.at[0], members - 1)
            each_head(meet.at[1])

    def handshake_down():
        @pl.when(is_head)
        def _():
            if crews > 1:
                pl.semaphore_wait(meet.at[1], crews - 1)
            each_member(meet.at[2])

    def handshake_done():
        @pl.when(jnp.logical_not(is_head))
        def _():
            pl.semaphore_wait(meet.at[2], 1)

    def cut(c):
        return pl.ds(c * CHUNK, CHUNK)

    def gate_step(i, carry):
        part = pl.ds(pl.multiple_of(i * ALIGN, ALIGN), ALIGN)
        place = pl.ds(pl.multiple_of(i * ALIGN + edge, ALIGN), ALIGN)
        sig = sigmoid(gate[part].astype(F32))
        sig_s[part] = sig
        gw[place] = (value[part].astype(F32) * sig).astype(BF16)
        return carry

    def remote(src, dst, send, recv, device):
        return pltpu.make_async_remote_copy(
            src_ref=src, dst_ref=dst, send_sem=send, recv_sem=recv,
            device_id=device, device_id_type=pl.DeviceIdType.MESH,
        )

    def halo_pair(ref, k):
        return (
            remote(ref.at[pl.ds(rows, edge)], ref.at[pl.ds(0, edge)],
                   halo_send.at[k], halo_recv.at[k], (nxt, tp)),
            remote(ref.at[pl.ds(edge, edge)], ref.at[pl.ds(rows + edge, edge)],
                   halo_send.at[k + 1], halo_recv.at[k + 1], (prv, tp)),
        )

    def send_halo(pair):
        @pl.when(has_nxt)
        def _():
            pair[0].start()

        @pl.when(has_prv)
        def _():
            pair[1].start()

    def recv_prv(pair, ref):
        @pl.when(has_prv)
        def _():
            pair[0].wait_recv()

        @pl.when(sp == 0)
        def _():
            ref[pl.ds(0, edge)] = jnp.zeros((edge, channels), BF16)

    def recv_nxt(pair, ref):
        @pl.when(has_nxt)
        def _():
            pair[1].wait_recv()

        @pl.when(sp == n - 1)
        def _():
            ref[pl.ds(rows + edge, edge)] = jnp.zeros((edge, channels), BF16)

    def sent_halo(pair):
        @pl.when(has_nxt)
        def _():
            pair[0].wait_send()

        @pl.when(has_prv)
        def _():
            pair[1].wait_send()

    def settle(ref, count, sem):
        if count:
            part = ref.at[pl.ds(0, count)]
            pltpu.make_async_copy(part, part, sem).wait()

    gw_halo = halo_pair(gw, 0)
    gc_halo = halo_pair(gcw, 2)

    for load in loads[:4]:
        load.wait()
    for c in range(chunks):
        w_copy(c).start()
    for load in loads[len(pairs):]:
        load.start()
    sided = edge // ALIGN
    for r in range(sided):
        gate_step(r, 0)
        gate_step(rows // ALIGN - 1 - r, 0)
    pl.semaphore_wait(barrier, greeted)
    send_halo(gw_halo)
    handshake_up()
    loads[4].wait()
    loads[5].wait()

    tap = jnp.concatenate(
        [taps[...], jnp.zeros((plan.tap_rows - plan.kernel, channels), F32)], 0
    )
    tap_high = tap.astype(BF16)
    tap_low = (tap - tap_high.astype(F32)).astype(BF16)
    for k, part in enumerate((tap_high, tap_low, tap_high)):
        tcat[pl.ds(k * plan.tap_rows, plan.tap_rows)] = part

    def tap_phase():
        for c in range(chunks):
            ts[:, cut(c)] = dot(ft[...], tcat[:, cut(c)])

    tap_phase()
    loads[6].wait()
    loads[7].wait()
    lax.fori_loop(sided, rows // ALIGN - sided, gate_step, 0, unroll=7)

    def mix(a, b):
        return lax.dot_general(a, b, (((1,), (1,)), ((), ())), preferred_element_type=F32)

    def mix_step(c, carry):
        part = pl.ds(pl.multiple_of(c * CHUNK, CHUNK), CHUNK)
        w_copy(c).wait()
        gm[:, part] = mix(go[...], w[part])
        return carry

    def fold(x):
        out = x[:, :LANES]
        for k in range(1, x.shape[1] // LANES):
            out = out + x[:, k * LANES : (k + 1) * LANES]
        return out

    lanes = lax.broadcasted_iota(jnp.int32, (ALIGN, LANES), 1) < LANES // 2

    def multiply(at, size, tap_at, sign, source):
        freqs = size // 2
        for f in range(0, freqs, ALIGN):
            high, low = pl.ds(at + f, ALIGN), pl.ds(at + freqs + f, ALIGN)
            for c in range(chunks):
                re, im = source[high, cut(c)], source[low, cut(c)]
                ta = ts[pl.ds(tap_at + f, ALIGN), cut(c)]
                tb = ts[pl.ds(tap_at + freqs + f, ALIGN), cut(c)]
                prod[high, cut(c)] = (re * ta + sign * im * tb).astype(BF16)
                other = re * tb - sign * im * ta
                prod[low, cut(c)] = (sign * other).astype(BF16)

    def slot(r):
        return r - edge if edge <= r < rows - edge else (r + inner_rows if r < edge else r)

    main_rows = list(range(edge, rows - edge, ALIGN))
    middle = len(main_rows) // 2
    first_rows, second_rows = main_rows[:middle], main_rows[middle:]
    edge_rows = list(range(0, edge, ALIGN)) + list(range(rows - edge, rows, ALIGN))

    def stats(picked):
        for r in picked:
            one = two = None
            for c in range(chunks):
                x = conv[pl.ds(r, ALIGN), cut(c)]
                p, q = fold(x), fold(x * x)
                one, two = (p, q) if c == 0 else (one + p, two + q)
            st1[pl.ds(slot(r), ALIGN)] = jnp.where(
                lanes, jnp.sum(one, 1, keepdims=True), jnp.sum(two, 1, keepdims=True)
            )

    def transform_main(source, target, at, sign):
        target[pl.ds(0, rows)] = dot(mats[pl.ds(0, rows)], source[pl.ds(edge, rows)])
        multiply(0, rows, 0, sign, target)
        conv[pl.ds(edge, inner_rows)] = dot(mats[pl.ds(at, inner_rows)], prod[pl.ds(0, rows)])

    def transform_edges(source, target, at, sign):
        for e in range(2):
            window = source[pl.ds(e * (plan.wide - side), side)]
            target[pl.ds(rows + e * side, side)] = dot(emats[pl.ds(0, side)], window)
        for e in range(2):
            multiply(rows + e * side, side, rows, sign, target)
        for e in range(2):
            conv[pl.ds(e * (rows - edge), edge)] = dot(
                emats[pl.ds(at + e * edge, edge)], prod[pl.ds(rows + e * side, side)]
            )

    def swap(src, dst, start, count, k):
        place = pl.ds(start, count)
        return remote(
            src.at[place], dst.at[place], tp_send.at[k], tp_recv.at[k], (sp, 1 - tp)
        )

    cutoff = middle * ALIGN
    swap1 = [
        swap(st1, st1_in, 0, inner_rows, 0), swap(st1, st1_in, inner_rows, 2 * edge, 1)
    ]
    swap2 = [
        swap(st2, st2_in, 0, cutoff, 2), swap(st2, st2_in, cutoff, inner_rows - cutoff, 3),
        swap(st2, st2_in, inner_rows, 2 * edge, 4),
    ]

    def conv_main_phase():
        transform_main(gw, g_spec, plan.at_conv, 1.0)
        stats(main_rows)

    def conv_edge_phase():
        transform_edges(gw, g_spec, plan.edge_conv, 1.0)
        stats(edge_rows)

    loads[8].wait()
    conv_main_phase()
    swap1[0].start()
    handshake_across()
    loads[9].wait()
    lax.fori_loop(0, chunks, mix_step, 0)
    for load in loads[10:]:
        load.wait()
    hgain[...] = jnp.broadcast_to(0.5 * gain[...], hgain.shape)
    hshift[...] = jnp.broadcast_to(0.5 * shift[...], hshift.shape)

    def twice(x):
        return jnp.concatenate([x, x], 0)

    def halves(x):
        return x[:8] + x[8:]

    def norm_at(picked, opening):
        total_g, total_s = [None] * chunks, [None] * chunks
        for r in picked:
            part, place = pl.ds(r, ALIGN), pl.ds(slot(r), ALIGN)
            tot = (st1[place] + st1_in[place]) * (1.0 / width)
            mean = tot[:, :1]
            var = tot[:, LANES // 2 : LANES // 2 + 1] - mean * mean
            inv = lax.rsqrt(var + EPS)
            inv_s[place] = jnp.broadcast_to(inv, (ALIGN, LANES))
            one = two = None
            for c in range(chunks):
                hg = twice(hgain[:, cut(c)])
                normed = (conv[part, cut(c)] - mean) * inv
                half_pre = normed * hg + twice(hshift[:, cut(c)])
                th = jnp.tanh(half_pre)
                gp = gm[part, cut(c)] * (1.0 + th) * (1.0 + half_pre * (1.0 - th))
                gn = gp * hg
                gpn = gp * normed
                conv[part, cut(c)] = normed
                gm[part, cut(c)] = gn
                p, q = fold(gn), fold(gpn * hg)
                one, two = (p, q) if c == 0 else (one + p, two + q)
                g, h = halves(gpn), halves(gp)
                if total_g[c] is not None:
                    g, h = total_g[c] + g, total_s[c] + h
                total_g[c], total_s[c] = g, h
            st2[place] = jnp.where(
                lanes, jnp.sum(one, 1, keepdims=True), jnp.sum(two, 1, keepdims=True)
            )
        for c in range(chunks):
            if opening:
                colg[:, cut(c)] = total_g[c]
                cols[:, cut(c)] = total_s[c]
            else:
                colg[:, cut(c)] += total_g[c]
                cols[:, cut(c)] += total_s[c]

    def gc_at(picked):
        for r in picked:
            part, place = pl.ds(r, ALIGN), pl.ds(slot(r), ALIGN)
            tot = (st2[place] + st2_in[place]) * (1.0 / width)
            inv = inv_s[place]
            scaled = inv * tot
            m1 = scaled[:, :1]
            m2 = scaled[:, LANES // 2 : LANES // 2 + 1]
            inv = inv[:, :1]
            for c in range(chunks):
                gcw[pl.ds(r + edge, ALIGN), cut(c)] = (
                    inv * gm[part, cut(c)] - m1 - conv[part, cut(c)] * m2
                ).astype(BF16)

    swap1[0].wait_recv()
    norm_at(first_rows, True)
    swap2[0].start()
    recv_prv(gw_halo, gw)
    recv_nxt(gw_halo, gw)
    conv_edge_phase()
    swap1[1].start()
    handshake_down()
    norm_at(second_rows, False)
    swap2[1].start()
    swap2[0].wait_recv()
    gc_at(first_rows)
    swap1[1].wait_recv()
    norm_at(edge_rows, False)
    swap2[2].start()

    rg = jnp.sum(colg[...], 0, keepdims=True)
    rsh = jnp.sum(cols[...], 0, keepdims=True)
    groups = channels // LANES
    gs[sp] = jnp.concatenate(
        [x[:, k * LANES : (k + 1) * LANES] for x in (rg, rsh) for k in range(groups)], 0
    ).astype(BF16)

    def send_gs(d, carry):
        remote(gs.at[sp], gs.at[sp], all_send.at[0], all_recv.at[0], (peer(d), tp)).start()
        return carry

    handshake_done()
    lax.fori_loop(1, n, send_gs, 0)

    slots = owners.count * per
    if slots > tiles:
        rs_src[pl.ds(tiles, slots - tiles)] = jnp.zeros((slots - tiles, ALIGN, LANES), BF16)
    tall = plan.tap_rows // ALIGN

    def lag_part(at, size, f, c):
        high, low = pl.ds(at + f, ALIGN), pl.ds(at + size // 2 + f, ALIGN)
        re, im = spec_s[high, cut(c)], spec_s[low, cut(c)]
        hr, hi = g_spec[high, cut(c)], g_spec[low, cut(c)]
        return hr * re + hi * im, hr * im - hi * re

    def send_rs(i, carry):
        o = jnp.where(low_side, owners.count - 1 - i, i)
        to = owners.first + o

        @pl.when((to != sp) | (tp != 1))
        def _():
            remote(rs_src.at[pl.ds(o * per, per)], rs_in.at[2 * sp + tp],
                   all_send.at[1], all_recv.at[1], (to, 1)).start()

        return carry

    def spec_main_phase():
        spec_s[pl.ds(0, rows)] = dot(own[...], gcw[pl.ds(2 * edge, inner_rows)])
        for f in range(0, rows // 2, ALIGN):
            for c in range(chunks):
                dr, di = lag_part(0, rows, f, c)
                prod[pl.ds(f, ALIGN), cut(c)] = dr.astype(BF16)
                prod[pl.ds(rows // 2 + f, ALIGN), cut(c)] = di.astype(BF16)
        lag_s[...] = (
            dot(mats[pl.ds(plan.at_lags, plan.tap_rows)], prod[pl.ds(0, rows)])
            * plan.lag_scale[0]
        )

    def spec_edge_phase():
        for e in range(2):
            spec_s[pl.ds(rows + e * side, side)] = dot(
                eown[pl.ds(e * side, side)], gcw[pl.ds(edge + e * (rows - edge), edge)]
            )
        for f in range(0, side // 2, ALIGN):
            for c in range(chunks):
                r0, i0 = lag_part(rows, side, f, c)
                r1, i1 = lag_part(rows + side, side, f, c)
                prod[pl.ds(rows + f, ALIGN), cut(c)] = (r0 + r1).astype(BF16)
                prod[pl.ds(rows + side // 2 + f, ALIGN), cut(c)] = (i0 + i1).astype(BF16)
        out = lag_s[...] + plan.lag_scale[1] * dot(
            emats[pl.ds(plan.edge_lags, plan.tap_rows)], prod[pl.ds(rows, side)]
        )
        out = out.astype(BF16)
        for r in range(tall):
            for k in range(groups):
                rs_src[k * tall + r] = out[
                    r * ALIGN : (r + 1) * ALIGN, k * LANES : (k + 1) * LANES
                ]

    swap2[1].wait_recv()
    gc_at(second_rows)
    spec_main_phase()
    swap2[2].wait_recv()
    gc_at(edge_rows)
    spec_edge_phase()
    lax.fori_loop(0, owners.count, send_rs, 0)
    send_halo(gc_halo)

    def sum_phase():
        @pl.when(is_owner)
        def _():
            o = sp - owners.first
            rs_in[2 * sp + 1] = rs_src[pl.ds(o * per, per)]
            settle(rs_in, 2 * n - 1, all_recv.at[1])
            zero = jnp.zeros((2, per, ALIGN, LANES), F32)
            summed = lax.fori_loop(
                0, n, lambda i, t: t + rs_in[pl.ds(2 * i, 2)].astype(F32), zero, unroll=4
            )
            ag_src[...] = summed.astype(BF16)
            ag[o] = ag_src[1]

    def gather_phase(first, count):
        @pl.when(is_owner)
        def _():
            o = sp - owners.first

            def send_ag(i, carry):
                for t in range(2):
                    @pl.when((i != sp) | (t != 1))
                    def _():
                        remote(ag_src.at[t], ag.at[o],
                               all_send.at[2], all_recv.at[2], (i, t)).start()

                return carry

            lax.fori_loop(first, first + count, send_ag, 0)

    def finish(picked):
        for r in picked:
            part = pl.ds(r, ALIGN)
            for c in range(chunks):
                sig = sig_s[part, cut(c)]
                left = conv[part, cut(c)] * sig
                dv[part, cut(c)] = left.astype(BF16)
                dg[part, cut(c)] = (
                    left * value[part, cut(c)].astype(F32) * (1.0 - sig)
                ).astype(BF16)

    def out_main_phase():
        transform_main(gcw, spec_s, plan.at_grad, -1.0)
        finish(main_rows)

    def out_edge_phase():
        transform_edges(gcw, spec_s, plan.edge_grad, -1.0)
        finish(edge_rows)

    out_main_phase()
    sum_phase()
    gather_phase(0, n)
    recv_prv(gc_halo, gcw)
    recv_nxt(gc_halo, gcw)
    out_edge_phase()
    settle(gs, n - 1, all_recv.at[0])
    small = lax.fori_loop(
        0, n, lambda i, t: t + gs[i].astype(F32), jnp.zeros(gs.shape[1:], F32)
    )
    dgs_o[...] = small * (0.5 / math.sqrt(total))

    sent_halo(gw_halo)
    sent_halo(gc_halo)
    for each in swap1 + swap2:
        each.wait_send()
    settle(gs, n - 1, all_send.at[0])

    @pl.when(is_owner)
    def _():
        settle(rs_in, owners.count - 1, all_send.at[1])
        settle(ag, owners.count - 1, all_recv.at[2])

    @pl.when(jnp.logical_not(is_owner))
    def _():
        settle(rs_in, owners.count, all_send.at[1])
        settle(ag, owners.count, all_recv.at[2])

    for t in range(tiles):
        k, r = t // tall, t % tall
        count = min(ALIGN, plan.kernel - r * ALIGN)
        dt_o[pl.ds(r * ALIGN, count), pl.ds(k * LANES, LANES)] = ag[t // per, t % per].astype(F32)[
            :count
        ]

    @pl.when(is_owner)
    def _():
        settle(rs_in, 2 * n - 1, all_send.at[2])


def store(*refs):
    sources, targets, out_sem = refs[:4], refs[4:9], refs[9]
    groups = sources[3].shape[0] // 2
    views = list(sources[:3]) + [
        sources[3].at[pl.ds(0, groups)], sources[3].at[pl.ds(groups, groups)]
    ]
    copies = [
        pltpu.make_async_copy(a, b, out_sem.at[i]) for i, (a, b) in enumerate(zip(views, targets))
    ]
    for copy in copies:
        copy.start()
    for copy in copies:
        copy.wait()


def shards(n, value_in, gate_in, taps, gain, shift, w_out, grad_out):
    rows, channels = value_in.shape
    kernel = taps.shape[0]
    total = rows * n
    plan = Plan(rows, kernel, total)
    groups = channels // LANES
    tiles = plan.tap_rows // ALIGN * groups
    owners = Owners(n, tiles)
    per = owners.per
    model = grad_out.shape[1]
    mats = jnp.asarray(plan.main, BF16)
    emats = jnp.asarray(plan.edges, BF16)
    own = jnp.asarray(plan.own, BF16)
    eown = jnp.asarray(plan.own_edges, BF16)
    ft = jnp.asarray(plan.taps, BF16)
    hbm = pl.BlockSpec(memory_space=pltpu.HBM)
    vmem = pl.BlockSpec(memory_space=pltpu.VMEM)
    both = rows + 2 * plan.side
    chunks = channels // CHUNK
    dma = pltpu.SemaphoreType.DMA
    results = pl.pallas_call(
        functools.partial(body, plan, n, tiles, owners, total),
        out_shape=(
            pltpu.VMEM((rows, channels), BF16),
            pltpu.VMEM((rows, channels), BF16),
            pltpu.VMEM((kernel, channels), F32),
            pltpu.VMEM((2 * groups, LANES), F32),
        ),
        in_specs=[hbm] * 12,
        out_specs=(vmem,) * 4,
        scratch_shapes=[
            pltpu.VMEM((rows, channels), BF16),
            pltpu.VMEM((rows, channels), BF16),
            pltpu.VMEM((kernel, channels), F32),
            pltpu.VMEM((channels, model), BF16),
            pltpu.VMEM((rows, model), BF16),
            pltpu.VMEM(plan.main.shape, BF16),
            pltpu.VMEM(plan.edges.shape, BF16),
            pltpu.VMEM(plan.own.shape, BF16),
            pltpu.VMEM(plan.own_edges.shape, BF16),
            pltpu.VMEM((rows, channels), F32),
            pltpu.VMEM((plan.wide, channels), BF16),
            pltpu.VMEM((rows, channels), F32),
            pltpu.VMEM((rows, channels), F32),
            pltpu.VMEM((plan.wide, channels), BF16),
            pltpu.VMEM((3 * plan.tap_rows, channels), BF16),
            pltpu.VMEM((rows + plan.side, channels), F32),
            pltpu.VMEM((both, channels), F32),
            pltpu.VMEM((both, channels), F32),
            pltpu.VMEM((both, channels), BF16),
            pltpu.VMEM((plan.tap_rows, channels), F32),
            pltpu.VMEM((rows, LANES), F32),
            pltpu.VMEM((rows, LANES), F32),
            pltpu.VMEM((rows, LANES), F32),
            pltpu.VMEM((rows, LANES), F32),
            pltpu.VMEM((rows, LANES), F32),
            pltpu.VMEM((8, channels), F32),
            pltpu.VMEM((8, channels), F32),
            pltpu.VMEM((8, channels), F32),
            pltpu.VMEM((8, channels), F32),
            pltpu.VMEM((n, 2 * groups, LANES), BF16),
            pltpu.VMEM((owners.count * per, ALIGN, LANES), BF16),
            pltpu.VMEM((2 * n, per, ALIGN, LANES), BF16),
            pltpu.VMEM((2, per, ALIGN, LANES), BF16),
            pltpu.VMEM((owners.count, per, ALIGN, LANES), BF16),
            pltpu.VMEM(plan.taps.shape, BF16),
            pltpu.VMEM((1, channels), F32),
            pltpu.VMEM((1, channels), F32),
            pltpu.SemaphoreType.REGULAR((3,)),
            dma((15,)), dma((chunks,)), dma((4,)), dma((4,)),
            dma((5,)), dma((5,)), dma((3,)), dma((3,)),
        ],
        compiler_params=pltpu.CompilerParams(
            collective_id=0, has_side_effects=True, vmem_limit_bytes=VMEM_GRANT,
        ),
    )(
        *(
            pltpu.with_memory_space_constraint(x, pltpu.HBM)
            for x in (
                value_in, gate_in, taps, gain.reshape(1, -1), shift.reshape(1, -1), w_out,
                grad_out, mats, emats, own, eown, ft,
            )
        )
    )
    results = [pltpu.with_memory_space_constraint(x, pltpu.VMEM) for x in results]
    d_value, d_gate, d_taps, d_gain, d_shift = pl.pallas_call(
        store,
        out_shape=(
            jax.ShapeDtypeStruct((rows, channels), BF16),
            jax.ShapeDtypeStruct((rows, channels), BF16),
            jax.ShapeDtypeStruct((kernel, channels), F32),
            jax.ShapeDtypeStruct((groups, LANES), F32),
            jax.ShapeDtypeStruct((groups, LANES), F32),
        ),
        in_specs=[vmem] * 4,
        out_specs=(hbm,) * 5,
        scratch_shapes=[dma((5,))],
        compiler_params=pltpu.CompilerParams(vmem_limit_bytes=8 * 1024 * 1024),
    )(*results)
    return (d_value, d_gate, d_taps, d_gain.reshape(-1), d_shift.reshape(-1))


def solution(mesh):
    return jax.shard_map(
        functools.partial(shards, mesh.shape["sp"]),
        mesh=mesh,
        in_specs=(
            P("sp", "tp"),
            P("sp", "tp"),
            P(None, "tp"),
            P("tp"),
            P("tp"),
            P("tp", None),
            P("sp", None),
        ),
        out_specs=(P("sp", "tp"), P("sp", "tp"), P(None, "tp"), P("tp"), P("tp")),
        check_vma=False,
    )
```
